512 devices in a mesh: ep: 128 (over z, y, core), tp: 4 (over x).
Axes of the slice: x: 4, y: 8, z: 8, core: 2. Of those that a mesh axis runs over, the one named last changes fastest.
Arguments:
- tokens: bfloat16 [2048, 2048], P('ep'), may hold values from -6 to 6
- head_state: float32 [2048, 16, 4096], P('ep', 'tp'), may hold values from -6 to 6
- mixer_gain: float32 [2048], replicated, may hold values from 0.1 to 1.9
- w_query: bfloat16 [2048, 1024], P('ep', 'tp'), may hold values from -0.125 to 0.125
- w_key: bfloat16 [2048, 1024], P('ep', 'tp'), may hold values from -0.125 to 0.125
- w_value: bfloat16 [2048, 1024], P('ep', 'tp'), may hold values from -0.125 to 0.125
- decay_down: bfloat16 [2048, 64], replicated, may hold values from -0.125 to 0.125
- decay_up: bfloat16 [64, 1024], replicated, may hold values from -3 to 3
- decay_base: float32 [1024], P('tp'), may hold values from -4 to 0
- rate_down: bfloat16 [2048, 64], replicated, may hold values from -0.125 to 0.125
- rate_up: bfloat16 [64, 1024], replicated, may hold values from -0.75 to 0.75
- head_gain: float32 [1024], P('tp'), may hold values from 0.1 to 1.9
- w_out: bfloat16 [1024, 2048], P('tp', 'ep'), may hold values from -0.1875 to 0.1875
- expert_gain: float32 [2048], replicated, may hold values from 0.1 to 1.9
- expert_ids: int32 [2048, 2], P('ep'), may hold values from 0 to 127, all different within a row; in each aligned block of 16 rows (0 to 15, 16 to 31, ...) at most 1 rows name the same one
- route_weight: float32 [2048, 2], P('ep'), may hold values from 0.2 to 1
- w_gate: bfloat16 [128, 2048, 512], P('ep', None, 'tp'), may hold values from -0.125 to 0.125
- w_up: bfloat16 [128, 2048, 512], P('ep', None, 'tp'), may hold values from -0.125 to 0.125
- w_down: bfloat16 [128, 512, 2048], P('ep', 'tp'), may hold values from -0.25 to 0.25
Outputs:
- layer_out: bfloat16 [2048, 2048], P('ep', 'tp')
- next_state: float32 [2048, 16, 4096], P('ep', 'tp')
The draws below stay inside these ranges and needn't reach their ends.
Inputs may be any that keep to these rules, and one draw needn't show every extreme that they name: `expert_ids`: each row names 2 different experts; among the 16 rows of one index of ep no expert is named more than 1 times, and in the rows of some indices one expert is named exactly 1 times.
All inputs are finite; a program needn't handle non-finite values.
Results may differ from the reference program's by a relative error of at most 0.015.
Values may be sent and summed in bfloat16 or wider, within the bound.
No kernel may reach another device: no remote copies, remote signals or barrier semaphores. Data moves between devices by JAX's collectives and lax.ppermute only.
A program may use at most 64 MiB of HBM per device.

```python
import math
import jax
import jax.numpy as jnp
import numpy as np
from jax import lax

D = 2048
HEADS = 16
HS = 64
RANK = 64
FF = 512
TOP_K = 2
SEQ_DEV = 16
D_A = 1024
TOKENS = 2048
EXPERTS = 128
CAP = 1
N_EP = 128


def level_of(key, dims, pieces, smallest, top_value):
    def one(position, shards_of):
        draws = jax.random.uniform(jax.random.fold_in(jax.random.fold_in(key, 6), position), (shards_of,), jnp.float32, smallest / len(pieces), top_value / len(pieces))
        return jnp.repeat(jnp.exp(draws), dims[position] // shards_of).reshape((-1,) + (1,) * (len(dims) - position - 1))

    level = one(*pieces[0])
    for cut in pieces[1:]:
        level = level * one(*cut)
    return level


def assign_block(stream_key, own, number, rows, count, top, most, lean):
    ranking = jax.random.permutation(stream_key, count)
    packed, ordinary = load_shares(count, rows * top, most, lean, True), load_shares(count, rows * top, most, lean, False)
    places = jnp.arange(count)

    def named(sizes, offset_by):
        used = int((sizes > 0).sum())
        fixed = max(1, used // 4)
        passed = fixed + (places - fixed + offset_by * (used - fixed)) % max(1, count - fixed)
        return jnp.zeros((count,), jnp.int32).at[ranking[jnp.where(places < fixed, places, passed)]].set(jnp.asarray(sizes, jnp.int32))

    sizes = jnp.where(number % 4 == 0, named(packed, number // 4), named(ordinary, number - number // 4 - 1))
    mixed = jax.random.permutation(jax.random.fold_in(own, 3), count)
    giver, receiver = mixed[0:count // 2 * 2:2], mixed[1:count // 2 * 2:2]
    margin = jnp.minimum(sizes[giver] - 1, most - sizes[receiver]) // 2
    margin = jnp.where((giver == ranking[0]) | (receiver == ranking[0]) | (sizes[receiver] == 0), 0, jnp.maximum(margin, 0))
    passed = jax.random.randint(jax.random.fold_in(own, 4), (count // 2,), 0, 1 << 20) % (margin + 1)
    sizes = sizes.at[giver].add(-passed).at[receiver].add(passed)
    labels = jnp.searchsorted(jnp.cumsum(sizes), jnp.arange(rows * top), side="right").astype(jnp.int32)
    listing = labels.reshape(top, rows).T
    listing = listing[jax.random.permutation(jax.random.fold_in(own, 1), rows)]
    offset_by = jax.random.randint(jax.random.fold_in(own, 2), (rows, 1), 0, top)
    return jnp.take_along_axis(listing, (jnp.arange(top)[None, :] + offset_by) % top, axis=1)


def load_shares(amount, total, reach, skew, full):
    weights = [(1 << 20) // math.isqrt(standing ** skew) + 1 for standing in range(1, amount + 1)]
    largest = reach if full else min(reach, max(-(-total // amount), total * weights[0] // sum(weights)))
    least = 1 if total - largest >= amount - 1 else 0
    counts, spare = [largest] + [least] * (amount - 1), total - largest - least * (amount - 1)
    while spare > 0:
        free = [i for i in range(1, amount) if counts[i] < largest] or [i for i in range(1, amount) if counts[i] < reach]
        whole, budget = sum([weights[i] for i in free]), spare
        for i in free:
            addition = min(reach - counts[i], max(1, budget * weights[i] // whole), spare)
            counts[i] = counts[i] + addition
            spare = spare - addition
    return np.array(counts)


def gaussian(stream_key, dims, scale, limit, shards=(), kind=jnp.bfloat16):
    drawn = scale * jax.random.normal(stream_key, dims, jnp.float32)
    if shards:
        drawn = drawn * level_of(stream_key, dims, shards, -0.22, 0.18)
    return jnp.clip(drawn, -limit, limit).astype(kind)


def setup_inputs(seed: int = 0) -> dict:
    splits = jax.random.split(jax.random.key(seed), 20)
    tokens = gaussian(splits[0], (TOKENS, D), 1.0, 6.0, ((0, 128),))
    head_state = gaussian(splits[1], (TOKENS, HEADS, HS * HS), 1.0, 6.0, ((0, 128), (1, 4)), jnp.float32)
    mixer_gain = jnp.clip(1.0 + 0.18 * jax.random.normal(splits[2], (D,), jnp.float32), 0.1, 1.9)
    w_query = gaussian(splits[3], (D, D_A), D ** -0.5, 0.125, ((0, 128), (1, 4)))
    w_key = gaussian(splits[4], (D, D_A), D ** -0.5, 0.125, ((0, 128), (1, 4)))
    w_value = gaussian(splits[5], (D, D_A), D ** -0.5, 0.125, ((0, 128), (1, 4)))
    decay_down = gaussian(splits[6], (D, RANK), D ** -0.5, 0.125)
    decay_up = gaussian(splits[7], (RANK, D_A), 0.5, 3.0)
    decay_base = jnp.clip(-4.0 + 4.0 * jax.random.uniform(splits[8], (D_A,), jnp.float32) ** level_of(splits[8], (D_A,), ((0, 4),), -0.2, 0.2), -4.0, 0.0)
    rate_down = gaussian(splits[9], (D, RANK), D ** -0.5, 0.125)
    rate_up = gaussian(splits[10], (RANK, D_A), RANK ** -0.5, 0.75)
    head_gain = jnp.clip(1.0 + 0.18 * jax.random.normal(splits[11], (D_A,), jnp.float32), 0.1, 1.9)
    w_out = gaussian(splits[12], (D_A, D), D_A ** -0.5, 0.1875, ((0, 4), (1, 128)))
    expert_gain = jnp.clip(1.0 + 0.18 * jax.random.normal(splits[13], (D,), jnp.float32), 0.1, 1.9)
    expert_ids_keys = jax.random.split(jax.random.fold_in(splits[14], 1), TOKENS // SEQ_DEV)
    expert_ids_turns = jax.random.permutation(jax.random.fold_in(splits[14], 3), TOKENS // SEQ_DEV)
    expert_ids = jax.vmap(lambda own, number: assign_block(jax.random.fold_in(splits[14], 2), own, number, SEQ_DEV, EXPERTS, TOP_K, CAP, 2))(expert_ids_keys, expert_ids_turns).reshape((TOKENS, TOP_K))
    route_weight = jnp.clip(jnp.exp(math.log(1.0) - 1.609438 * jax.random.uniform(splits[15], (TOKENS, TOP_K), jnp.float32) ** level_of(splits[15], (TOKENS, TOP_K), ((0, 128),), -0.2, 0.2)), 0.2, 1.0)
    w_gate = gaussian(splits[16], (EXPERTS, D, FF), D ** -0.5, 0.125, ((0, 128), (2, 4)))
    w_up = gaussian(splits[17], (EXPERTS, D, FF), D ** -0.5, 0.125, ((0, 128), (2, 4)))
    w_down = gaussian(splits[18], (EXPERTS, FF, D), FF ** -0.5, 0.25, ((0, 128), (1, 4)))
    return {"tokens": tokens, "head_state": head_state, "mixer_gain": mixer_gain, "w_query": w_query, "w_key": w_key, "w_value": w_value, "decay_down": decay_down, "decay_up": decay_up, "decay_base": decay_base, "rate_down": rate_down, "rate_up": rate_up, "head_gain": head_gain, "w_out": w_out, "expert_gain": expert_gain, "expert_ids": expert_ids, "route_weight": route_weight, "w_gate": w_gate, "w_up": w_up, "w_down": w_down}


norm_eps = 1e-06
group_eps = 0.00064

def rms_scale(activity, gain):
    widened = activity.astype(jnp.float32)
    scaled = widened * lax.rsqrt(lax.optimization_barrier(jnp.mean(widened * widened, axis=-1, keepdims=True)) + norm_eps)
    return (scaled * gain).astype(jnp.bfloat16)

def low_rank(normed, decay_down, decay_up, decay_base, rate_down, rate_up):
    decay_low = jnp.tanh(jnp.dot(normed, decay_down, preferred_element_type=jnp.float32)).astype(jnp.bfloat16)
    decay_pre = decay_base + jnp.dot(decay_low, decay_up, preferred_element_type=jnp.float32)
    decays = jnp.exp(-jnp.exp(-jax.nn.softplus(-decay_pre) - 0.5))
    rate_low = jnp.dot(normed, rate_down, preferred_element_type=jnp.float32).astype(jnp.bfloat16)
    rates = jax.nn.sigmoid(jnp.dot(rate_low, rate_up, preferred_element_type=jnp.float32))
    return (decays, rates)

def recurrence(queries, key_rows, value_rows, decays, rates, old_state, head_gain):
    row_count, head_count, _ = old_state.shape
    head_size = queries.shape[1] // head_count
    head_shape = (row_count, head_count, head_size)
    query_heads = queries.astype(jnp.float32).reshape(head_shape)
    key_heads = key_rows.astype(jnp.float32).reshape(head_shape)
    value_heads = value_rows.astype(jnp.float32).reshape(head_shape)
    decay_heads = decays.reshape(head_shape)
    rate_heads = rates.reshape(head_shape)
    unit_keys = key_heads * lax.rsqrt(lax.optimization_barrier(jnp.sum(key_heads * key_heads, axis=-1, keepdims=True)) + 1.0)
    state_grid = old_state.reshape(row_count, head_count, head_size, head_size)
    removed = lax.optimization_barrier(jnp.sum(state_grid * unit_keys[:, :, None, :], axis=-1))
    updated = state_grid * decay_heads[:, :, None, :] - removed[:, :, :, None] * (unit_keys * rate_heads)[:, :, None, :] + value_heads[:, :, :, None] * key_heads[:, :, None, :]
    readout = lax.optimization_barrier(jnp.sum(updated * query_heads[:, :, None, :], axis=-1))
    centred = readout - lax.optimization_barrier(jnp.mean(readout, axis=-1, keepdims=True))
    spread = lax.optimization_barrier(jnp.mean(centred * centred, axis=-1, keepdims=True))
    scaled = centred * lax.rsqrt(spread + group_eps) * head_gain.reshape(head_count, head_size)
    return (updated.reshape(row_count, head_count, head_size * head_size), scaled.reshape(row_count, head_count * head_size).astype(jnp.bfloat16))

def reference(tokens, head_state, mixer_gain, w_query, w_key, w_value, decay_down, decay_up, decay_base, rate_down, rate_up, head_gain, w_out, expert_gain, expert_ids, route_weight, w_gate, w_up, w_down):
    normed = rms_scale(tokens, mixer_gain)
    queries = jnp.dot(normed, w_query, preferred_element_type=jnp.float32).astype(jnp.bfloat16)
    key_rows = jnp.dot(normed, w_key, preferred_element_type=jnp.float32).astype(jnp.bfloat16)
    value_rows = jnp.dot(normed, w_value, preferred_element_type=jnp.float32).astype(jnp.bfloat16)
    decays, rates = low_rank(normed, decay_down, decay_up, decay_base, rate_down, rate_up)
    next_state, head_out = recurrence(queries, key_rows, value_rows, decays, rates, head_state, head_gain)
    mixed_out = jnp.dot(head_out, w_out, preferred_element_type=jnp.float32)
    residual = (tokens.astype(jnp.float32) + mixed_out).astype(jnp.bfloat16)
    expert_in = rms_scale(residual, expert_gain)
    top_count = expert_ids.shape[1]
    flat_ids = expert_ids.reshape(-1).astype(jnp.int32)
    pair_count = flat_ids.shape[0]
    shares = (route_weight / lax.optimization_barrier(jnp.sum(route_weight, axis=1, keepdims=True))).reshape(-1)
    buffer_rows = N_EP * CAP
    positions = jnp.arange(pair_count, dtype=jnp.int32)

    def one_expert(running, inputs):
        expert, gate_local, up_local, down_local = inputs
        matches = flat_ids == expert
        order_keys = jnp.where(matches, positions, positions + pair_count)
        chosen = jnp.argsort(order_keys)[:buffer_rows].astype(jnp.int32)
        in_range = jnp.arange(buffer_rows, dtype=jnp.int32) < jnp.sum(matches.astype(jnp.int32))
        owners = (chosen // top_count).astype(jnp.int32)
        picked = expert_in[owners]
        gate_act = jnp.dot(picked, gate_local, preferred_element_type=jnp.float32)
        up_act = jnp.dot(picked, up_local, preferred_element_type=jnp.float32)
        hidden = (jax.nn.silu(gate_act) * up_act).astype(jnp.bfloat16)
        result = jnp.dot(hidden, down_local, preferred_element_type=jnp.float32).astype(jnp.bfloat16)
        weights = jnp.where(in_range, shares[chosen], 0.0)
        running = running.at[owners].add(weights[:, None] * result.astype(jnp.float32))
        return (running, None)
    zero_sums = jnp.zeros(expert_in.shape, jnp.float32)
    routed, _ = lax.scan(one_expert, zero_sums, (jnp.arange(EXPERTS, dtype=jnp.int32), w_gate, w_up, w_down))
    layer_out = (residual.astype(jnp.float32) + routed).astype(jnp.bfloat16)
    return (layer_out, next_state)
```

```python
import math

import jax
import jax.numpy as jnp
from jax import lax
from jax.sharding import Mesh, PartitionSpec as P

norm_eps = 1e-06
group_eps = 0.00064
EP = ("z", "y", "c")
PLANE = ("y", "c")


def swap(array, axis):
    return lax.all_to_all(array, axis, split_axis=0, concat_axis=0, tiled=True)


def to_all(array, axis):
    return swap(jnp.broadcast_to(array, (lax.axis_size(axis), *array.shape)), axis)


def rms_scale(activity, gain):
    widened = activity.astype(jnp.float32)
    scaled = widened * lax.rsqrt(jnp.mean(widened * widened, axis=-1, keepdims=True) + norm_eps)
    return (scaled * gain).astype(jnp.bfloat16)


def low_rank(normed, decay_down, decay_up, decay_base, rate_down, rate_up):
    decay_low = jnp.tanh(jnp.dot(normed, decay_down, preferred_element_type=jnp.float32)).astype(
        jnp.bfloat16
    )
    decay_pre = decay_base + jnp.dot(decay_low, decay_up, preferred_element_type=jnp.float32)
    decays = jnp.exp(-jnp.exp(-jax.nn.softplus(-decay_pre) - 0.5))
    rate_low = jnp.dot(normed, rate_down, preferred_element_type=jnp.float32).astype(jnp.bfloat16)
    rates = jax.nn.sigmoid(jnp.dot(rate_low, rate_up, preferred_element_type=jnp.float32))
    return (decays, rates)


def recurrence(queries, key_rows, value_rows, decays, rates, old_state, head_gain):
    row_count, head_count, _ = old_state.shape
    head_size = queries.shape[1] // head_count
    head_shape = (row_count, head_count, head_size)
    query_heads = queries.astype(jnp.float32).reshape(head_shape)
    key_heads = key_rows.astype(jnp.float32).reshape(head_shape)
    value_heads = value_rows.astype(jnp.float32).reshape(head_shape)
    decay_heads = decays.reshape(head_shape)
    rate_heads = rates.reshape(head_shape)
    unit_keys = key_heads * lax.rsqrt(jnp.sum(key_heads * key_heads, axis=-1, keepdims=True) + 1.0)
    state_grid = old_state.reshape(row_count, head_count, head_size, head_size)
    removed = jnp.sum(state_grid * unit_keys[:, :, None, :], axis=-1)
    updated = (
        state_grid * decay_heads[:, :, None, :]
        - removed[:, :, :, None] * (unit_keys * rate_heads)[:, :, None, :]
        + value_heads[:, :, :, None] * key_heads[:, :, None, :]
    )
    readout = jnp.sum(updated * query_heads[:, :, None, :], axis=-1)
    centred = readout - jnp.mean(readout, axis=-1, keepdims=True)
    spread = jnp.mean(centred * centred, axis=-1, keepdims=True)
    scaled = centred * lax.rsqrt(spread + group_eps) * head_gain.reshape(head_count, head_size)
    return (
        updated.reshape(row_count, head_count, head_size * head_size),
        scaled.reshape(row_count, head_count * head_size).astype(jnp.bfloat16),
    )


def body(
    tokens,
    head_state,
    mixer_gain,
    w_query,
    w_key,
    w_value,
    decay_down,
    decay_up,
    decay_base,
    rate_down,
    rate_up,
    head_gain,
    w_out,
    expert_gain,
    expert_ids,
    route_weight,
    w_gate,
    w_up,
    w_down,
):
    rows, width = tokens.shape
    cols = w_query.shape[1]
    layers = lax.axis_size("z")
    lanes = lax.axis_size("tp")
    experts = lax.axis_size(EP)
    lane = lax.axis_index("tp")
    block = width // layers
    quarter = width // lanes

    weights = lax.all_gather(
        jnp.concatenate([w_query, w_key, w_value, w_out.T], axis=1), PLANE, axis=0, tiled=True
    )
    normed = rms_scale(tokens, mixer_gain)
    spread_rows = swap(normed.reshape(rows, layers, block).transpose(1, 0, 2), "z")
    partial_rows = jnp.dot(
        spread_rows.reshape(layers * rows, block),
        weights[:, : 3 * cols],
        preferred_element_type=jnp.float32,
    ).astype(jnp.bfloat16)
    summed = swap(partial_rows.reshape(layers, rows, 3 * cols), "z")
    projected = jnp.sum(summed.astype(jnp.float32), axis=0).astype(jnp.bfloat16)
    queries, key_rows, value_rows = jnp.split(projected, 3, axis=1)
    decays, rates = low_rank(
        normed,
        decay_down,
        lax.dynamic_slice_in_dim(decay_up, lane * cols, cols, 1),
        decay_base,
        rate_down,
        lax.dynamic_slice_in_dim(rate_up, lane * cols, cols, 1),
    )
    next_state, head_out = recurrence(
        queries, key_rows, value_rows, decays, rates, head_state, head_gain
    )
    heads_here = to_all(head_out, "z").reshape(layers * rows, cols)
    partial_out = lax.dot_general(
        heads_here,
        weights[:, 3 * cols :],
        (((1,), (1,)), ((), ())),
        preferred_element_type=jnp.float32,
    ).astype(jnp.bfloat16)
    home_out = swap(partial_out.reshape(layers, rows, block), "z")
    quarters = home_out.reshape(lanes, layers // lanes, rows, block).transpose(0, 2, 1, 3)
    mixed_parts = swap(quarters.reshape(lanes, rows, quarter), "tp")
    mixed_out = jnp.sum(mixed_parts.astype(jnp.float32), axis=0)
    own_tokens = lax.dynamic_slice_in_dim(tokens, lane * quarter, quarter, 1)
    residual = (own_tokens.astype(jnp.float32) + mixed_out).astype(jnp.bfloat16)

    match = expert_ids[:, :, None] == jnp.arange(experts, dtype=jnp.int32)[None, None, :]
    picker = jnp.any(match, axis=1).astype(jnp.bfloat16)
    outbound = jnp.einsum("ts,td->sd", picker, residual, preferred_element_type=jnp.float32)
    arrived = swap(outbound.astype(jnp.bfloat16).reshape(experts, 1, quarter), EP)
    whole = to_all(arrived.reshape(experts, quarter), "tp")
    widened = whole.astype(jnp.float32)
    mean_square = jnp.sum(widened * widened, axis=(0, 2), keepdims=True) / width
    gains = expert_gain.reshape(lanes, 1, quarter)
    flat_rows = (widened * lax.rsqrt(mean_square + norm_eps) * gains).astype(jnp.bfloat16)
    flat_rows = flat_rows.transpose(1, 0, 2).reshape(experts, width)
    gate_act = jnp.dot(flat_rows, w_gate[0], preferred_element_type=jnp.float32)
    up_act = jnp.dot(flat_rows, w_up[0], preferred_element_type=jnp.float32)
    hidden = (jax.nn.silu(gate_act) * up_act).astype(jnp.bfloat16)
    expert_parts = jnp.dot(hidden, w_down[0], preferred_element_type=jnp.float32)
    expert_parts = expert_parts.astype(jnp.bfloat16).reshape(experts, lanes, quarter)
    gathered = swap(expert_parts.transpose(1, 0, 2), "tp")
    reduced = jnp.sum(gathered.astype(jnp.float32), axis=0).astype(jnp.bfloat16)
    returned = swap(reduced.reshape(experts, 1, quarter), EP).reshape(experts, quarter)
    shares = route_weight / jnp.sum(route_weight, axis=1, keepdims=True)
    combine = jnp.sum(match.astype(jnp.float32) * shares[:, :, None], axis=1)
    routed = jnp.dot(combine, returned.astype(jnp.float32))
    layer_out = (residual.astype(jnp.float32) + routed).astype(jnp.bfloat16)
    return (layer_out, next_state)


def solution(mesh):
    side = math.isqrt(mesh.shape["ep"] // 2)
    grid = Mesh(
        mesh.devices.reshape(side, side, 2, mesh.shape["tp"]), ("z", "y", "c", "tp")
    )
    return jax.shard_map(
        body,
        mesh=grid,
        in_specs=(
            P(EP, None),
            P(EP, "tp", None),
            P(),
            P(EP, "tp"),
            P(EP, "tp"),
            P(EP, "tp"),
            P(),
            P(),
            P("tp"),
            P(),
            P(),
            P("tp"),
            P("tp", EP),
            P(),
            P(EP, None),
            P(EP, None),
            P(EP, None, "tp"),
            P(EP, None, "tp"),
            P(EP, "tp", None),
        ),
        out_specs=(P(EP, "tp"), P(EP, "tp", None)),
        check_vma=False,
    )
```

```python
import functools
import math

import jax
import jax.numpy as jnp
from jax import lax
from jax.experimental import pallas as pl
from jax.experimental.pallas import tpu as pltpu
from jax.sharding import Mesh, PartitionSpec as P

norm_eps = 1e-06
group_eps = 0.00064
EP = ("z", "y", "c")
PLANE = ("y", "c")


def swap(array, axis):
    return lax.all_to_all(array, axis, split_axis=0, concat_axis=0, tiled=True)


def to_all(array, axis):
    return swap(jnp.broadcast_to(array, (lax.axis_size(axis), *array.shape)), axis)


def rms_scale(activity, gain):
    widened = activity.astype(jnp.float32)
    scaled = widened * lax.rsqrt(jnp.mean(widened * widened, axis=-1, keepdims=True) + norm_eps)
    return (scaled * gain).astype(jnp.bfloat16)


def low_rank(normed, decay_down, decay_up, decay_base, rate_down, rate_up):
    decay_low = jnp.tanh(jnp.dot(normed, decay_down, preferred_element_type=jnp.float32)).astype(
        jnp.bfloat16
    )
    decay_pre = decay_base + jnp.dot(decay_low, decay_up, preferred_element_type=jnp.float32)
    decays = jnp.exp(-jnp.exp(-jax.nn.softplus(-decay_pre) - 0.5))
    rate_low = jnp.dot(normed, rate_down, preferred_element_type=jnp.float32).astype(jnp.bfloat16)
    rates = jax.nn.sigmoid(jnp.dot(rate_low, rate_up, preferred_element_type=jnp.float32))
    return (decays, rates)


def split_terms(value):
    high = value.astype(jnp.bfloat16)
    return high, (value - high.astype(jnp.float32)).astype(jnp.bfloat16)


def exact_dot(value, chooser):
    high, low = split_terms(value)
    return jnp.dot(high, chooser, preferred_element_type=jnp.float32) + jnp.dot(
        low, chooser, preferred_element_type=jnp.float32
    )


def recurrence_kernel(size, parts, decays, rates, gain, state, new_state, spread_out):
    count, cols = decays.shape
    heads = cols // size
    lines = state.shape[1]
    wide = state.shape[2]
    f32, bf16 = jnp.float32, jnp.bfloat16
    iota = lambda shape, dim: lax.broadcasted_iota(jnp.int32, shape, dim)
    projected = jnp.sum(parts[...].astype(f32), axis=0).astype(bf16).astype(f32)
    queries = projected[:, :cols]
    keys = projected[:, cols : 2 * cols]
    values = projected[:, 2 * cols :]
    square = (cols, cols)
    same_head = iota(square, 0) // size == iota(square, 1) // size
    head_sum = jnp.where(same_head, 1.0, 0.0).astype(f32)
    head_mean = head_sum * (1.0 / size)
    total = lambda x, m: jnp.dot(x, m, precision=lax.Precision.HIGHEST, preferred_element_type=f32)
    units = keys * lax.rsqrt(total(keys * keys, head_sum) + 1.0)
    removal = units * rates[...]

    def by_line(x):
        copies = jnp.broadcast_to(x[:, None, :], (count, 2 * heads, cols))
        chosen = iota(copies.shape, 2) // size == iota(copies.shape, 1) % heads
        kept = jnp.where(chosen, copies, 0.0)
        folded = kept[:, :, :wide]
        for start in range(wide, cols, wide):
            folded = folded + kept[:, :, start : start + wide]
        folded = folded.reshape(count * 2 * heads, wide)
        both = folded + pltpu.roll(folded, size, 1)
        return both.reshape(count, 1, 2 * heads, wide)

    grid_shape = (count, lines // (2 * heads), 2 * heads, wide)
    flat = (count * lines, wide)
    old = state[...].reshape(grid_shape)
    halves = (wide, wide)
    half_sum = jnp.where(iota(halves, 0) // size == iota(halves, 1) // size, 1.0, 0.0).astype(bf16)
    removed = exact_dot((old * by_line(units)).reshape(flat), half_sum).reshape(grid_shape)
    pick = (lines, cols)
    line, col = iota(pick, 0), iota(pick, 1)
    owner = (col // size == line % heads) & ((col % size) // 2 == line // heads)
    value_rows = jnp.where(owner[None], jnp.broadcast_to(values[:, None, :], (count, *pick)), 0.0)
    tall = (cols, wide)
    to_half = jnp.where(iota(tall, 0) % 2 == iota(tall, 1) // size, 1.0, 0.0).astype(bf16)
    value_grid = jnp.dot(
        value_rows.reshape(count * lines, cols).astype(bf16), to_half, preferred_element_type=f32
    ).reshape(grid_shape)
    updated = old * by_line(decays[...]) - removed * by_line(removal) + value_grid * by_line(keys)
    new_state[...] = updated.reshape(new_state.shape)
    broad = (wide, cols)
    from_half = jnp.where(iota(broad, 0) // size == iota(broad, 1) % 2, 1.0, 0.0).astype(bf16)
    reads = exact_dot((updated * by_line(queries)).reshape(flat), from_half)
    readout = jnp.sum(jnp.where(owner[None], reads.reshape(count, *pick), 0.0), axis=1)
    centred = readout - total(readout, head_mean)
    spread = total(centred * centred, head_mean)
    scaled = (centred * lax.rsqrt(spread + group_eps) * gain[...]).astype(bf16)
    spread_out[...] = jnp.broadcast_to(scaled[None], spread_out.shape)


def recurrence(parts, decays, rates, old_state, head_gain):
    layers = parts.shape[0]
    count, cols = decays.shape
    heads, area = old_state.shape[1:]
    size = math.isqrt(area)
    wide = 2 * size
    lines = area // wide
    state = old_state.reshape(count, heads, lines, wide).transpose(0, 2, 1, 3)
    state = state.reshape(count, lines * heads, wide)
    new_state, spread_out = pl.pallas_call(
        functools.partial(recurrence_kernel, size),
        out_shape=(
            jax.ShapeDtypeStruct(state.shape, jnp.float32),
            jax.ShapeDtypeStruct((layers, count, cols), jnp.bfloat16),
        ),
        compiler_params=pltpu.CompilerParams(vmem_limit_bytes=40 << 20),
        name="recurrence",
    )(parts, decays, rates, head_gain.reshape(1, cols), state)
    new_state = new_state.reshape(count, lines, heads, wide).transpose(0, 2, 1, 3)
    return new_state.reshape(old_state.shape), spread_out


def expert_kernel(rows, gain, gate, up, down, result):
    lanes, _, quarter = rows.shape
    f32 = jnp.float32
    squares = jnp.zeros((rows.shape[1], 1), f32)
    for part in range(lanes):
        widened = rows[part].astype(f32)
        squares = squares + jnp.sum(widened * widened, axis=1, keepdims=True)
    scale = lax.rsqrt(squares / (lanes * quarter) + norm_eps)
    gate_act = up_act = 0.0
    for part in range(lanes):
        here = slice(part * quarter, (part + 1) * quarter)
        normed = (rows[part].astype(f32) * scale * gain[part]).astype(jnp.bfloat16)
        gate_act = gate_act + jnp.dot(normed, gate[here], preferred_element_type=f32)
        up_act = up_act + jnp.dot(normed, up[here], preferred_element_type=f32)
    hidden = (gate_act / (1.0 + jnp.exp(-gate_act)) * up_act).astype(jnp.bfloat16)
    for part in range(lanes):
        here = slice(part * quarter, (part + 1) * quarter)
        product = jnp.dot(hidden, down[:, here], preferred_element_type=f32)
        result[part] = product.astype(jnp.bfloat16)


def expert_rows(rows, gain, gate, up, down):
    lanes, _, quarter = rows.shape
    return pl.pallas_call(
        expert_kernel,
        out_shape=jax.ShapeDtypeStruct(rows.shape, jnp.bfloat16),
        compiler_params=pltpu.CompilerParams(vmem_limit_bytes=20 << 20),
        name="expert",
    )(rows, gain.reshape(lanes, 1, quarter), gate, up, down)


def body(
    tokens,
    head_state,
    mixer_gain,
    w_query,
    w_key,
    w_value,
    decay_down,
    decay_up,
    decay_base,
    rate_down,
    rate_up,
    head_gain,
    w_out,
    expert_gain,
    expert_ids,
    route_weight,
    w_gate,
    w_up,
    w_down,
):
    rows, width = tokens.shape
    cols = w_query.shape[1]
    layers = lax.axis_size("z")
    lanes = lax.axis_size("tp")
    experts = lax.axis_size(EP)
    lane = lax.axis_index("tp")
    block = width // layers
    quarter = width // lanes

    weights = lax.all_gather(
        jnp.concatenate([w_query, w_key, w_value, w_out.T], axis=1), PLANE, axis=0, tiled=True
    )
    normed = rms_scale(tokens, mixer_gain)
    spread_rows = swap(normed.reshape(rows, layers, block).transpose(1, 0, 2), "z")
    partial_rows = jnp.dot(
        spread_rows.reshape(layers * rows, block),
        weights[:, : 3 * cols],
        preferred_element_type=jnp.float32,
    ).astype(jnp.bfloat16)
    summed = swap(partial_rows.reshape(layers, rows, 3 * cols), "z")
    decays, rates = low_rank(
        normed,
        decay_down,
        lax.dynamic_slice_in_dim(decay_up, lane * cols, cols, 1),
        decay_base,
        rate_down,
        lax.dynamic_slice_in_dim(rate_up, lane * cols, cols, 1),
    )
    next_state, spread_out = recurrence(summed, decays, rates, head_state, head_gain)
    heads_here = swap(spread_out, "z").reshape(layers * rows, cols)
    partial_out = lax.dot_general(
        heads_here,
        weights[:, 3 * cols :],
        (((1,), (1,)), ((), ())),
        preferred_element_type=jnp.float32,
    ).astype(jnp.bfloat16)
    home_out = swap(partial_out.reshape(layers, rows, block), "z")
    quarters = home_out.reshape(lanes, layers // lanes, rows, block).transpose(0, 2, 1, 3)
    mixed_parts = swap(quarters.reshape(lanes, rows, quarter), "tp")
    mixed_out = jnp.sum(mixed_parts.astype(jnp.float32), axis=0)
    own_tokens = lax.dynamic_slice_in_dim(tokens, lane * quarter, quarter, 1)
    residual = (own_tokens.astype(jnp.float32) + mixed_out).astype(jnp.bfloat16)

    match = expert_ids[:, :, None] == jnp.arange(experts, dtype=jnp.int32)[None, None, :]
    picker = jnp.any(match, axis=1).astype(jnp.bfloat16)
    outbound = jnp.einsum("ts,td->sd", picker, residual, preferred_element_type=jnp.float32)
    arrived = swap(outbound.astype(jnp.bfloat16).reshape(experts, 1, quarter), EP)
    whole = to_all(arrived.reshape(experts, quarter), "tp")
    expert_parts = expert_rows(whole, expert_gain, w_gate[0], w_up[0], w_down[0])
    gathered = swap(expert_parts, "tp")
    reduced = jnp.sum(gathered.astype(jnp.float32), axis=0).astype(jnp.bfloat16)
    returned = swap(reduced.reshape(experts, 1, quarter), EP).reshape(experts, quarter)
    shares = route_weight / jnp.sum(route_weight, axis=1, keepdims=True)
    combine = jnp.sum(match.astype(jnp.float32) * shares[:, :, None], axis=1)
    routed = jnp.dot(combine, returned.astype(jnp.float32))
    layer_out = (residual.astype(jnp.float32) + routed).astype(jnp.bfloat16)
    return (layer_out, next_state)


def solution(mesh):
    side = math.isqrt(mesh.shape["ep"] // 2)
    grid = Mesh(
        mesh.devices.reshape(side, side, 2, mesh.shape["tp"]), ("z", "y", "c", "tp")
    )
    return jax.shard_map(
        body,
        mesh=grid,
        in_specs=(
            P(EP, None),
            P(EP, "tp", None),
            P(),
            P(EP, "tp"),
            P(EP, "tp"),
            P(EP, "tp"),
            P(),
            P(),
            P("tp"),
            P(),
            P(),
            P("tp"),
            P("tp", EP),
            P(),
            P(EP, None),
            P(EP, None),
            P(EP, None, "tp"),
            P(EP, None, "tp"),
            P(EP, "tp", None),
        ),
        out_specs=(P(EP, "tp"), P(EP, "tp", None)),
        check_vma=False,
    )
```

```python
import functools
import math

import jax
import jax.numpy as jnp
from jax import lax
from jax.experimental import pallas as pl
from jax.experimental.pallas import tpu as pltpu
from jax.sharding import Mesh, PartitionSpec as P

norm_eps = 1e-06
group_eps = 0.00064
EP = ("z", "y", "c")
PLANE = ("y", "c")


def swap(array, axis):
    return lax.all_to_all(array, axis, split_axis=0, concat_axis=0, tiled=True)


def rms_scale(activity, gain):
    widened = activity.astype(jnp.float32)
    scaled = widened * lax.rsqrt(jnp.mean(widened * widened, axis=-1, keepdims=True) + norm_eps)
    return (scaled * gain).astype(jnp.bfloat16)


def low_rank(normed, decay_down, decay_up, decay_base, rate_down, rate_up):
    decay_low = jnp.tanh(jnp.dot(normed, decay_down, preferred_element_type=jnp.float32)).astype(
        jnp.bfloat16
    )
    decay_pre = decay_base + jnp.dot(decay_low, decay_up, preferred_element_type=jnp.float32)
    decays = jnp.exp(-jnp.exp(-jax.nn.softplus(-decay_pre) - 0.5))
    rate_low = jnp.dot(normed, rate_down, preferred_element_type=jnp.float32).astype(jnp.bfloat16)
    rates = jax.nn.sigmoid(jnp.dot(rate_low, rate_up, preferred_element_type=jnp.float32))
    return (decays, rates)


def split_terms(value):
    high = value.astype(jnp.bfloat16)
    return high, (value - high.astype(jnp.float32)).astype(jnp.bfloat16)


def exact_dot(value, chooser):
    high, low = split_terms(value)
    return jnp.dot(high, chooser, preferred_element_type=jnp.float32) + jnp.dot(
        low, chooser, preferred_element_type=jnp.float32
    )


def recurrence_kernel(size, parts, decays, rates, gain, state, new_state, spread_out):
    count, cols = decays.shape
    heads = cols // size
    lines = state.shape[1]
    wide = state.shape[2]
    f32, bf16 = jnp.float32, jnp.bfloat16
    iota = lambda shape, dim: lax.broadcasted_iota(jnp.int32, shape, dim)
    projected = jnp.sum(parts[...].astype(f32), axis=0).astype(bf16).astype(f32)
    queries = projected[:, :cols]
    keys = projected[:, cols : 2 * cols]
    values = projected[:, 2 * cols :]
    square = (cols, cols)
    same_head = iota(square, 0) // size == iota(square, 1) // size
    head_sum = jnp.where(same_head, 1.0, 0.0).astype(f32)
    head_mean = head_sum * (1.0 / size)
    total = lambda x, m: jnp.dot(x, m, precision=lax.Precision.HIGHEST, preferred_element_type=f32)
    units = keys * lax.rsqrt(total(keys * keys, head_sum) + 1.0)
    removal = units * rates[...]

    def by_line(x):
        copies = jnp.broadcast_to(x[:, None, :], (count, 2 * heads, cols))
        chosen = iota(copies.shape, 2) // size == iota(copies.shape, 1) % heads
        kept = jnp.where(chosen, copies, 0.0)
        folded = kept[:, :, :wide]
        for start in range(wide, cols, wide):
            folded = folded + kept[:, :, start : start + wide]
        folded = folded.reshape(count * 2 * heads, wide)
        both = folded + pltpu.roll(folded, size, 1)
        return both.reshape(count, 1, 2 * heads, wide)

    grid_shape = (count, lines // (2 * heads), 2 * heads, wide)
    flat = (count * lines, wide)
    old = state[...].reshape(grid_shape)
    halves = (wide, wide)
    half_sum = jnp.where(iota(halves, 0) // size == iota(halves, 1) // size, 1.0, 0.0).astype(bf16)
    removed = exact_dot((old * by_line(units)).reshape(flat), half_sum).reshape(grid_shape)
    pick = (lines, cols)
    line, col = iota(pick, 0), iota(pick, 1)
    owner = (col // size == line % heads) & ((col % size) // 2 == line // heads)
    value_rows = jnp.where(owner[None], jnp.broadcast_to(values[:, None, :], (count, *pick)), 0.0)
    tall = (cols, wide)
    to_half = jnp.where(iota(tall, 0) % 2 == iota(tall, 1) // size, 1.0, 0.0).astype(bf16)
    value_grid = jnp.dot(
        value_rows.reshape(count * lines, cols).astype(bf16), to_half, preferred_element_type=f32
    ).reshape(grid_shape)
    updated = old * by_line(decays[...]) - removed * by_line(removal) + value_grid * by_line(keys)
    new_state[...] = updated.reshape(new_state.shape)
    broad = (wide, cols)
    from_half = jnp.where(iota(broad, 0) // size == iota(broad, 1) % 2, 1.0, 0.0).astype(bf16)
    reads = exact_dot((updated * by_line(queries)).reshape(flat), from_half)
    readout = jnp.sum(jnp.where(owner[None], reads.reshape(count, *pick), 0.0), axis=1)
    centred = readout - total(readout, head_mean)
    spread = total(centred * centred, head_mean)
    scaled = (centred * lax.rsqrt(spread + group_eps) * gain[...]).astype(bf16)
    spread_out[...] = jnp.broadcast_to(scaled[None], spread_out.shape)


def recurrence(parts, decays, rates, old_state, head_gain):
    layers = parts.shape[0]
    count, cols = decays.shape
    heads, area = old_state.shape[1:]
    size = math.isqrt(area)
    wide = 2 * size
    lines = area // wide
    state = old_state.reshape(count, heads, lines, wide).transpose(0, 2, 1, 3)
    state = state.reshape(count, lines * heads, wide)
    new_state, spread_out = pl.pallas_call(
        functools.partial(recurrence_kernel, size),
        out_shape=(
            jax.ShapeDtypeStruct(state.shape, jnp.float32),
            jax.ShapeDtypeStruct((layers, count, cols), jnp.bfloat16),
        ),
        compiler_params=pltpu.CompilerParams(vmem_limit_bytes=40 << 20),
        name="recurrence",
    )(parts, decays, rates, head_gain.reshape(1, cols), state)
    new_state = new_state.reshape(count, lines, heads, wide).transpose(0, 2, 1, 3)
    return new_state.reshape(old_state.shape), spread_out


def dispatch_kernel(slots, lane, parts, tokens, gain, outbound, kept, residual, lines, rows):
    layers, lanes, count, block = parts.shape
    wide = lines.shape[2]
    f32 = jnp.float32
    squares = jnp.zeros((count, 1), f32)
    for z in range(layers):
        mixed = parts[z, 0].astype(f32)
        for part in range(1, lanes):
            mixed = mixed + parts[z, part].astype(f32)
        here = tokens[:, z * block : (z + 1) * block].astype(f32)
        residual[z] = (here + mixed).astype(jnp.bfloat16).astype(f32)
        squares = squares + jnp.sum(residual[z] * residual[z], axis=1, keepdims=True)
    scale = lax.rsqrt(squares / (layers * block) + norm_eps)
    for z in range(layers):
        normed = residual[z] * scale * gain[:, z * block : (z + 1) * block]
        for piece in range(block // wide):
            lines[:count, z * (block // wide) + piece, :] = normed[:, piece * wide : (piece + 1) * wide]
    lines[count] = jnp.zeros(lines.shape[1:], f32)
    rows[...] = lines[...].astype(jnp.bfloat16)

    def send(step, carry):
        outbound[step] = rows[slots[step]]
        return carry

    lax.fori_loop(0, outbound.shape[0], send, 0, unroll=8)
    own = layers // lanes
    for piece in range(own):
        kept[:, piece * block : (piece + 1) * block] = residual[lane[0] * own + piece]


def dispatch(parts, tokens, gain, slots, lane):
    layers, lanes, count, block = parts.shape
    width = layers * block
    wide = 128
    pieces = width // wide
    vmem = pl.BlockSpec(memory_space=pltpu.VMEM)
    smem = pl.BlockSpec(memory_space=pltpu.SMEM)
    return pl.pallas_call(
        dispatch_kernel,
        in_specs=[smem, smem, vmem, vmem, vmem],
        out_specs=(vmem, vmem),
        out_shape=(
            jax.ShapeDtypeStruct((slots.shape[0], pieces, wide), jnp.bfloat16),
            jax.ShapeDtypeStruct((count, width // lanes), jnp.float32),
        ),
        scratch_shapes=[
            pltpu.VMEM((layers, count, block), jnp.float32),
            pltpu.VMEM((count + 1, pieces, wide), jnp.float32),
            pltpu.VMEM((count + 1, pieces, wide), jnp.bfloat16),
        ],
        compiler_params=pltpu.CompilerParams(vmem_limit_bytes=20 << 20),
        name="dispatch",
    )(slots, lane.reshape(1), parts, tokens, gain.reshape(1, width))


def expert_kernel(rows, gate, up, down, result, lines):
    _, pieces, wide = rows.shape
    lanes, _, quarter = result.shape
    f32 = jnp.float32
    lines[...] = rows[...].astype(f32)
    gate_act = up_act = 0.0
    for piece in range(0, pieces, 2):
        here = slice(piece * wide, (piece + 2) * wide)
        both = jnp.concatenate([lines[:, piece, :], lines[:, piece + 1, :]], axis=1)
        both = both.astype(jnp.bfloat16)
        gate_act = gate_act + jnp.dot(both, gate[here], preferred_element_type=f32)
        up_act = up_act + jnp.dot(both, up[here], preferred_element_type=f32)
    hidden = (gate_act / (1.0 + jnp.exp(-gate_act)) * up_act).astype(jnp.bfloat16)
    for part in range(lanes):
        here = slice(part * quarter, (part + 1) * quarter)
        product = jnp.dot(hidden, down[:, here], preferred_element_type=f32)
        result[part] = product.astype(jnp.bfloat16)


def expert_rows(rows, gate, up, down, lanes):
    return pl.pallas_call(
        expert_kernel,
        out_shape=jax.ShapeDtypeStruct(
            (lanes, rows.shape[0], down.shape[1] // lanes), jnp.bfloat16
        ),
        scratch_shapes=[pltpu.VMEM(rows.shape, jnp.float32)],
        compiler_params=pltpu.CompilerParams(vmem_limit_bytes=20 << 20),
        name="expert",
    )(rows, gate, up, down)


def body(
    tokens,
    head_state,
    mixer_gain,
    w_query,
    w_key,
    w_value,
    decay_down,
    decay_up,
    decay_base,
    rate_down,
    rate_up,
    head_gain,
    w_out,
    expert_gain,
    expert_ids,
    route_weight,
    w_gate,
    w_up,
    w_down,
):
    rows, width = tokens.shape
    cols = w_query.shape[1]
    layers = lax.axis_size("z")
    lanes = lax.axis_size("tp")
    experts = lax.axis_size(EP)
    lane = lax.axis_index("tp")
    block = width // layers
    quarter = width // lanes

    weights = lax.all_gather(
        jnp.concatenate([w_query, w_key, w_value, w_out.T], axis=1), PLANE, axis=0, tiled=True
    )
    normed = rms_scale(tokens, mixer_gain)
    spread_rows = swap(normed.reshape(rows, layers, block).transpose(1, 0, 2), "z")
    partial_rows = jnp.dot(
        spread_rows.reshape(layers * rows, block),
        weights[:, : 3 * cols],
        preferred_element_type=jnp.float32,
    ).astype(jnp.bfloat16)
    summed = swap(partial_rows.reshape(layers, rows, 3 * cols), "z")
    decays, rates = low_rank(
        normed,
        decay_down,
        lax.dynamic_slice_in_dim(decay_up, lane * cols, cols, 1),
        decay_base,
        rate_down,
        lax.dynamic_slice_in_dim(rate_up, lane * cols, cols, 1),
    )
    next_state, spread_out = recurrence(summed, decays, rates, head_state, head_gain)
    heads_here = swap(spread_out, "z").reshape(layers * rows, cols)
    partial_out = lax.dot_general(
        heads_here,
        weights[:, 3 * cols :],
        (((1,), (1,)), ((), ())),
        preferred_element_type=jnp.float32,
    ).astype(jnp.bfloat16)
    home_out = swap(
        jnp.broadcast_to(
            partial_out.reshape(layers, 1, rows, block), (layers, lanes, rows, block)
        ).reshape(layers * lanes, rows, block),
        ("z", "tp"),
    ).reshape(layers, lanes, rows, block)
    match = expert_ids[:, :, None] == jnp.arange(experts, dtype=jnp.int32)[None, None, :]
    order = jnp.arange(rows, dtype=jnp.int32)[:, None, None]
    slots = jnp.min(jnp.where(match, order, rows), axis=(0, 1))
    outbound, residual = dispatch(home_out, tokens, expert_gain, slots, lane)
    arrived = swap(outbound, EP)
    expert_parts = expert_rows(arrived, w_gate[0], w_up[0], w_down[0], lanes)
    gathered = swap(expert_parts, "tp")
    reduced = jnp.sum(gathered.astype(jnp.float32), axis=0).astype(jnp.bfloat16)
    returned = swap(reduced.reshape(experts, 1, quarter), EP).reshape(experts, quarter)
    shares = route_weight / jnp.sum(route_weight, axis=1, keepdims=True)
    combine = jnp.sum(match.astype(jnp.float32) * shares[:, :, None], axis=1)
    routed = jnp.dot(combine, returned.astype(jnp.float32))
    layer_out = (residual + routed).astype(jnp.bfloat16)
    return (layer_out, next_state)


def solution(mesh):
    side = math.isqrt(mesh.shape["ep"] // 2)
    grid = Mesh(
        mesh.devices.reshape(side, side, 2, mesh.shape["tp"]), ("z", "y", "c", "tp")
    )
    return jax.shard_map(
        body,
        mesh=grid,
        in_specs=(
            P(EP, None),
            P(EP, "tp", None),
            P(),
            P(EP, "tp"),
            P(EP, "tp"),
            P(EP, "tp"),
            P(),
            P(),
            P("tp"),
            P(),
            P(),
            P("tp"),
            P("tp", EP),
            P(),
            P(EP, None),
            P(EP, None),
            P(EP, None, "tp"),
            P(EP, None, "tp"),
            P(EP, "tp", None),
        ),
        out_specs=(P(EP, "tp"), P(EP, "tp", None)),
        check_vma=False,
    )
```

```python
import functools
import math

import jax
import jax.numpy as jnp
from jax import lax
from jax.experimental import pallas as pl
from jax.experimental.pallas import tpu as pltpu
from jax.sharding import Mesh, PartitionSpec as P

norm_eps = 1e-06
group_eps = 0.00064
EP = ("z", "y", "c")


def swap(array, axis):
    return lax.all_to_all(array, axis, split_axis=0, concat_axis=0, tiled=True)


def low_rank(normed, decay_down, decay_up, decay_base, rate_down, rate_up):
    decay_low = jnp.tanh(jnp.dot(normed, decay_down, preferred_element_type=jnp.float32)).astype(
        jnp.bfloat16
    )
    decay_pre = decay_base + jnp.dot(decay_low, decay_up, preferred_element_type=jnp.float32)
    decays = jnp.exp(-jnp.exp(-jax.nn.softplus(-decay_pre) - 0.5))
    rate_low = jnp.dot(normed, rate_down, preferred_element_type=jnp.float32).astype(jnp.bfloat16)
    rates = jax.nn.sigmoid(jnp.dot(rate_low, rate_up, preferred_element_type=jnp.float32))
    return (decays, rates)


def split_terms(value):
    high = value.astype(jnp.bfloat16)
    return high, (value - high.astype(jnp.float32)).astype(jnp.bfloat16)


def exact_dot(value, chooser):
    high, low = split_terms(value)
    return jnp.dot(high, chooser, preferred_element_type=jnp.float32) + jnp.dot(
        low, chooser, preferred_element_type=jnp.float32
    )


def prepare_kernel(tokens, gain, query, key, value, out, rows, normed, weights):
    layers, _, block = rows.shape
    f32 = jnp.float32
    widened = tokens[...].astype(f32)
    scale = lax.rsqrt(jnp.mean(widened * widened, axis=1, keepdims=True) + norm_eps)
    scaled = (widened * scale * gain[...]).astype(jnp.bfloat16)
    normed[...] = scaled
    for z in range(layers):
        rows[z] = scaled[:, z * block : (z + 1) * block]
    joined = jnp.concatenate([query[...], key[...], value[...], out[...]], axis=1)
    for y in range(weights.shape[0]):
        weights[y] = joined


def prepare(tokens, gain, pieces, layers, peers):
    count, width = tokens.shape
    bf16 = jnp.bfloat16
    total = sum(piece.shape[1] for piece in pieces)
    return pl.pallas_call(
        prepare_kernel,
        out_shape=(
            jax.ShapeDtypeStruct((layers, count, width // layers), bf16),
            jax.ShapeDtypeStruct((count, width), bf16),
            jax.ShapeDtypeStruct((peers, pieces[0].shape[0], total), bf16),
        ),
        compiler_params=pltpu.CompilerParams(vmem_limit_bytes=20 << 20),
        name="prepare",
    )(tokens, gain.reshape(1, width), *pieces)


def project_kernel(rows, weights, result, whole):
    cores, peers, depth, _ = weights.shape
    layers, count, cols = result.shape
    for y in range(peers):
        for c in range(cores):
            start = (y * cores + c) * depth
            whole[start : start + depth, :] = weights[c, y, :, :cols]
    product = jnp.dot(
        rows[...].reshape(layers * count, rows.shape[2]),
        whole[...],
        preferred_element_type=jnp.float32,
    )
    result[...] = product.astype(jnp.bfloat16).reshape(result.shape)


def project(rows, weights, cols):
    layers, count, block = rows.shape
    return pl.pallas_call(
        project_kernel,
        out_shape=jax.ShapeDtypeStruct((layers, count, cols), jnp.bfloat16),
        scratch_shapes=[pltpu.VMEM((block, cols), jnp.bfloat16)],
        compiler_params=pltpu.CompilerParams(vmem_limit_bytes=20 << 20),
        name="project",
    )(rows, weights)


def output_kernel(heads, weights, result, whole):
    cores, peers, depth, total = weights.shape
    layers, lanes, count, block = result.shape
    cols = heads.shape[2]
    for y in range(peers):
        for c in range(cores):
            start = (y * cores + c) * depth
            whole[start : start + depth, :] = weights[c, y, :, total - cols :]
    product = lax.dot_general(
        heads[...].reshape(layers * count, cols),
        whole[...],
        (((1,), (1,)), ((), ())),
        preferred_element_type=jnp.float32,
    )
    product = product.astype(jnp.bfloat16).reshape(layers, 1, count, block)
    result[...] = jnp.broadcast_to(product, result.shape)


def output(heads, weights, lanes, block):
    layers, count, cols = heads.shape
    return pl.pallas_call(
        output_kernel,
        out_shape=jax.ShapeDtypeStruct((layers, lanes, count, block), jnp.bfloat16),
        scratch_shapes=[pltpu.VMEM((block, cols), jnp.bfloat16)],
        compiler_params=pltpu.CompilerParams(vmem_limit_bytes=20 << 20),
        name="output",
    )(heads, weights)


def recurrence_kernel(size, parts, decays, rates, gain, state, new_state, spread_out):
    count, cols = decays.shape
    heads = cols // size
    lines = state.shape[1]
    wide = state.shape[2]
    f32, bf16 = jnp.float32, jnp.bfloat16
    iota = lambda shape, dim: lax.broadcasted_iota(jnp.int32, shape, dim)
    projected = jnp.sum(parts[...].astype(f32), axis=0).astype(bf16).astype(f32)
    queries = projected[:, :cols]
    keys = projected[:, cols : 2 * cols]
    values = projected[:, 2 * cols :]
    square = (cols, cols)
    same_head = iota(square, 0) // size == iota(square, 1) // size
    head_sum = jnp.where(same_head, 1.0, 0.0).astype(f32)
    head_mean = head_sum * (1.0 / size)
    total = lambda x, m: jnp.dot(x, m, precision=lax.Precision.HIGHEST, preferred_element_type=f32)
    units = keys * lax.rsqrt(total(keys * keys, head_sum) + 1.0)
    removal = units * rates[...]

    def by_line(x):
        copies = jnp.broadcast_to(x[:, None, :], (count, 2 * heads, cols))
        chosen = iota(copies.shape, 2) // size == iota(copies.shape, 1) % heads
        kept = jnp.where(chosen, copies, 0.0)
        folded = kept[:, :, :wide]
        for start in range(wide, cols, wide):
            folded = folded + kept[:, :, start : start + wide]
        folded = folded.reshape(count * 2 * heads, wide)
        both = folded + pltpu.roll(folded, size, 1)
        return both.reshape(count, 1, 2 * heads, wide)

    grid_shape = (count, lines // (2 * heads), 2 * heads, wide)
    flat = (count * lines, wide)
    old = state[...].reshape(grid_shape)
    halves = (wide, wide)
    half_sum = jnp.where(iota(halves, 0) // size == iota(halves, 1) // size, 1.0, 0.0).astype(bf16)
    removed = exact_dot((old * by_line(units)).reshape(flat), half_sum).reshape(grid_shape)
    pick = (lines, cols)
    line, col = iota(pick, 0), iota(pick, 1)
    owner = (col // size == line % heads) & ((col % size) // 2 == line // heads)
    value_rows = jnp.where(owner[None], jnp.broadcast_to(values[:, None, :], (count, *pick)), 0.0)
    tall = (cols, wide)
    to_half = jnp.where(iota(tall, 0) % 2 == iota(tall, 1) // size, 1.0, 0.0).astype(bf16)
    value_grid = jnp.dot(
        value_rows.reshape(count * lines, cols).astype(bf16), to_half, preferred_element_type=f32
    ).reshape(grid_shape)
    updated = old * by_line(decays[...]) - removed * by_line(removal) + value_grid * by_line(keys)
    new_state[...] = updated.reshape(new_state.shape)
    broad = (wide, cols)
    from_half = jnp.where(iota(broad, 0) // size == iota(broad, 1) % 2, 1.0, 0.0).astype(bf16)
    reads = exact_dot((updated * by_line(queries)).reshape(flat), from_half)
    readout = jnp.sum(jnp.where(owner[None], reads.reshape(count, *pick), 0.0), axis=1)
    centred = readout - total(readout, head_mean)
    spread = total(centred * centred, head_mean)
    scaled = (centred * lax.rsqrt(spread + group_eps) * gain[...]).astype(bf16)
    spread_out[...] = jnp.broadcast_to(scaled[None], spread_out.shape)


def recurrence(parts, decays, rates, old_state, head_gain):
    layers = parts.shape[0]
    count, cols = decays.shape
    heads, area = old_state.shape[1:]
    size = math.isqrt(area)
    wide = 2 * size
    lines = area // wide
    state = old_state.reshape(count, heads, lines, wide).transpose(0, 2, 1, 3)
    state = state.reshape(count, lines * heads, wide)
    new_state, spread_out = pl.pallas_call(
        functools.partial(recurrence_kernel, size),
        out_shape=(
            jax.ShapeDtypeStruct(state.shape, jnp.float32),
            jax.ShapeDtypeStruct((layers, count, cols), jnp.bfloat16),
        ),
        compiler_params=pltpu.CompilerParams(vmem_limit_bytes=40 << 20),
        name="recurrence",
    )(parts, decays, rates, head_gain.reshape(1, cols), state)
    new_state = new_state.reshape(count, lines, heads, wide).transpose(0, 2, 1, 3)
    return new_state.reshape(old_state.shape), spread_out


def dispatch_kernel(slots, lane, parts, tokens, gain, outbound, kept, residual, lines, rows):
    layers, lanes, count, block = parts.shape
    wide = lines.shape[2]
    f32 = jnp.float32
    squares = jnp.zeros((count, 1), f32)
    for z in range(layers):
        mixed = parts[z, 0].astype(f32)
        for part in range(1, lanes):
            mixed = mixed + parts[z, part].astype(f32)
        here = tokens[:, z * block : (z + 1) * block].astype(f32)
        residual[z] = (here + mixed).astype(jnp.bfloat16).astype(f32)
        squares = squares + jnp.sum(residual[z] * residual[z], axis=1, keepdims=True)
    scale = lax.rsqrt(squares / (layers * block) + norm_eps)
    for z in range(layers):
        normed = residual[z] * scale * gain[:, z * block : (z + 1) * block]
        for piece in range(block // wide):
            lines[:count, z * (block // wide) + piece, :] = normed[:, piece * wide : (piece + 1) * wide]
    lines[count] = jnp.zeros(lines.shape[1:], f32)
    rows[...] = lines[...].astype(jnp.bfloat16)

    def send(step, carry):
        outbound[step] = rows[slots[step]]
        return carry

    lax.fori_loop(0, outbound.shape[0], send, 0, unroll=8)
    own = layers // lanes
    for piece in range(own):
        kept[:, piece * block : (piece + 1) * block] = residual[lane[0] * own + piece]


def dispatch(parts, tokens, gain, slots, lane):
    layers, lanes, count, block = parts.shape
    width = layers * block
    wide = 128
    pieces = width // wide
    vmem = pl.BlockSpec(memory_space=pltpu.VMEM)
    smem = pl.BlockSpec(memory_space=pltpu.SMEM)
    return pl.pallas_call(
        dispatch_kernel,
        in_specs=[smem, smem, vmem, vmem, vmem],
        out_specs=(vmem, vmem),
        out_shape=(
            jax.ShapeDtypeStruct((slots.shape[0], pieces, wide), jnp.bfloat16),
            jax.ShapeDtypeStruct((count, width // lanes), jnp.float32),
        ),
        scratch_shapes=[
            pltpu.VMEM((layers, count, block), jnp.float32),
            pltpu.VMEM((count + 1, pieces, wide), jnp.float32),
            pltpu.VMEM((count + 1, pieces, wide), jnp.bfloat16),
        ],
        compiler_params=pltpu.CompilerParams(vmem_limit_bytes=20 << 20),
        name="dispatch",
    )(slots, lane.reshape(1), parts, tokens, gain.reshape(1, width))


def expert_kernel(rows, gate, up, down, result, lines):
    _, pieces, wide = rows.shape
    lanes, _, quarter = result.shape
    f32 = jnp.float32
    lines[...] = rows[...].astype(f32)
    gate_act = up_act = 0.0
    for piece in range(0, pieces, 2):
        here = slice(piece * wide, (piece + 2) * wide)
        both = jnp.concatenate([lines[:, piece, :], lines[:, piece + 1, :]], axis=1)
        both = both.astype(jnp.bfloat16)
        gate_act = gate_act + jnp.dot(both, gate[here], preferred_element_type=f32)
        up_act = up_act + jnp.dot(both, up[here], preferred_element_type=f32)
    hidden = (gate_act / (1.0 + jnp.exp(-gate_act)) * up_act).astype(jnp.bfloat16)
    for part in range(lanes):
        here = slice(part * quarter, (part + 1) * quarter)
        product = jnp.dot(hidden, down[:, here], preferred_element_type=f32)
        result[part] = product.astype(jnp.bfloat16)


def expert_rows(rows, gate, up, down, lanes):
    return pl.pallas_call(
        expert_kernel,
        out_shape=jax.ShapeDtypeStruct(
            (lanes, rows.shape[0], down.shape[1] // lanes), jnp.bfloat16
        ),
        scratch_shapes=[pltpu.VMEM(rows.shape, jnp.float32)],
        compiler_params=pltpu.CompilerParams(vmem_limit_bytes=20 << 20),
        name="expert",
    )(rows, gate, up, down)


def body(
    tokens,
    head_state,
    mixer_gain,
    w_query,
    w_key,
    w_value,
    decay_down,
    decay_up,
    decay_base,
    rate_down,
    rate_up,
    head_gain,
    w_out,
    expert_gain,
    expert_ids,
    route_weight,
    w_gate,
    w_up,
    w_down,
):
    rows, width = tokens.shape
    cols = w_query.shape[1]
    layers = lax.axis_size("z")
    lanes = lax.axis_size("tp")
    experts = lax.axis_size(EP)
    lane = lax.axis_index("tp")
    block = width // layers
    quarter = width // lanes

    spread_rows, normed, own_weights = prepare(
        tokens, mixer_gain, (w_query, w_key, w_value, w_out.T), layers, lax.axis_size("y")
    )
    own_weights = swap(own_weights, "y")
    spread_rows = swap(spread_rows, "z")
    weights = lax.all_gather(own_weights, "c", axis=0)
    summed = swap(project(spread_rows, weights, 3 * cols), "z")
    decays, rates = low_rank(
        normed,
        decay_down,
        lax.dynamic_slice_in_dim(decay_up, lane * cols, cols, 1),
        decay_base,
        rate_down,
        lax.dynamic_slice_in_dim(rate_up, lane * cols, cols, 1),
    )
    next_state, spread_out = recurrence(summed, decays, rates, head_state, head_gain)
    partial_out = output(swap(spread_out, "z"), weights, lanes, block)
    home_out = swap(partial_out.reshape(layers * lanes, rows, block), ("z", "tp"))
    home_out = home_out.reshape(layers, lanes, rows, block)
    match = expert_ids[:, :, None] == jnp.arange(experts, dtype=jnp.int32)[None, None, :]
    order = jnp.arange(rows, dtype=jnp.int32)[:, None, None]
    slots = jnp.min(jnp.where(match, order, rows), axis=(0, 1))
    outbound, residual = dispatch(home_out, tokens, expert_gain, slots, lane)
    arrived = swap(outbound, EP)
    expert_parts = expert_rows(arrived, w_gate[0], w_up[0], w_down[0], lanes)
    gathered = swap(expert_parts, "tp")
    reduced = jnp.sum(gathered.astype(jnp.float32), axis=0).astype(jnp.bfloat16)
    returned = swap(reduced.reshape(experts, 1, quarter), EP).reshape(experts, quarter)
    shares = route_weight / jnp.sum(route_weight, axis=1, keepdims=True)
    combine = jnp.sum(match.astype(jnp.float32) * shares[:, :, None], axis=1)
    routed = jnp.dot(combine, returned.astype(jnp.float32))
    layer_out = (residual + routed).astype(jnp.bfloat16)
    return (layer_out, next_state)


def solution(mesh):
    side = math.isqrt(mesh.shape["ep"] // 2)
    grid = Mesh(
        mesh.devices.reshape(side, side, 2, mesh.shape["tp"]), ("z", "y", "c", "tp")
    )
    return jax.shard_map(
        body,
        mesh=grid,
        in_specs=(
            P(EP, None),
            P(EP, "tp", None),
            P(),
            P(EP, "tp"),
            P(EP, "tp"),
            P(EP, "tp"),
            P(),
            P(),
            P("tp"),
            P(),
            P(),
            P("tp"),
            P("tp", EP),
            P(),
            P(EP, None),
            P(EP, None),
            P(EP, None, "tp"),
            P(EP, None, "tp"),
            P(EP, "tp", None),
        ),
        out_specs=(P(EP, "tp"), P(EP, "tp", None)),
        check_vma=False,
    )
```

```python
import functools
import math

import jax
import jax.numpy as jnp
from jax import lax
from jax.experimental import pallas as pl
from jax.experimental.pallas import tpu as pltpu
from jax.sharding import Mesh, PartitionSpec as P

norm_eps = 1e-06
group_eps = 0.00064
EP = ("z", "y", "c")
PLANE = ("y", "c")


def swap(array, axis):
    return lax.all_to_all(array, axis, split_axis=0, concat_axis=0, tiled=True)


def norm_kernel(tokens, gain, rows, normed):
    layers, _, block = rows.shape
    f32 = jnp.float32
    widened = tokens[...].astype(f32)
    scale = lax.rsqrt(jnp.mean(widened * widened, axis=1, keepdims=True) + norm_eps)
    scaled = (widened * scale * gain[...]).astype(jnp.bfloat16)
    normed[...] = scaled
    for z in range(layers):
        rows[z] = scaled[:, z * block : (z + 1) * block]


def norm(tokens, gain, layers):
    count, width = tokens.shape
    bf16 = jnp.bfloat16
    return pl.pallas_call(
        norm_kernel,
        out_shape=(
            jax.ShapeDtypeStruct((layers, count, width // layers), bf16),
            jax.ShapeDtypeStruct((count, width), bf16),
        ),
        compiler_params=pltpu.CompilerParams(vmem_limit_bytes=20 << 20),
        name="norm",
    )(tokens, gain.reshape(1, width))


def low_rank_kernel(lane, normed, down, up, base, rate_down, rate_up, gain, result):
    f32, bf16 = jnp.float32, jnp.bfloat16
    _, count, cols = result.shape
    own = pl.ds(pl.multiple_of(lane[0] * cols, cols), cols)
    rows = normed[...]
    across = lambda w: lax.dot_general(
        rows, w[...], (((1,), (1,)), ((), ())), preferred_element_type=f32
    )
    decay_low = jnp.tanh(across(down)).astype(bf16)
    decay_pre = base[...] + jnp.dot(decay_low, up[:, own], preferred_element_type=f32)
    softplus = jnp.maximum(-decay_pre, 0.0) + jnp.log1p(jnp.exp(-jnp.abs(decay_pre)))
    result[0] = jnp.exp(-jnp.exp(-softplus - 0.5))
    rate_low = across(rate_down).astype(bf16)
    rate_pre = jnp.dot(rate_low, rate_up[:, own], preferred_element_type=f32)
    result[1] = 1.0 / (1.0 + jnp.exp(-rate_pre))
    result[2] = jnp.broadcast_to(gain[...], (count, cols))


def low_rank(normed, decay_down, decay_up, decay_base, rate_down, rate_up, head_gain, lane):
    cols = decay_base.shape[0]
    vmem = pl.BlockSpec(memory_space=pltpu.VMEM)
    return pl.pallas_call(
        low_rank_kernel,
        in_specs=[pl.BlockSpec(memory_space=pltpu.SMEM)] + [vmem] * 7,
        out_specs=vmem,
        out_shape=jax.ShapeDtypeStruct((3, normed.shape[0], cols), jnp.float32),
        compiler_params=pltpu.CompilerParams(vmem_limit_bytes=20 << 20),
        name="low_rank",
    )(
        lane.reshape(1),
        normed,
        decay_down.T,
        decay_up,
        decay_base.reshape(1, cols),
        rate_down.T,
        rate_up,
        head_gain.reshape(1, cols),
    )


def split_terms(value):
    high = value.astype(jnp.bfloat16)
    return high, (value - high.astype(jnp.float32)).astype(jnp.bfloat16)


def exact_dot(value, chooser):
    high, low = split_terms(value)
    return jnp.dot(high, chooser, preferred_element_type=jnp.float32) + jnp.dot(
        low, chooser, preferred_element_type=jnp.float32
    )


def recurrence_kernel(size, parts, factors, state, new_state, spread_out):
    decays, rates, gain = factors[0], factors[1], factors[2]
    count, cols = decays.shape
    heads = cols // size
    lines = state.shape[1]
    wide = state.shape[2]
    f32, bf16 = jnp.float32, jnp.bfloat16
    iota = lambda shape, dim: lax.broadcasted_iota(jnp.int32, shape, dim)
    projected = jnp.sum(parts[...].astype(f32), axis=0).astype(bf16).astype(f32)
    queries = projected[:, :cols]
    keys = projected[:, cols : 2 * cols]
    values = projected[:, 2 * cols :]
    square = (cols, cols)
    same_head = iota(square, 0) // size == iota(square, 1) // size
    head_sum = jnp.where(same_head, 1.0, 0.0).astype(f32)
    head_mean = head_sum * (1.0 / size)
    total = lambda x, m: jnp.dot(x, m, precision=lax.Precision.HIGHEST, preferred_element_type=f32)
    units = keys * lax.rsqrt(total(keys * keys, head_sum) + 1.0)
    removal = units * rates

    def by_line(x):
        copies = jnp.broadcast_to(x[:, None, :], (count, 2 * heads, cols))
        chosen = iota(copies.shape, 2) // size == iota(copies.shape, 1) % heads
        kept = jnp.where(chosen, copies, 0.0)
        folded = kept[:, :, :wide]
        for start in range(wide, cols, wide):
            folded = folded + kept[:, :, start : start + wide]
        folded = folded.reshape(count * 2 * heads, wide)
        both = folded + pltpu.roll(folded, size, 1)
        return both.reshape(count, 1, 2 * heads, wide)

    grid_shape = (count, lines // (2 * heads), 2 * heads, wide)
    flat = (count * lines, wide)
    old = state[...].reshape(grid_shape)
    halves = (wide, wide)
    half_sum = jnp.where(iota(halves, 0) // size == iota(halves, 1) // size, 1.0, 0.0).astype(bf16)
    removed = exact_dot((old * by_line(units)).reshape(flat), half_sum).reshape(grid_shape)
    pick = (lines, cols)
    line, col = iota(pick, 0), iota(pick, 1)
    owner = (col // size == line % heads) & ((col % size) // 2 == line // heads)
    value_rows = jnp.where(owner[None], jnp.broadcast_to(values[:, None, :], (count, *pick)), 0.0)
    tall = (cols, wide)
    to_half = jnp.where(iota(tall, 0) % 2 == iota(tall, 1) // size, 1.0, 0.0).astype(bf16)
    value_grid = jnp.dot(
        value_rows.reshape(count * lines, cols).astype(bf16), to_half, preferred_element_type=f32
    ).reshape(grid_shape)
    updated = old * by_line(decays) - removed * by_line(removal) + value_grid * by_line(keys)
    new_state[...] = updated.reshape(new_state.shape)
    broad = (wide, cols)
    from_half = jnp.where(iota(broad, 0) // size == iota(broad, 1) % 2, 1.0, 0.0).astype(bf16)
    reads = exact_dot((updated * by_line(queries)).reshape(flat), from_half)
    readout = jnp.sum(jnp.where(owner[None], reads.reshape(count, *pick), 0.0), axis=1)
    centred = readout - total(readout, head_mean)
    spread = total(centred * centred, head_mean)
    scaled = (centred * lax.rsqrt(spread + group_eps) * gain).astype(bf16)
    spread_out[...] = jnp.broadcast_to(scaled[None], spread_out.shape)


def recurrence(parts, factors, old_state):
    layers = parts.shape[0]
    _, count, cols = factors.shape
    heads, area = old_state.shape[1:]
    size = math.isqrt(area)
    wide = 2 * size
    lines = area // wide
    state = old_state.reshape(count, heads, lines, wide).transpose(0, 2, 1, 3)
    state = state.reshape(count, lines * heads, wide)
    new_state, spread_out = pl.pallas_call(
        functools.partial(recurrence_kernel, size),
        out_shape=(
            jax.ShapeDtypeStruct(state.shape, jnp.float32),
            jax.ShapeDtypeStruct((layers, count, cols), jnp.bfloat16),
        ),
        compiler_params=pltpu.CompilerParams(vmem_limit_bytes=40 << 20),
        name="recurrence",
    )(parts, factors, state)
    new_state = new_state.reshape(count, lines, heads, wide).transpose(0, 2, 1, 3)
    return new_state.reshape(old_state.shape), spread_out


def output_kernel(heads, weights, result):
    layers, lanes, count, block = result.shape
    cols = heads.shape[2]
    product = lax.dot_general(
        heads[...].reshape(layers * count, cols),
        weights[:, weights.shape[1] - cols :],
        (((1,), (1,)), ((), ())),
        preferred_element_type=jnp.float32,
    )
    product = product.astype(jnp.bfloat16).reshape(layers, 1, count, block)
    result[...] = jnp.broadcast_to(product, result.shape)


def output(heads, weights, lanes):
    layers, count, _ = heads.shape
    shape = (layers, lanes, count, weights.shape[0])
    return pl.pallas_call(
        output_kernel,
        out_shape=jax.ShapeDtypeStruct(shape, jnp.bfloat16),
        compiler_params=pltpu.CompilerParams(vmem_limit_bytes=20 << 20),
        name="output",
    )(heads, weights)


def dispatch_kernel(slots, lane, parts, tokens, gain, outbound, kept, residual, lines, rows):
    layers, lanes, count, block = parts.shape
    wide = lines.shape[2]
    f32 = jnp.float32
    squares = jnp.zeros((count, 1), f32)
    for z in range(layers):
        mixed = parts[z, 0].astype(f32)
        for part in range(1, lanes):
            mixed = mixed + parts[z, part].astype(f32)
        here = tokens[:, z * block : (z + 1) * block].astype(f32)
        residual[z] = (here + mixed).astype(jnp.bfloat16).astype(f32)
        squares = squares + jnp.sum(residual[z] * residual[z], axis=1, keepdims=True)
    scale = lax.rsqrt(squares / (layers * block) + norm_eps)
    for z in range(layers):
        normed = residual[z] * scale * gain[:, z * block : (z + 1) * block]
        for piece in range(block // wide):
            lines[:count, z * (block // wide) + piece, :] = normed[:, piece * wide : (piece + 1) * wide]
    lines[count] = jnp.zeros(lines.shape[1:], f32)
    rows[...] = lines[...].astype(jnp.bfloat16)

    def send(step, carry):
        outbound[step] = rows[slots[step]]
        return carry

    lax.fori_loop(0, outbound.shape[0], send, 0, unroll=8)
    own = layers // lanes
    for piece in range(own):
        kept[:, piece * block : (piece + 1) * block] = residual[lane[0] * own + piece]


def dispatch(parts, tokens, gain, slots, lane):
    layers, lanes, count, block = parts.shape
    width = layers * block
    wide = 128
    pieces = width // wide
    vmem = pl.BlockSpec(memory_space=pltpu.VMEM)
    smem = pl.BlockSpec(memory_space=pltpu.SMEM)
    return pl.pallas_call(
        dispatch_kernel,
        in_specs=[smem, smem, vmem, vmem, vmem],
        out_specs=(vmem, vmem),
        out_shape=(
            jax.ShapeDtypeStruct((slots.shape[0], pieces, wide), jnp.bfloat16),
            jax.ShapeDtypeStruct((count, width // lanes), jnp.float32),
        ),
        scratch_shapes=[
            pltpu.VMEM((layers, count, block), jnp.float32),
            pltpu.VMEM((count + 1, pieces, wide), jnp.float32),
            pltpu.VMEM((count + 1, pieces, wide), jnp.bfloat16),
        ],
        compiler_params=pltpu.CompilerParams(vmem_limit_bytes=20 << 20),
        name="dispatch",
    )(slots, lane.reshape(1), parts, tokens, gain.reshape(1, width))


def expert_kernel(rows, gate, up, down, result, lines):
    _, pieces, wide = rows.shape
    lanes, _, quarter = result.shape
    f32 = jnp.float32
    lines[...] = rows[...].astype(f32)
    gate_act = up_act = 0.0
    for piece in range(0, pieces, 2):
        here = slice(piece * wide, (piece + 2) * wide)
        both = jnp.concatenate([lines[:, piece, :], lines[:, piece + 1, :]], axis=1)
        both = both.astype(jnp.bfloat16)
        gate_act = gate_act + jnp.dot(both, gate[here], preferred_element_type=f32)
        up_act = up_act + jnp.dot(both, up[here], preferred_element_type=f32)
    hidden = (gate_act / (1.0 + jnp.exp(-gate_act)) * up_act).astype(jnp.bfloat16)
    for part in range(lanes):
        here = slice(part * quarter, (part + 1) * quarter)
        product = jnp.dot(hidden, down[:, here], preferred_element_type=f32)
        result[part] = product.astype(jnp.bfloat16)


def expert_rows(rows, gate, up, down, lanes):
    return pl.pallas_call(
        expert_kernel,
        out_shape=jax.ShapeDtypeStruct(
            (lanes, rows.shape[0], down.shape[1] // lanes), jnp.bfloat16
        ),
        scratch_shapes=[pltpu.VMEM(rows.shape, jnp.float32)],
        compiler_params=pltpu.CompilerParams(vmem_limit_bytes=20 << 20),
        name="expert",
    )(rows, gate, up, down)


def settle_kernel(parts, result, lines):
    lanes, _, quarter = parts.shape
    pieces, wide = lines.shape[1:]
    total = parts[0].astype(jnp.float32)
    for part in range(1, lanes):
        total = total + parts[part].astype(jnp.float32)
    for piece in range(pieces):
        lines[:, piece, :] = total[:, piece * wide : (piece + 1) * wide]
    result[...] = lines[...].astype(jnp.bfloat16)


def settle(parts):
    _, count, quarter = parts.shape
    shape = (count, quarter // 128, 128)
    return pl.pallas_call(
        settle_kernel,
        out_shape=jax.ShapeDtypeStruct(shape, jnp.bfloat16),
        scratch_shapes=[pltpu.VMEM(shape, jnp.float32)],
        compiler_params=pltpu.CompilerParams(vmem_limit_bytes=20 << 20),
        name="settle",
    )(parts)


def combine_kernel(chosen, shares, returned, residual, result, lines):
    count, pieces, wide = lines.shape
    top = chosen.shape[0] // count
    for row in range(count):
        total = 0.0
        for k in range(top):
            place = row * top + k
            total = total + shares[place] * returned[chosen[place]].astype(jnp.float32)
        lines[row] = total
    for piece in range(pieces):
        here = slice(piece * wide, (piece + 1) * wide)
        result[:, here] = (residual[:, here] + lines[:, piece, :]).astype(jnp.bfloat16)


def combine(chosen, shares, returned, residual):
    count, quarter = residual.shape
    vmem = pl.BlockSpec(memory_space=pltpu.VMEM)
    smem = pl.BlockSpec(memory_space=pltpu.SMEM)
    return pl.pallas_call(
        combine_kernel,
        in_specs=[smem, smem, vmem, vmem],
        out_specs=vmem,
        out_shape=jax.ShapeDtypeStruct((count, quarter), jnp.bfloat16),
        scratch_shapes=[pltpu.VMEM((count, *returned.shape[1:]), jnp.float32)],
        compiler_params=pltpu.CompilerParams(vmem_limit_bytes=20 << 20),
        name="combine",
    )(chosen, shares, returned, residual)


def body(
    tokens,
    head_state,
    mixer_gain,
    w_query,
    w_key,
    w_value,
    decay_down,
    decay_up,
    decay_base,
    rate_down,
    rate_up,
    head_gain,
    w_out,
    expert_gain,
    expert_ids,
    route_weight,
    w_gate,
    w_up,
    w_down,
):
    rows, width = tokens.shape
    cols = w_query.shape[1]
    layers = lax.axis_size("z")
    lanes = lax.axis_size("tp")
    experts = lax.axis_size(EP)
    lane = lax.axis_index("tp")
    block = width // layers

    spread_rows, normed = norm(tokens, mixer_gain, layers)
    spread_rows = swap(spread_rows, "z")
    weights = lax.all_gather(
        jnp.concatenate([w_query, w_key, w_value, w_out.T], axis=1), PLANE, axis=0, tiled=True
    )
    partial_rows = jnp.dot(
        spread_rows.reshape(layers * rows, block),
        weights[:, : 3 * cols],
        preferred_element_type=jnp.float32,
    ).astype(jnp.bfloat16)
    summed = swap(partial_rows.reshape(layers, rows, 3 * cols), "z")
    factors = low_rank(
        normed, decay_down, decay_up, decay_base, rate_down, rate_up, head_gain, lane
    )
    match = expert_ids[:, :, None] == jnp.arange(experts, dtype=jnp.int32)[None, None, :]
    order = jnp.arange(rows, dtype=jnp.int32)[:, None, None]
    slots = jnp.min(jnp.where(match, order, rows), axis=(0, 1))
    shares = (route_weight / jnp.sum(route_weight, axis=1, keepdims=True)).reshape(-1)
    chosen = expert_ids.reshape(-1)
    summed, factors, slots, shares, chosen = lax.optimization_barrier(
        (summed, factors, slots, shares, chosen)
    )
    next_state, spread_out = recurrence(summed, factors, head_state)
    partial_out = output(swap(spread_out, "z"), weights, lanes)
    home_out = swap(partial_out.reshape(layers * lanes, rows, block), ("z", "tp"))
    home_out = home_out.reshape(layers, lanes, rows, block)
    outbound, residual = dispatch(home_out, tokens, expert_gain, slots, lane)
    arrived = swap(outbound, EP)
    expert_parts = expert_rows(arrived, w_gate[0], w_up[0], w_down[0], lanes)
    returned = swap(settle(swap(expert_parts, "tp")), EP)
    layer_out = combine(chosen, shares, returned, residual)
    return (layer_out, next_state)


def solution(mesh):
    side = math.isqrt(mesh.shape["ep"] // 2)
    grid = Mesh(
        mesh.devices.reshape(side, side, 2, mesh.shape["tp"]), ("z", "y", "c", "tp")
    )
    return jax.shard_map(
        body,
        mesh=grid,
        in_specs=(
            P(EP, None),
            P(EP, "tp", None),
            P(),
            P(EP, "tp"),
            P(EP, "tp"),
            P(EP, "tp"),
            P(),
            P(),
            P("tp"),
            P(),
            P(),
            P("tp"),
            P("tp", EP),
            P(),
            P(EP, None),
            P(EP, None),
            P(EP, None, "tp"),
            P(EP, None, "tp"),
            P(EP, "tp", None),
        ),
        out_specs=(P(EP, "tp"), P(EP, "tp", None)),
        check_vma=False,
    )
```

```python
import functools
import math

import jax
import jax.numpy as jnp
from jax import lax
from jax.experimental import pallas as pl
from jax.experimental.pallas import tpu as pltpu
from jax.sharding import Mesh, PartitionSpec as P

norm_eps = 1e-06
group_eps = 0.00064
EP = ("z", "y", "c")
PLANE = ("y", "c")


def swap(array, axis):
    return lax.all_to_all(array, axis, split_axis=0, concat_axis=0, tiled=True)


def norm_kernel(experts, tokens_in, gain_in, ids_in, rows, normed, tokens, gain, ids, done):
    layers, depth, block = rows.shape
    count = tokens.shape[0]
    f32, bf16 = jnp.float32, jnp.bfloat16
    sources = (tokens_in, gain_in, ids_in)
    copies = [
        pltpu.make_async_copy(source, target, done.at[k])
        for k, (source, target) in enumerate(zip(sources, (tokens, gain, ids)))
    ]
    for copy in copies:
        copy.start()
    for copy in copies:
        copy.wait()
    widened = tokens[...].astype(f32)
    scale = lax.rsqrt(jnp.mean(widened * widened, axis=1, keepdims=True) + norm_eps)
    scaled = (widened * scale * gain[...]).astype(bf16)
    normed[...] = scaled
    table_shape = (experts, count)
    row = lax.broadcasted_iota(jnp.int32, table_shape, 0)
    named = row == ids[0:1, :]
    for k in range(1, ids.shape[0]):
        named = named | (row == ids[k : k + 1, :])
    offsets = lax.broadcasted_iota(jnp.int32, (8, count), 1) - count
    table = count + lax.dot_general(
        offsets.astype(f32).astype(bf16),
        jnp.where(named, 1.0, 0.0).astype(bf16),
        (((1,), (1,)), ((), ())),
        preferred_element_type=f32,
    )
    table = jnp.concatenate([table, table], axis=0).astype(bf16)
    for z in range(layers):
        here = slice(z * block, (z + 1) * block)
        rows[z, :count] = scaled[:, here]
        rows[z, count : 2 * count] = tokens[:, here]
        rows[z, 2 * count :, :experts] = table


def norm(tokens, gain, expert_ids, layers, experts):
    count, width = tokens.shape
    bf16 = jnp.bfloat16
    top = expert_ids.shape[1]
    return pl.pallas_call(
        functools.partial(norm_kernel, experts),
        in_specs=[pl.BlockSpec(memory_space=pltpu.HBM)] * 3,
        out_shape=(
            jax.ShapeDtypeStruct((layers, 3 * count, width // layers), bf16),
            jax.ShapeDtypeStruct((count, width), bf16),
        ),
        scratch_shapes=[
            pltpu.VMEM((count, width), bf16),
            pltpu.VMEM((1, width), jnp.float32),
            pltpu.VMEM((top, count), jnp.int32),
            pltpu.SemaphoreType.DMA((3,)),
        ],
        compiler_params=pltpu.CompilerParams(vmem_limit_bytes=20 << 20),
        name="norm",
    )(tokens, gain.reshape(1, width), expert_ids.T)


def project_kernel(rows, weights, result):
    layers, count, cols = result.shape
    product = jnp.dot(
        rows[:, :count, :].reshape(layers * count, rows.shape[2]),
        weights[:, :cols],
        preferred_element_type=jnp.float32,
    )
    result[...] = product.astype(jnp.bfloat16).reshape(result.shape)


def project(rows, weights, count, cols):
    return pl.pallas_call(
        project_kernel,
        out_shape=jax.ShapeDtypeStruct((rows.shape[0], count, cols), jnp.bfloat16),
        compiler_params=pltpu.CompilerParams(vmem_limit_bytes=20 << 20),
        name="project",
    )(rows, weights)


def low_rank_kernel(lane, normed, down, up, base, rate_down, rate_up, gain, result):
    f32, bf16 = jnp.float32, jnp.bfloat16
    _, count, cols = result.shape
    own = pl.ds(pl.multiple_of(lane[0] * cols, cols), cols)
    rows = normed[...]
    across = lambda w: lax.dot_general(
        rows, w[...], (((1,), (1,)), ((), ())), preferred_element_type=f32
    )
    decay_low = jnp.tanh(across(down)).astype(bf16)
    decay_pre = base[...] + jnp.dot(decay_low, up[:, own], preferred_element_type=f32)
    softplus = jnp.maximum(-decay_pre, 0.0) + jnp.log1p(jnp.exp(-jnp.abs(decay_pre)))
    result[0] = jnp.exp(-jnp.exp(-softplus - 0.5))
    rate_low = across(rate_down).astype(bf16)
    rate_pre = jnp.dot(rate_low, rate_up[:, own], preferred_element_type=f32)
    result[1] = 1.0 / (1.0 + jnp.exp(-rate_pre))
    result[2] = jnp.broadcast_to(gain[...], (count, cols))


def low_rank(normed, decay_down, decay_up, decay_base, rate_down, rate_up, head_gain, lane):
    cols = decay_base.shape[0]
    vmem = pl.BlockSpec(memory_space=pltpu.VMEM)
    return pl.pallas_call(
        low_rank_kernel,
        in_specs=[pl.BlockSpec(memory_space=pltpu.SMEM)] + [vmem] * 7,
        out_specs=vmem,
        out_shape=jax.ShapeDtypeStruct((3, normed.shape[0], cols), jnp.float32),
        compiler_params=pltpu.CompilerParams(vmem_limit_bytes=20 << 20),
        name="low_rank",
    )(
        lane.reshape(1),
        normed,
        decay_down.T,
        decay_up,
        decay_base.reshape(1, cols),
        rate_down.T,
        rate_up,
        head_gain.reshape(1, cols),
    )


def split_terms(value):
    high = value.astype(jnp.bfloat16)
    return high, (value - high.astype(jnp.float32)).astype(jnp.bfloat16)


def exact_dot(value, chooser):
    high, low = split_terms(value)
    return jnp.dot(high, chooser, preferred_element_type=jnp.float32) + jnp.dot(
        low, chooser, preferred_element_type=jnp.float32
    )


def recurrence_kernel(size, parts, factors, state, new_state, spread_out):
    decays, rates, gain = factors[0], factors[1], factors[2]
    count, cols = decays.shape
    heads = cols // size
    lines = state.shape[1]
    wide = state.shape[2]
    f32, bf16 = jnp.float32, jnp.bfloat16
    iota = lambda shape, dim: lax.broadcasted_iota(jnp.int32, shape, dim)
    projected = jnp.sum(parts[...].astype(f32), axis=0).astype(bf16).astype(f32)
    queries = projected[:, :cols]
    keys = projected[:, cols : 2 * cols]
    values = projected[:, 2 * cols :]
    square = (cols, cols)
    same_head = iota(square, 0) // size == iota(square, 1) // size
    head_sum = jnp.where(same_head, 1.0, 0.0).astype(f32)
    head_mean = head_sum * (1.0 / size)
    total = lambda x, m: jnp.dot(x, m, precision=lax.Precision.HIGHEST, preferred_element_type=f32)
    units = keys * lax.rsqrt(total(keys * keys, head_sum) + 1.0)
    removal = units * rates

    def by_line(x):
        copies = jnp.broadcast_to(x[:, None, :], (count, 2 * heads, cols))
        chosen = iota(copies.shape, 2) // size == iota(copies.shape, 1) % heads
        kept = jnp.where(chosen, copies, 0.0)
        folded = kept[:, :, :wide]
        for start in range(wide, cols, wide):
            folded = folded + kept[:, :, start : start + wide]
        folded = folded.reshape(count * 2 * heads, wide)
        both = folded + pltpu.roll(folded, size, 1)
        return both.reshape(count, 1, 2 * heads, wide)

    grid_shape = (count, lines // (2 * heads), 2 * heads, wide)
    flat = (count * lines, wide)
    old = state[...].reshape(grid_shape)
    halves = (wide, wide)
    half_sum = jnp.where(iota(halves, 0) // size == iota(halves, 1) // size, 1.0, 0.0).astype(bf16)
    removed = exact_dot((old * by_line(units)).reshape(flat), half_sum).reshape(grid_shape)
    pick = (lines, cols)
    line, col = iota(pick, 0), iota(pick, 1)
    owner = (col // size == line % heads) & ((col % size) // 2 == line // heads)
    value_rows = jnp.where(owner[None], jnp.broadcast_to(values[:, None, :], (count, *pick)), 0.0)
    tall = (cols, wide)
    to_half = jnp.where(iota(tall, 0) % 2 == iota(tall, 1) // size, 1.0, 0.0).astype(bf16)
    value_grid = jnp.dot(
        value_rows.reshape(count * lines, cols).astype(bf16), to_half, preferred_element_type=f32
    ).reshape(grid_shape)
    updated = old * by_line(decays) - removed * by_line(removal) + value_grid * by_line(keys)
    new_state[...] = updated.reshape(new_state.shape)
    broad = (wide, cols)
    from_half = jnp.where(iota(broad, 0) // size == iota(broad, 1) % 2, 1.0, 0.0).astype(bf16)
    reads = exact_dot((updated * by_line(queries)).reshape(flat), from_half)
    readout = jnp.sum(jnp.where(owner[None], reads.reshape(count, *pick), 0.0), axis=1)
    centred = readout - total(readout, head_mean)
    spread = total(centred * centred, head_mean)
    scaled = (centred * lax.rsqrt(spread + group_eps) * gain).astype(bf16)
    spread_out[...] = jnp.broadcast_to(scaled[None], spread_out.shape)


def recurrence(parts, factors, old_state):
    layers = parts.shape[0]
    _, count, cols = factors.shape
    heads, area = old_state.shape[1:]
    size = math.isqrt(area)
    wide = 2 * size
    lines = area // wide
    state = old_state.reshape(count, heads, lines, wide).transpose(0, 2, 1, 3)
    state = state.reshape(count, lines * heads, wide)
    new_state, spread_out = pl.pallas_call(
        functools.partial(recurrence_kernel, size),
        out_shape=(
            jax.ShapeDtypeStruct(state.shape, jnp.float32),
            jax.ShapeDtypeStruct((layers, count, cols), jnp.bfloat16),
        ),
        compiler_params=pltpu.CompilerParams(vmem_limit_bytes=40 << 20),
        name="recurrence",
    )(parts, factors, state)
    new_state = new_state.reshape(count, lines, heads, wide).transpose(0, 2, 1, 3)
    return new_state.reshape(old_state.shape), spread_out


def output_kernel(heads, weights, result):
    layers, count, cols = heads.shape
    product = lax.dot_general(
        heads[...].reshape(layers * count, cols),
        weights[:, weights.shape[1] - cols :],
        (((1,), (1,)), ((), ())),
        preferred_element_type=jnp.float32,
    )
    result[...] = product.astype(jnp.bfloat16).reshape(result.shape)


def output(heads, weights, lanes):
    layers, count, _ = heads.shape
    shape = (lanes, layers * count // lanes, weights.shape[0])
    return pl.pallas_call(
        output_kernel,
        out_shape=jax.ShapeDtypeStruct(shape, jnp.bfloat16),
        compiler_params=pltpu.CompilerParams(vmem_limit_bytes=20 << 20),
        name="output",
    )(heads, weights)


def dispatch_kernel(slots, lane, parts, rows, outbound, residual, lines):
    lanes, some, block = parts.shape
    own = rows.shape[0] // lanes
    count = some // own
    experts, _, wide = lines.shape
    pieces = block // wide
    f32, bf16 = jnp.float32, jnp.bfloat16
    mixed = parts[0].astype(f32)
    for part in range(1, lanes):
        mixed = mixed + parts[part].astype(f32)
    for k in range(own):
        here = rows[lane[0] * own + k, count : 2 * count, :].astype(f32)
        total = (here + mixed[k * count : (k + 1) * count]).astype(bf16).astype(f32)
        base = k * (count + 1)
        for piece in range(pieces):
            residual[base : base + count, piece, :] = total[:, piece * wide : (piece + 1) * wide]
        residual[base + count] = jnp.zeros((pieces, wide), f32)

    def send(expert, carry):
        for k in range(own):
            slot = slots[k * experts + expert] + k * (count + 1)
            lines[expert, k * pieces : (k + 1) * pieces, :] = residual[slot]
        return carry

    lax.fori_loop(0, experts, send, 0, unroll=8)
    outbound[...] = lines[...].astype(bf16)


def dispatch(parts, rows, slots, lane, experts):
    lanes, some, block = parts.shape
    own = rows.shape[0] // lanes
    wide = 128
    pieces = block // wide
    vmem = pl.BlockSpec(memory_space=pltpu.VMEM)
    smem = pl.BlockSpec(memory_space=pltpu.SMEM)
    shape = (experts, own * pieces, wide)
    return pl.pallas_call(
        dispatch_kernel,
        in_specs=[smem, smem, vmem, vmem],
        out_specs=vmem,
        out_shape=jax.ShapeDtypeStruct(shape, jnp.bfloat16),
        scratch_shapes=[
            pltpu.VMEM((own + some, pieces, wide), jnp.float32),
            pltpu.VMEM(shape, jnp.float32),
        ],
        compiler_params=pltpu.CompilerParams(vmem_limit_bytes=20 << 20),
        name="dispatch",
    )(slots, lane.reshape(1), parts, rows)


def assemble_kernel(layers, arrived, result, lines):
    lanes, some, width = result.shape
    peers = arrived.shape[0] // layers
    wide = arrived.shape[2]
    own = some // peers
    pieces = arrived.shape[1] // own
    lines[...] = arrived[...].astype(jnp.float32)
    for k in range(own):
        for z in range(layers):
            for piece in range(pieces):
                start = (z * pieces + piece) * wide
                block = lines[z * peers : (z + 1) * peers, k * pieces + piece, :]
                block = block.astype(jnp.bfloat16)
                for part in range(lanes):
                    result[part, k * peers : (k + 1) * peers, start : start + wide] = block


def assemble(arrived, layers, lanes, width):
    some = arrived.shape[0] // lanes
    return pl.pallas_call(
        functools.partial(assemble_kernel, layers),
        out_shape=jax.ShapeDtypeStruct((lanes, some, width), jnp.bfloat16),
        scratch_shapes=[pltpu.VMEM(arrived.shape, jnp.float32)],
        compiler_params=pltpu.CompilerParams(vmem_limit_bytes=20 << 20),
        name="assemble",
    )(arrived)


def expert_kernel(rows, gain, gate, up, down, result):
    lanes, count, quarter = result.shape
    width = rows.shape[2]
    f32 = jnp.float32
    widened = rows[...].astype(f32).reshape(count, width)
    scale = lax.rsqrt(jnp.mean(widened * widened, axis=1, keepdims=True) + norm_eps)
    normed = (widened * scale * gain[...]).astype(jnp.bfloat16)
    gate_act = jnp.dot(normed, gate[...], preferred_element_type=f32)
    up_act = jnp.dot(normed, up[...], preferred_element_type=f32)
    hidden = (gate_act / (1.0 + jnp.exp(-gate_act)) * up_act).astype(jnp.bfloat16)
    for part in range(lanes):
        here = slice(part * quarter, (part + 1) * quarter)
        product = jnp.dot(hidden, down[:, here], preferred_element_type=f32)
        result[part] = product.astype(jnp.bfloat16)


def expert_rows(rows, gain, gate, up, down):
    lanes, some, width = rows.shape
    return pl.pallas_call(
        expert_kernel,
        out_shape=jax.ShapeDtypeStruct((lanes, lanes * some, width // lanes), jnp.bfloat16),
        compiler_params=pltpu.CompilerParams(vmem_limit_bytes=20 << 20),
        name="expert",
    )(rows, gain.reshape(1, width), gate, up, down)


def settle_kernel(lane, parts, rows, result, lines):
    lanes, count, quarter = parts.shape
    pieces, wide = lines.shape[1:]
    own = pl.ds(pl.multiple_of(lane[0] * quarter, quarter), quarter)
    total = rows[:, :, own].astype(jnp.float32).reshape(count, quarter)
    for part in range(lanes):
        total = total + parts[part].astype(jnp.float32)
    for piece in range(pieces):
        lines[:, piece, :] = total[:, piece * wide : (piece + 1) * wide]
    result[...] = lines[...].astype(jnp.bfloat16)


def settle(parts, rows, lane):
    _, count, quarter = parts.shape
    shape = (count, quarter // 128, 128)
    vmem = pl.BlockSpec(memory_space=pltpu.VMEM)
    return pl.pallas_call(
        settle_kernel,
        in_specs=[pl.BlockSpec(memory_space=pltpu.SMEM), vmem, vmem],
        out_specs=vmem,
        out_shape=jax.ShapeDtypeStruct(shape, jnp.bfloat16),
        scratch_shapes=[pltpu.VMEM(shape, jnp.float32)],
        compiler_params=pltpu.CompilerParams(vmem_limit_bytes=20 << 20),
        name="settle",
    )(lane.reshape(1), parts, rows)


def combine_kernel(chosen, shares, returned, result, lines):
    count, pieces, wide = lines.shape
    top = chosen.shape[0] // count
    for row in range(count):
        total = 0.0
        for k in range(top):
            place = row * top + k
            total = total + shares[place] * returned[chosen[place]].astype(jnp.float32)
        lines[row] = total
    for piece in range(pieces):
        here = slice(piece * wide, (piece + 1) * wide)
        result[:, here] = lines[:, piece, :].astype(jnp.bfloat16)


def combine(chosen, shares, returned, count):
    _, pieces, wide = returned.shape
    vmem = pl.BlockSpec(memory_space=pltpu.VMEM)
    smem = pl.BlockSpec(memory_space=pltpu.SMEM)
    return pl.pallas_call(
        combine_kernel,
        in_specs=[smem, smem, vmem],
        out_specs=vmem,
        out_shape=jax.ShapeDtypeStruct((count, pieces * wide), jnp.bfloat16),
        scratch_shapes=[pltpu.VMEM((count, pieces, wide), jnp.float32)],
        compiler_params=pltpu.CompilerParams(vmem_limit_bytes=20 << 20),
        name="combine",
    )(chosen, shares, returned)


def body(
    tokens,
    head_state,
    mixer_gain,
    w_query,
    w_key,
    w_value,
    decay_down,
    decay_up,
    decay_base,
    rate_down,
    rate_up,
    head_gain,
    w_out,
    expert_gain,
    expert_ids,
    route_weight,
    w_gate,
    w_up,
    w_down,
):
    rows, width = tokens.shape
    cols = w_query.shape[1]
    layers = lax.axis_size("z")
    lanes = lax.axis_size("tp")
    experts = lax.axis_size(EP)
    lane = lax.axis_index("tp")

    spread_rows, normed = norm(tokens, mixer_gain, expert_ids, layers, experts)
    spread_rows = swap(spread_rows, "z")
    weights = lax.all_gather(
        jnp.concatenate([w_query, w_key, w_value, w_out.T], axis=1), PLANE, axis=0, tiled=True
    )
    summed = swap(project(spread_rows, weights, rows, 3 * cols), "z")
    factors = low_rank(
        normed, decay_down, decay_up, decay_base, rate_down, rate_up, head_gain, lane
    )
    own = layers // lanes
    slots = lax.dynamic_slice_in_dim(spread_rows[:, 2 * rows, :experts], lane * own, own, 0)
    slots = slots.astype(jnp.int32).reshape(-1)
    shares = (route_weight / jnp.sum(route_weight, axis=1, keepdims=True)).reshape(-1)
    chosen = expert_ids.reshape(-1)
    summed, factors, slots, shares, chosen = lax.optimization_barrier(
        (summed, factors, slots, shares, chosen)
    )
    next_state, spread_out = recurrence(summed, factors, head_state)
    mixed_parts = swap(output(swap(spread_out, "z"), weights, lanes), "tp")
    arrived = swap(dispatch(mixed_parts, spread_rows, slots, lane, experts), EP)
    whole = swap(assemble(arrived, layers, lanes, width), "tp")
    expert_parts = expert_rows(whole, expert_gain, w_gate[0], w_up[0], w_down[0])
    returned = swap(settle(swap(expert_parts, "tp"), whole, lane), EP)
    layer_out = combine(chosen, shares, returned, rows)
    return (layer_out, next_state)


def solution(mesh):
    side = math.isqrt(mesh.shape["ep"] // 2)
    grid = Mesh(
        mesh.devices.reshape(side, side, 2, mesh.shape["tp"]), ("z", "y", "c", "tp")
    )
    return jax.shard_map(
        body,
        mesh=grid,
        in_specs=(
            P(EP, None),
            P(EP, "tp", None),
            P(),
            P(EP, "tp"),
            P(EP, "tp"),
            P(EP, "tp"),
            P(),
            P(),
            P("tp"),
            P(),
            P(),
            P("tp"),
            P("tp", EP),
            P(),
            P(EP, None),
            P(EP, None),
            P(EP, None, "tp"),
            P(EP, None, "tp"),
            P(EP, "tp", None),
        ),
        out_specs=(P(EP, "tp"), P(EP, "tp", None)),
        check_vma=False,
    )
```

```python
import functools
import math

import jax
import jax.numpy as jnp
from jax import lax
from jax.experimental import pallas as pl
from jax.experimental.pallas import tpu as pltpu
from jax.sharding import Mesh, PartitionSpec as P

norm_eps = 1e-06
group_eps = 0.00064
EP = ("z", "y", "c")
PLANE = ("y", "c")


def swap(array, axis):
    return lax.all_to_all(array, axis, split_axis=0, concat_axis=0, tiled=True)


def norm_kernel(experts, tokens_in, gain_in, ids_in, rows, normed, tokens, gain, ids, done):
    layers, depth, block = rows.shape
    count = tokens.shape[0]
    f32, bf16 = jnp.float32, jnp.bfloat16
    sources = (tokens_in, gain_in, ids_in)
    copies = [
        pltpu.make_async_copy(source, target, done.at[k])
        for k, (source, target) in enumerate(zip(sources, (tokens, gain, ids)))
    ]
    for copy in copies:
        copy.start()
    for copy in copies:
        copy.wait()
    widened = tokens[...].astype(f32)
    scale = lax.rsqrt(jnp.mean(widened * widened, axis=1, keepdims=True) + norm_eps)
    scaled = (widened * scale * gain[...]).astype(bf16)
    normed[...] = scaled
    table_shape = (experts, count)
    row = lax.broadcasted_iota(jnp.int32, table_shape, 0)
    named = row == ids[0:1, :]
    for k in range(1, ids.shape[0]):
        named = named | (row == ids[k : k + 1, :])
    offsets = lax.broadcasted_iota(jnp.int32, (8, count), 1) - count
    table = count + lax.dot_general(
        offsets.astype(f32).astype(bf16),
        jnp.where(named, 1.0, 0.0).astype(bf16),
        (((1,), (1,)), ((), ())),
        preferred_element_type=f32,
    )
    table = jnp.concatenate([table, table], axis=0).astype(bf16)
    for z in range(layers):
        here = slice(z * block, (z + 1) * block)
        rows[z, :count] = scaled[:, here]
        rows[z, count : 2 * count] = tokens[:, here]
        rows[z, 2 * count :, :experts] = table


def norm(tokens, gain, expert_ids, layers, experts):
    count, width = tokens.shape
    bf16 = jnp.bfloat16
    top = expert_ids.shape[1]
    inputs = (tokens, gain.reshape(1, width), expert_ids.T)
    return pl.pallas_call(
        functools.partial(norm_kernel, experts),
        in_specs=[pl.BlockSpec(memory_space=pltpu.HBM)] * 3,
        out_shape=(
            jax.ShapeDtypeStruct((layers, 3 * count, width // layers), bf16),
            jax.ShapeDtypeStruct((count, width), bf16),
        ),
        scratch_shapes=[
            pltpu.VMEM((count, width), bf16),
            pltpu.VMEM((1, width), jnp.float32),
            pltpu.VMEM((top, count), jnp.int32),
            pltpu.SemaphoreType.DMA((3,)),
        ],
        compiler_params=pltpu.CompilerParams(vmem_limit_bytes=20 << 20),
        name="norm",
    )(*(pltpu.with_memory_space_constraint(x, pltpu.HBM) for x in inputs))


def project_kernel(rows, weights, result):
    layers, count, cols = result.shape
    product = jnp.dot(
        rows[:, :count, :].reshape(layers * count, rows.shape[2]),
        weights[:, :cols],
        preferred_element_type=jnp.float32,
    )
    result[...] = product.astype(jnp.bfloat16).reshape(result.shape)


def project(rows, weights, count, cols):
    return pl.pallas_call(
        project_kernel,
        out_shape=jax.ShapeDtypeStruct((rows.shape[0], count, cols), jnp.bfloat16),
        compiler_params=pltpu.CompilerParams(vmem_limit_bytes=20 << 20),
        name="project",
    )(rows, weights)


def low_rank_kernel(lane, normed, down, up, base, rate_down, rate_up, gain, result):
    f32, bf16 = jnp.float32, jnp.bfloat16
    _, count, cols = result.shape
    own = pl.ds(pl.multiple_of(lane[0] * cols, cols), cols)
    rows = normed[...]
    across = lambda w: lax.dot_general(
        rows, w[...], (((1,), (1,)), ((), ())), preferred_element_type=f32
    )
    decay_low = jnp.tanh(across(down)).astype(bf16)
    decay_pre = base[...] + jnp.dot(decay_low, up[:, own], preferred_element_type=f32)
    softplus = jnp.maximum(-decay_pre, 0.0) + jnp.log1p(jnp.exp(-jnp.abs(decay_pre)))
    result[0] = jnp.exp(-jnp.exp(-softplus - 0.5))
    rate_low = across(rate_down).astype(bf16)
    rate_pre = jnp.dot(rate_low, rate_up[:, own], preferred_element_type=f32)
    result[1] = 1.0 / (1.0 + jnp.exp(-rate_pre))
    result[2] = jnp.broadcast_to(gain[...], (count, cols))


def low_rank(normed, decay_down, decay_up, decay_base, rate_down, rate_up, head_gain, lane):
    cols = decay_base.shape[0]
    vmem = pl.BlockSpec(memory_space=pltpu.VMEM)
    return pl.pallas_call(
        low_rank_kernel,
        in_specs=[pl.BlockSpec(memory_space=pltpu.SMEM)] + [vmem] * 7,
        out_specs=vmem,
        out_shape=jax.ShapeDtypeStruct((3, normed.shape[0], cols), jnp.float32),
        compiler_params=pltpu.CompilerParams(vmem_limit_bytes=20 << 20),
        name="low_rank",
    )(
        lane.reshape(1),
        normed,
        decay_down.T,
        decay_up,
        decay_base.reshape(1, cols),
        rate_down.T,
        rate_up,
        head_gain.reshape(1, cols),
    )


def split_terms(value):
    high = value.astype(jnp.bfloat16)
    return high, (value - high.astype(jnp.float32)).astype(jnp.bfloat16)


def exact_dot(value, chooser):
    high, low = split_terms(value)
    return jnp.dot(high, chooser, preferred_element_type=jnp.float32) + jnp.dot(
        low, chooser, preferred_element_type=jnp.float32
    )


def recurrence_kernel(size, parts, factors, state, new_state, spread_out):
    decays, rates, gain = factors[0], factors[1], factors[2]
    count, cols = decays.shape
    heads = cols // size
    lines = state.shape[1]
    wide = state.shape[2]
    f32, bf16 = jnp.float32, jnp.bfloat16
    iota = lambda shape, dim: lax.broadcasted_iota(jnp.int32, shape, dim)
    projected = jnp.sum(parts[...].astype(f32), axis=0).astype(bf16).astype(f32)
    queries = projected[:, :cols]
    keys = projected[:, cols : 2 * cols]
    values = projected[:, 2 * cols :]
    square = (cols, cols)
    same_head = iota(square, 0) // size == iota(square, 1) // size
    head_sum = jnp.where(same_head, 1.0, 0.0).astype(f32)
    head_mean = head_sum * (1.0 / size)
    total = lambda x, m: jnp.dot(x, m, precision=lax.Precision.HIGHEST, preferred_element_type=f32)
    units = keys * lax.rsqrt(total(keys * keys, head_sum) + 1.0)
    removal = units * rates

    def by_line(x):
        copies = jnp.broadcast_to(x[:, None, :], (count, 2 * heads, cols))
        chosen = iota(copies.shape, 2) // size == iota(copies.shape, 1) % heads
        kept = jnp.where(chosen, copies, 0.0)
        folded = kept[:, :, :wide]
        for start in range(wide, cols, wide):
            folded = folded + kept[:, :, start : start + wide]
        folded = folded.reshape(count * 2 * heads, wide)
        both = folded + pltpu.roll(folded, size, 1)
        return both.reshape(count, 1, 2 * heads, wide)

    grid_shape = (count, lines // (2 * heads), 2 * heads, wide)
    flat = (count * lines, wide)
    old = state[...].reshape(grid_shape)
    halves = (wide, wide)
    half_sum = jnp.where(iota(halves, 0) // size == iota(halves, 1) // size, 1.0, 0.0).astype(bf16)
    removed = exact_dot((old * by_line(units)).reshape(flat), half_sum).reshape(grid_shape)
    pick = (lines, cols)
    line, col = iota(pick, 0), iota(pick, 1)
    owner = (col // size == line % heads) & ((col % size) // 2 == line // heads)
    value_rows = jnp.where(owner[None], jnp.broadcast_to(values[:, None, :], (count, *pick)), 0.0)
    tall = (cols, wide)
    to_half = jnp.where(iota(tall, 0) % 2 == iota(tall, 1) // size, 1.0, 0.0).astype(bf16)
    value_grid = jnp.dot(
        value_rows.reshape(count * lines, cols).astype(bf16), to_half, preferred_element_type=f32
    ).reshape(grid_shape)
    updated = old * by_line(decays) - removed * by_line(removal) + value_grid * by_line(keys)
    new_state[...] = updated.reshape(new_state.shape)
    broad = (wide, cols)
    from_half = jnp.where(iota(broad, 0) // size == iota(broad, 1) % 2, 1.0, 0.0).astype(bf16)
    reads = exact_dot((updated * by_line(queries)).reshape(flat), from_half)
    readout = jnp.sum(jnp.where(owner[None], reads.reshape(count, *pick), 0.0), axis=1)
    centred = readout - total(readout, head_mean)
    spread = total(centred * centred, head_mean)
    scaled = (centred * lax.rsqrt(spread + group_eps) * gain).astype(bf16)
    spread_out[...] = jnp.broadcast_to(scaled[None], spread_out.shape)


def recurrence(parts, factors, old_state):
    layers = parts.shape[0]
    _, count, cols = factors.shape
    heads, area = old_state.shape[1:]
    size = math.isqrt(area)
    wide = 2 * size
    lines = area // wide
    state = old_state.reshape(count, heads, lines, wide).transpose(0, 2, 1, 3)
    state = state.reshape(count, lines * heads, wide)
    new_state, spread_out = pl.pallas_call(
        functools.partial(recurrence_kernel, size),
        out_shape=(
            jax.ShapeDtypeStruct(state.shape, jnp.float32),
            jax.ShapeDtypeStruct((layers, count, cols), jnp.bfloat16),
        ),
        compiler_params=pltpu.CompilerParams(vmem_limit_bytes=40 << 20),
        name="recurrence",
    )(parts, factors, state)
    new_state = new_state.reshape(count, lines, heads, wide).transpose(0, 2, 1, 3)
    return new_state.reshape(old_state.shape), spread_out


def output_kernel(heads, weights, result):
    layers, count, cols = heads.shape
    product = lax.dot_general(
        heads[...].reshape(layers * count, cols),
        weights[:, weights.shape[1] - cols :],
        (((1,), (1,)), ((), ())),
        preferred_element_type=jnp.float32,
    )
    result[...] = product.astype(jnp.bfloat16).reshape(result.shape)


def output(heads, weights, lanes):
    layers, count, _ = heads.shape
    shape = (lanes, layers * count // lanes, weights.shape[0])
    return pl.pallas_call(
        output_kernel,
        out_shape=jax.ShapeDtypeStruct(shape, jnp.bfloat16),
        compiler_params=pltpu.CompilerParams(vmem_limit_bytes=20 << 20),
        name="output",
    )(heads, weights)


def dispatch_kernel(lane, parts, rows, outbound, lines):
    lanes, some, block = parts.shape
    own = rows.shape[0] // lanes
    count = some // own
    experts, _, wide = lines.shape
    pieces = block // wide
    f32, bf16 = jnp.float32, jnp.bfloat16
    mixed = parts[0].astype(f32)
    for part in range(1, lanes):
        mixed = mixed + parts[part].astype(f32)
    order = lax.broadcasted_iota(jnp.int32, (count, experts), 0).astype(f32)
    for k in range(own):
        source = lane[0] * own + k
        here = rows[source, count : 2 * count, :].astype(f32)
        residual = (here + mixed[k * count : (k + 1) * count]).astype(bf16)
        table = rows[source, 2 * count :, :experts].astype(f32)
        chosen = jnp.where(table == order, 1.0, 0.0).astype(bf16)
        packed = lax.dot_general(
            chosen, residual, (((0,), (0,)), ((), ())), preferred_element_type=f32
        )
        for piece in range(pieces):
            lines[:, k * pieces + piece, :] = packed[:, piece * wide : (piece + 1) * wide]
    outbound[...] = lines[...].astype(bf16)


def dispatch(parts, rows, lane, experts):
    lanes, some, block = parts.shape
    own = rows.shape[0] // lanes
    wide = 128
    shape = (experts, own * (block // wide), wide)
    vmem = pl.BlockSpec(memory_space=pltpu.VMEM)
    return pl.pallas_call(
        dispatch_kernel,
        in_specs=[pl.BlockSpec(memory_space=pltpu.SMEM), vmem, vmem],
        out_specs=vmem,
        out_shape=jax.ShapeDtypeStruct(shape, jnp.bfloat16),
        scratch_shapes=[pltpu.VMEM(shape, jnp.float32)],
        compiler_params=pltpu.CompilerParams(vmem_limit_bytes=20 << 20),
        name="dispatch",
    )(lane.reshape(1), parts, rows)


def assemble_kernel(layers, arrived, result, lines):
    lanes, some, width = result.shape
    peers = arrived.shape[0] // layers
    wide = arrived.shape[2]
    own = some // peers
    pieces = arrived.shape[1] // own
    lines[...] = arrived[...].astype(jnp.float32)
    for k in range(own):
        for z in range(layers):
            for piece in range(pieces):
                start = (z * pieces + piece) * wide
                block = lines[z * peers : (z + 1) * peers, k * pieces + piece, :]
                block = block.astype(jnp.bfloat16)
                for part in range(lanes):
                    result[part, k * peers : (k + 1) * peers, start : start + wide] = block


def assemble(arrived, layers, lanes, width):
    some = arrived.shape[0] // lanes
    return pl.pallas_call(
        functools.partial(assemble_kernel, layers),
        out_shape=jax.ShapeDtypeStruct((lanes, some, width), jnp.bfloat16),
        scratch_shapes=[pltpu.VMEM(arrived.shape, jnp.float32)],
        compiler_params=pltpu.CompilerParams(vmem_limit_bytes=20 << 20),
        name="assemble",
    )(arrived)


def expert_kernel(rows, gain, gate, up, down, result):
    lanes, count, quarter = result.shape
    width = rows.shape[2]
    f32 = jnp.float32
    widened = rows[...].astype(f32).reshape(count, width)
    scale = lax.rsqrt(jnp.mean(widened * widened, axis=1, keepdims=True) + norm_eps)
    normed = (widened * scale * gain[...]).astype(jnp.bfloat16)
    gate_act = jnp.dot(normed, gate[...], preferred_element_type=f32)
    up_act = jnp.dot(normed, up[...], preferred_element_type=f32)
    hidden = (gate_act / (1.0 + jnp.exp(-gate_act)) * up_act).astype(jnp.bfloat16)
    for part in range(lanes):
        here = slice(part * quarter, (part + 1) * quarter)
        product = jnp.dot(hidden, down[:, here], preferred_element_type=f32)
        result[part] = product.astype(jnp.bfloat16)


def expert_rows(rows, gain, gate, up, down):
    lanes, some, width = rows.shape
    return pl.pallas_call(
        expert_kernel,
        out_shape=jax.ShapeDtypeStruct((lanes, lanes * some, width // lanes), jnp.bfloat16),
        compiler_params=pltpu.CompilerParams(vmem_limit_bytes=20 << 20),
        name="expert",
    )(rows, gain.reshape(1, width), gate, up, down)


def settle_kernel(lane, parts, rows, result, lines):
    lanes, count, quarter = parts.shape
    pieces, wide = lines.shape[1:]
    own = pl.ds(pl.multiple_of(lane[0] * quarter, quarter), quarter)
    total = rows[:, :, own].astype(jnp.float32).reshape(count, quarter)
    for part in range(lanes):
        total = total + parts[part].astype(jnp.float32)
    for piece in range(pieces):
        lines[:, piece, :] = total[:, piece * wide : (piece + 1) * wide]
    result[...] = lines[...].astype(jnp.bfloat16)


def settle(parts, rows, lane):
    _, count, quarter = parts.shape
    shape = (count, quarter // 128, 128)
    vmem = pl.BlockSpec(memory_space=pltpu.VMEM)
    return pl.pallas_call(
        settle_kernel,
        in_specs=[pl.BlockSpec(memory_space=pltpu.SMEM), vmem, vmem],
        out_specs=vmem,
        out_shape=jax.ShapeDtypeStruct(shape, jnp.bfloat16),
        scratch_shapes=[pltpu.VMEM(shape, jnp.float32)],
        compiler_params=pltpu.CompilerParams(vmem_limit_bytes=20 << 20),
        name="settle",
    )(lane.reshape(1), parts, rows)


def combine_kernel(weights, returned, result, lines):
    pieces, wide = returned.shape[1:]
    lines[...] = returned[...].astype(jnp.float32)
    high, low = split_terms(weights[...])
    for piece in range(pieces):
        here = lines[:, piece, :].astype(jnp.bfloat16)
        total = jnp.dot(high, here, preferred_element_type=jnp.float32)
        total = total + jnp.dot(low, here, preferred_element_type=jnp.float32)
        result[:, piece * wide : (piece + 1) * wide] = total.astype(jnp.bfloat16)


def combine(weights, returned):
    _, pieces, wide = returned.shape
    return pl.pallas_call(
        combine_kernel,
        out_shape=jax.ShapeDtypeStruct((weights.shape[0], pieces * wide), jnp.bfloat16),
        scratch_shapes=[pltpu.VMEM(returned.shape, jnp.float32)],
        compiler_params=pltpu.CompilerParams(vmem_limit_bytes=20 << 20),
        name="combine",
    )(weights, returned)


def body(
    tokens,
    head_state,
    mixer_gain,
    w_query,
    w_key,
    w_value,
    decay_down,
    decay_up,
    decay_base,
    rate_down,
    rate_up,
    head_gain,
    w_out,
    expert_gain,
    expert_ids,
    route_weight,
    w_gate,
    w_up,
    w_down,
):
    rows, width = tokens.shape
    cols = w_query.shape[1]
    layers = lax.axis_size("z")
    lanes = lax.axis_size("tp")
    experts = lax.axis_size(EP)
    lane = lax.axis_index("tp")

    spread_rows, normed = norm(tokens, mixer_gain, expert_ids, layers, experts)
    spread_rows = swap(spread_rows, "z")
    weights = lax.all_gather(
        jnp.concatenate([w_query, w_key, w_value, w_out.T], axis=1), PLANE, axis=0
    )
    weights = weights.reshape(-1, weights.shape[2])
    summed = swap(project(spread_rows, weights, rows, 3 * cols), "z")
    factors = low_rank(
        normed, decay_down, decay_up, decay_base, rate_down, rate_up, head_gain, lane
    )
    shares = route_weight / jnp.sum(route_weight, axis=1, keepdims=True)
    match = expert_ids[:, :, None] == jnp.arange(experts, dtype=jnp.int32)[None, None, :]
    shares = jnp.sum(jnp.where(match, shares[:, :, None], 0.0), axis=1)
    summed, factors, shares = lax.optimization_barrier((summed, factors, shares))
    next_state, spread_out = recurrence(summed, factors, head_state)
    mixed_parts = swap(output(swap(spread_out, "z"), weights, lanes), "tp")
    arrived = swap(dispatch(mixed_parts, spread_rows, lane, experts), EP)
    whole = swap(assemble(arrived, layers, lanes, width), "tp")
    expert_parts = expert_rows(whole, expert_gain, w_gate[0], w_up[0], w_down[0])
    returned = swap(settle(swap(expert_parts, "tp"), whole, lane), EP)
    layer_out = combine(shares, returned)
    return (layer_out, next_state)


def solution(mesh):
    side = math.isqrt(mesh.shape["ep"] // 2)
    grid = Mesh(
        mesh.devices.reshape(side, side, 2, mesh.shape["tp"]), ("z", "y", "c", "tp")
    )
    return jax.shard_map(
        body,
        mesh=grid,
        in_specs=(
            P(EP, None),
            P(EP, "tp", None),
            P(),
            P(EP, "tp"),
            P(EP, "tp"),
            P(EP, "tp"),
            P(),
            P(),
            P("tp"),
            P(),
            P(),
            P("tp"),
            P("tp", EP),
            P(),
            P(EP, None),
            P(EP, None),
            P(EP, None, "tp"),
            P(EP, None, "tp"),
            P(EP, "tp", None),
        ),
        out_specs=(P(EP, "tp"), P(EP, "tp", None)),
        check_vma=False,
    )
```

```python
import functools
import math

import jax
import jax.numpy as jnp
from jax import lax
from jax.experimental import pallas as pl
from jax.experimental.pallas import tpu as pltpu
from jax.sharding import Mesh, PartitionSpec as P

norm_eps = 1e-06
group_eps = 0.00064
EP = ("z", "y", "c")
PLANE = ("y", "c")


def swap(array, axis):
    return lax.all_to_all(array, axis, split_axis=0, concat_axis=0, tiled=True)


def norm_kernel(experts, *refs):
    sources, refs = refs[:6], refs[6:]
    rows, normed, ids, base, head_gain, route, tokens, gain, done = refs
    layers, depth, block = rows.shape
    count = tokens.shape[0]
    f32, bf16 = jnp.float32, jnp.bfloat16
    targets = (tokens, gain, ids, base, head_gain, route)
    copies = [
        pltpu.make_async_copy(source, target, done.at[k])
        for k, (source, target) in enumerate(zip(sources, targets))
    ]
    for copy in copies:
        copy.start()
    for copy in copies:
        copy.wait()
    widened = tokens[...].astype(f32)
    scale = lax.rsqrt(jnp.mean(widened * widened, axis=1, keepdims=True) + norm_eps)
    scaled = (widened * scale * gain[...]).astype(bf16)
    normed[...] = scaled
    table_shape = (experts, count)
    row = lax.broadcasted_iota(jnp.int32, table_shape, 0)
    named = row == ids[0:1, :]
    for k in range(1, ids.shape[0]):
        named = named | (row == ids[k : k + 1, :])
    offsets = lax.broadcasted_iota(jnp.int32, (8, count), 1) - count
    table = count + lax.dot_general(
        offsets.astype(f32).astype(bf16),
        jnp.where(named, 1.0, 0.0).astype(bf16),
        (((1,), (1,)), ((), ())),
        preferred_element_type=f32,
    )
    table = jnp.concatenate([table, table], axis=0).astype(bf16)
    for z in range(layers):
        here = slice(z * block, (z + 1) * block)
        rows[z, :count] = scaled[:, here]
        rows[z, count : 2 * count] = tokens[:, here]
        rows[z, 2 * count :, :experts] = table


def norm(tokens, gain, expert_ids, decay_base, head_gain, route_weight, layers, experts):
    count, width = tokens.shape
    bf16 = jnp.bfloat16
    line = lambda x: x.reshape(1, -1)
    small = (expert_ids.T, line(decay_base), line(head_gain), route_weight.T)
    inputs = (tokens, line(gain), *small)
    return pl.pallas_call(
        functools.partial(norm_kernel, experts),
        in_specs=[pl.BlockSpec(memory_space=pltpu.HBM)] * len(inputs),
        out_shape=(
            jax.ShapeDtypeStruct((layers, 3 * count, width // layers), bf16),
            jax.ShapeDtypeStruct((count, width), bf16),
            *(jax.ShapeDtypeStruct(x.shape, x.dtype) for x in small),
        ),
        scratch_shapes=[
            pltpu.VMEM((count, width), bf16),
            pltpu.VMEM((1, width), jnp.float32),
            pltpu.SemaphoreType.DMA((len(inputs),)),
        ],
        compiler_params=pltpu.CompilerParams(vmem_limit_bytes=20 << 20),
        name="norm",
    )(*(pltpu.with_memory_space_constraint(x, pltpu.HBM) for x in inputs))


def project_kernel(rows, weights, result):
    layers, count, cols = result.shape
    product = jnp.dot(
        rows[:, :count, :].reshape(layers * count, rows.shape[2]),
        weights[:, :cols],
        preferred_element_type=jnp.float32,
    )
    result[...] = product.astype(jnp.bfloat16).reshape(result.shape)


def project(rows, weights, count, cols):
    return pl.pallas_call(
        project_kernel,
        out_shape=jax.ShapeDtypeStruct((rows.shape[0], count, cols), jnp.bfloat16),
        compiler_params=pltpu.CompilerParams(vmem_limit_bytes=20 << 20),
        name="project",
    )(rows, weights)


def low_rank_kernel(
    lane, normed, down, up, base, rate_down, rate_up, gain, ids, route, result, shares
):
    f32, bf16 = jnp.float32, jnp.bfloat16
    _, count, cols = result.shape
    own = pl.ds(pl.multiple_of(lane[0] * cols, cols), cols)
    rows = normed[...]
    across = lambda w: lax.dot_general(
        rows, w[...], (((1,), (1,)), ((), ())), preferred_element_type=f32
    )
    decay_low = jnp.tanh(across(down)).astype(bf16)
    decay_pre = base[...] + jnp.dot(decay_low, up[:, own], preferred_element_type=f32)
    softplus = jnp.maximum(-decay_pre, 0.0) + jnp.log1p(jnp.exp(-jnp.abs(decay_pre)))
    result[0] = jnp.exp(-jnp.exp(-softplus - 0.5))
    rate_low = across(rate_down).astype(bf16)
    rate_pre = jnp.dot(rate_low, rate_up[:, own], preferred_element_type=f32)
    result[1] = 1.0 / (1.0 + jnp.exp(-rate_pre))
    result[2] = jnp.broadcast_to(gain[...], (count, cols))
    route_sum = jnp.sum(route[...], axis=0, keepdims=True)
    row = lax.broadcasted_iota(jnp.int32, shares.shape, 0)
    weights = jnp.zeros(shares.shape, f32)
    for k in range(ids.shape[0]):
        share = route[k : k + 1, :] / route_sum
        weights = weights + jnp.where(row == ids[k : k + 1, :], share, 0.0)
    shares[...] = weights


def low_rank(normed, decay_down, decay_up, rate_down, rate_up, small, experts, lane):
    ids, base, head_gain, route = small
    count, cols = normed.shape[0], base.shape[1]
    vmem = pl.BlockSpec(memory_space=pltpu.VMEM)
    return pl.pallas_call(
        low_rank_kernel,
        in_specs=[pl.BlockSpec(memory_space=pltpu.SMEM)] + [vmem] * 9,
        out_specs=(vmem, vmem),
        out_shape=(
            jax.ShapeDtypeStruct((3, count, cols), jnp.float32),
            jax.ShapeDtypeStruct((experts, count), jnp.float32),
        ),
        compiler_params=pltpu.CompilerParams(vmem_limit_bytes=20 << 20),
        name="low_rank",
    )(
        lane.reshape(1),
        normed,
        decay_down.T,
        decay_up,
        base,
        rate_down.T,
        rate_up,
        head_gain,
        ids,
        route,
    )


def split_terms(value):
    high = value.astype(jnp.bfloat16)
    return high, (value - high.astype(jnp.float32)).astype(jnp.bfloat16)


def exact_dot(value, chooser):
    high, low = split_terms(value)
    return jnp.dot(high, chooser, preferred_element_type=jnp.float32) + jnp.dot(
        low, chooser, preferred_element_type=jnp.float32
    )


def recurrence_kernel(size, parts, factors, state, new_state, spread_out, fresh, done):
    decays, rates, gain = factors[0], factors[1], factors[2]
    count, cols = decays.shape
    heads = cols // size
    lines = state.shape[1]
    wide = state.shape[2]
    f32, bf16 = jnp.float32, jnp.bfloat16
    iota = lambda shape, dim: lax.broadcasted_iota(jnp.int32, shape, dim)
    projected = jnp.sum(parts[...].astype(f32), axis=0).astype(bf16).astype(f32)
    queries = projected[:, :cols]
    keys = projected[:, cols : 2 * cols]
    values = projected[:, 2 * cols :]
    square = (cols, cols)
    same_head = iota(square, 0) // size == iota(square, 1) // size
    head_sum = jnp.where(same_head, 1.0, 0.0).astype(bf16)
    head_mean = jnp.where(same_head, 1.0 / size, 0.0).astype(bf16)
    units = keys * lax.rsqrt(exact_dot(keys * keys, head_sum) + 1.0)
    removal = units * rates

    def by_line(x):
        copies = jnp.broadcast_to(x[:, None, :], (count, 2 * heads, cols))
        chosen = iota(copies.shape, 2) // size == iota(copies.shape, 1) % heads
        kept = jnp.where(chosen, copies, 0.0)
        folded = kept[:, :, :wide]
        for start in range(wide, cols, wide):
            folded = folded + kept[:, :, start : start + wide]
        folded = folded.reshape(count * 2 * heads, wide)
        both = folded + pltpu.roll(folded, size, 1)
        return both.reshape(count, 1, 2 * heads, wide)

    grid_shape = (count, lines // (2 * heads), 2 * heads, wide)
    flat = (count * lines, wide)
    old = state[...].reshape(grid_shape)
    halves = (wide, wide)
    half_sum = jnp.where(iota(halves, 0) // size == iota(halves, 1) // size, 1.0, 0.0).astype(bf16)
    removed = exact_dot((old * by_line(units)).reshape(flat), half_sum).reshape(grid_shape)
    pick = (lines, cols)
    line, col = iota(pick, 0), iota(pick, 1)
    owner = (col // size == line % heads) & ((col % size) // 2 == line // heads)
    value_rows = jnp.where(owner[None], jnp.broadcast_to(values[:, None, :], (count, *pick)), 0.0)
    tall = (cols, wide)
    to_half = jnp.where(iota(tall, 0) % 2 == iota(tall, 1) // size, 1.0, 0.0).astype(bf16)
    value_grid = jnp.dot(
        value_rows.reshape(count * lines, cols).astype(bf16), to_half, preferred_element_type=f32
    ).reshape(grid_shape)
    updated = old * by_line(decays) - removed * by_line(removal) + value_grid * by_line(keys)
    fresh[...] = updated.reshape(fresh.shape)
    store = pltpu.make_async_copy(fresh, new_state, done)
    store.start()
    broad = (wide, cols)
    from_half = jnp.where(iota(broad, 0) // size == iota(broad, 1) % 2, 1.0, 0.0).astype(bf16)
    reads = exact_dot((updated * by_line(queries)).reshape(flat), from_half)
    readout = jnp.sum(jnp.where(owner[None], reads.reshape(count, *pick), 0.0), axis=1)
    centred = readout - exact_dot(readout, head_mean)
    spread = exact_dot(centred * centred, head_mean)
    scaled = (centred * lax.rsqrt(spread + group_eps) * gain).astype(bf16)
    spread_out[...] = jnp.broadcast_to(scaled[None], spread_out.shape)
    store.wait()


def recurrence(parts, factors, old_state):
    layers = parts.shape[0]
    _, count, cols = factors.shape
    heads, area = old_state.shape[1:]
    size = math.isqrt(area)
    wide = 2 * size
    lines = area // wide
    state = old_state.reshape(count, heads, lines, wide).transpose(0, 2, 1, 3)
    state = state.reshape(count, lines * heads, wide)
    new_state, spread_out = pl.pallas_call(
        functools.partial(recurrence_kernel, size),
        out_shape=(
            jax.ShapeDtypeStruct(state.shape, jnp.float32),
            jax.ShapeDtypeStruct((layers, count, cols), jnp.bfloat16),
        ),
        out_specs=(
            pl.BlockSpec(memory_space=pltpu.HBM),
            pl.BlockSpec(memory_space=pltpu.VMEM),
        ),
        scratch_shapes=[pltpu.VMEM(state.shape, jnp.float32), pltpu.SemaphoreType.DMA],
        compiler_params=pltpu.CompilerParams(vmem_limit_bytes=40 << 20),
        name="recurrence",
    )(parts, factors, state)
    new_state = new_state.reshape(count, lines, heads, wide).transpose(0, 2, 1, 3)
    return new_state.reshape(old_state.shape), spread_out


def output_kernel(heads, weights, result):
    layers, count, cols = heads.shape
    product = lax.dot_general(
        heads[...].reshape(layers * count, cols),
        weights[:, weights.shape[1] - cols :],
        (((1,), (1,)), ((), ())),
        preferred_element_type=jnp.float32,
    )
    result[...] = product.astype(jnp.bfloat16).reshape(result.shape)


def output(heads, weights, lanes):
    layers, count, _ = heads.shape
    shape = (lanes, layers * count // lanes, weights.shape[0])
    return pl.pallas_call(
        output_kernel,
        out_shape=jax.ShapeDtypeStruct(shape, jnp.bfloat16),
        compiler_params=pltpu.CompilerParams(vmem_limit_bytes=20 << 20),
        name="output",
    )(heads, weights)


def dispatch_kernel(lane, parts, rows, outbound, lines):
    lanes, some, block = parts.shape
    own = rows.shape[0] // lanes
    count = some // own
    experts, _, wide = lines.shape
    pieces = block // wide
    f32, bf16 = jnp.float32, jnp.bfloat16
    mixed = parts[0].astype(f32)
    for part in range(1, lanes):
        mixed = mixed + parts[part].astype(f32)
    order = lax.broadcasted_iota(jnp.int32, (count, experts), 0).astype(f32)
    for k in range(own):
        source = lane[0] * own + k
        here = rows[source, count : 2 * count, :].astype(f32)
        residual = (here + mixed[k * count : (k + 1) * count]).astype(bf16)
        table = rows[source, 2 * count :, :experts].astype(f32)
        chosen = jnp.where(table == order, 1.0, 0.0).astype(bf16)
        packed = lax.dot_general(
            chosen, residual, (((0,), (0,)), ((), ())), preferred_element_type=f32
        )
        for piece in range(pieces):
            lines[:, k * pieces + piece, :] = packed[:, piece * wide : (piece + 1) * wide]
    outbound[...] = lines[...].astype(bf16)


def dispatch(parts, rows, lane, experts):
    lanes, some, block = parts.shape
    own = rows.shape[0] // lanes
    wide = 128
    shape = (experts, own * (block // wide), wide)
    vmem = pl.BlockSpec(memory_space=pltpu.VMEM)
    return pl.pallas_call(
        dispatch_kernel,
        in_specs=[pl.BlockSpec(memory_space=pltpu.SMEM), vmem, vmem],
        out_specs=vmem,
        out_shape=jax.ShapeDtypeStruct(shape, jnp.bfloat16),
        scratch_shapes=[pltpu.VMEM(shape, jnp.float32)],
        compiler_params=pltpu.CompilerParams(vmem_limit_bytes=20 << 20),
        name="dispatch",
    )(lane.reshape(1), parts, rows)


def assemble_kernel(layers, arrived, result, lines):
    lanes, some, width = result.shape
    peers = arrived.shape[0] // layers
    wide = arrived.shape[2]
    own = some // peers
    pieces = arrived.shape[1] // own
    lines[...] = arrived[...].astype(jnp.float32)
    for k in range(own):
        for z in range(layers):
            for piece in range(pieces):
                start = (z * pieces + piece) * wide
                block = lines[z * peers : (z + 1) * peers, k * pieces + piece, :]
                block = block.astype(jnp.bfloat16)
                for part in range(lanes):
                    result[part, k * peers : (k + 1) * peers, start : start + wide] = block


def assemble(arrived, layers, lanes, width):
    some = arrived.shape[0] // lanes
    return pl.pallas_call(
        functools.partial(assemble_kernel, layers),
        out_shape=jax.ShapeDtypeStruct((lanes, some, width), jnp.bfloat16),
        scratch_shapes=[pltpu.VMEM(arrived.shape, jnp.float32)],
        compiler_params=pltpu.CompilerParams(vmem_limit_bytes=20 << 20),
        name="assemble",
    )(arrived)


def expert_kernel(rows, gain, gate, up, down, result):
    lanes, count, quarter = result.shape
    width = rows.shape[2]
    f32 = jnp.float32
    widened = rows[...].astype(f32).reshape(count, width)
    scale = lax.rsqrt(jnp.mean(widened * widened, axis=1, keepdims=True) + norm_eps)
    normed = (widened * scale * gain[...]).astype(jnp.bfloat16)
    gate_act = jnp.dot(normed, gate[...], preferred_element_type=f32)
    up_act = jnp.dot(normed, up[...], preferred_element_type=f32)
    hidden = (gate_act / (1.0 + jnp.exp(-gate_act)) * up_act).astype(jnp.bfloat16)
    for part in range(lanes):
        here = slice(part * quarter, (part + 1) * quarter)
        product = jnp.dot(hidden, down[:, here], preferred_element_type=f32)
        result[part] = product.astype(jnp.bfloat16)


def expert_rows(rows, gain, gate, up, down):
    lanes, some, width = rows.shape
    return pl.pallas_call(
        expert_kernel,
        out_shape=jax.ShapeDtypeStruct((lanes, lanes * some, width // lanes), jnp.bfloat16),
        compiler_params=pltpu.CompilerParams(vmem_limit_bytes=20 << 20),
        name="expert",
    )(rows, gain.reshape(1, width), gate, up, down)


def settle_kernel(lane, parts, rows, result, lines):
    lanes, count, quarter = parts.shape
    pieces, wide = lines.shape[1:]
    own = pl.ds(pl.multiple_of(lane[0] * quarter, quarter), quarter)
    total = rows[:, :, own].astype(jnp.float32).reshape(count, quarter)
    for part in range(lanes):
        total = total + parts[part].astype(jnp.float32)
    for piece in range(pieces):
        lines[:, piece, :] = total[:, piece * wide : (piece + 1) * wide]
    result[...] = lines[...].astype(jnp.bfloat16)


def settle(parts, rows, lane):
    _, count, quarter = parts.shape
    shape = (count, quarter // 128, 128)
    vmem = pl.BlockSpec(memory_space=pltpu.VMEM)
    return pl.pallas_call(
        settle_kernel,
        in_specs=[pl.BlockSpec(memory_space=pltpu.SMEM), vmem, vmem],
        out_specs=vmem,
        out_shape=jax.ShapeDtypeStruct(shape, jnp.bfloat16),
        scratch_shapes=[pltpu.VMEM(shape, jnp.float32)],
        compiler_params=pltpu.CompilerParams(vmem_limit_bytes=20 << 20),
        name="settle",
    )(lane.reshape(1), parts, rows)


def combine_kernel(shares, returned, result, lines):
    _, pieces, wide = returned.shape
    f32 = jnp.float32
    lines[...] = returned[...].astype(f32)
    terms = split_terms(shares[...])
    for piece in range(pieces):
        here = lines[:, piece, :].astype(jnp.bfloat16)
        total = 0.0
        for term in terms:
            total = total + lax.dot_general(
                term, here, (((0,), (0,)), ((), ())), preferred_element_type=f32
            )
        result[:, piece * wide : (piece + 1) * wide] = total.astype(jnp.bfloat16)


def combine(shares, returned):
    _, pieces, wide = returned.shape
    return pl.pallas_call(
        combine_kernel,
        out_shape=jax.ShapeDtypeStruct((shares.shape[1], pieces * wide), jnp.bfloat16),
        scratch_shapes=[pltpu.VMEM(returned.shape, jnp.float32)],
        compiler_params=pltpu.CompilerParams(vmem_limit_bytes=20 << 20),
        name="combine",
    )(shares, returned)


def body(
    tokens,
    head_state,
    mixer_gain,
    w_query,
    w_key,
    w_value,
    decay_down,
    decay_up,
    decay_base,
    rate_down,
    rate_up,
    head_gain,
    w_out,
    expert_gain,
    expert_ids,
    route_weight,
    w_gate,
    w_up,
    w_down,
):
    rows, width = tokens.shape
    cols = w_query.shape[1]
    layers = lax.axis_size("z")
    lanes = lax.axis_size("tp")
    experts = lax.axis_size(EP)
    lane = lax.axis_index("tp")

    spread_rows, normed, *small = norm(
        tokens, mixer_gain, expert_ids, decay_base, head_gain, route_weight, layers, experts
    )
    spread_rows = swap(spread_rows, "z")
    weights = lax.all_gather(
        jnp.concatenate([w_query, w_key, w_value, w_out.T], axis=1), PLANE, axis=0
    )
    weights = weights.reshape(-1, weights.shape[2])
    weights, normed = lax.optimization_barrier((weights, normed))
    factors, shares = low_rank(
        normed, decay_down, decay_up, rate_down, rate_up, small, experts, lane
    )
    spread_rows, factors, shares = lax.optimization_barrier((spread_rows, factors, shares))
    summed = swap(project(spread_rows, weights, rows, 3 * cols), "z")
    next_state, spread_out = recurrence(summed, factors, head_state)
    mixed_parts = swap(output(swap(spread_out, "z"), weights, lanes), "tp")
    arrived = swap(dispatch(mixed_parts, spread_rows, lane, experts), EP)
    whole = swap(assemble(arrived, layers, lanes, width), "tp")
    expert_parts = expert_rows(whole, expert_gain, w_gate[0], w_up[0], w_down[0])
    returned = swap(settle(swap(expert_parts, "tp"), whole, lane), EP)
    layer_out = combine(shares, returned)
    return (layer_out, next_state)


def solution(mesh):
    side = math.isqrt(mesh.shape["ep"] // 2)
    grid = Mesh(
        mesh.devices.reshape(side, side, 2, mesh.shape["tp"]), ("z", "y", "c", "tp")
    )
    return jax.shard_map(
        body,
        mesh=grid,
        in_specs=(
            P(EP, None),
            P(EP, "tp", None),
            P(),
            P(EP, "tp"),
            P(EP, "tp"),
            P(EP, "tp"),
            P(),
            P(),
            P("tp"),
            P(),
            P(),
            P("tp"),
            P("tp", EP),
            P(),
            P(EP, None),
            P(EP, None),
            P(EP, None, "tp"),
            P(EP, None, "tp"),
            P(EP, "tp", None),
        ),
        out_specs=(P(EP, "tp"), P(EP, "tp", None)),
        check_vma=False,
    )
```

```python
import functools
import math

import jax
import jax.numpy as jnp
from jax import lax
from jax.experimental import pallas as pl
from jax.experimental.pallas import tpu as pltpu
from jax.sharding import Mesh, PartitionSpec as P

norm_eps = 1e-06
group_eps = 0.00064
EP = ("z", "y", "c")
PLANE = ("y", "c")


def swap(array, axis):
    return lax.all_to_all(array, axis, split_axis=0, concat_axis=0, tiled=True)


def norm_kernel(experts, *refs):
    sources, refs = refs[:6], refs[6:]
    rows, normed, ids, base, head_gain, route, tokens, gain, done = refs
    layers, depth, block = rows.shape
    count = tokens.shape[0]
    f32, bf16 = jnp.float32, jnp.bfloat16
    targets = (tokens, gain, ids, base, head_gain, route)
    copies = [
        pltpu.make_async_copy(source, target, done.at[k])
        for k, (source, target) in enumerate(zip(sources, targets))
    ]
    for copy in copies:
        copy.start()
    for copy in copies:
        copy.wait()
    widened = tokens[...].astype(f32)
    scale = lax.rsqrt(jnp.mean(widened * widened, axis=1, keepdims=True) + norm_eps)
    scaled = (widened * scale * gain[...]).astype(bf16)
    normed[...] = scaled
    table_shape = (experts, count)
    row = lax.broadcasted_iota(jnp.int32, table_shape, 0)
    named = row == ids[0:1, :]
    for k in range(1, ids.shape[0]):
        named = named | (row == ids[k : k + 1, :])
    offsets = lax.broadcasted_iota(jnp.int32, (8, count), 1) - count
    table = count + lax.dot_general(
        offsets.astype(f32).astype(bf16),
        jnp.where(named, 1.0, 0.0).astype(bf16),
        (((1,), (1,)), ((), ())),
        preferred_element_type=f32,
    )
    table = jnp.concatenate([table, table], axis=0).astype(bf16)
    for z in range(layers):
        here = slice(z * block, (z + 1) * block)
        rows[z, :count] = scaled[:, here]
        rows[z, count : 2 * count] = tokens[:, here]
        rows[z, 2 * count :, :experts] = table


def norm(tokens, gain, expert_ids, decay_base, head_gain, route_weight, layers, experts):
    count, width = tokens.shape
    bf16 = jnp.bfloat16
    line = lambda x: x.reshape(1, -1)
    small = (expert_ids.T, line(decay_base), line(head_gain), route_weight.T)
    inputs = (tokens, line(gain), *small)
    return pl.pallas_call(
        functools.partial(norm_kernel, experts),
        in_specs=[pl.BlockSpec(memory_space=pltpu.HBM)] * len(inputs),
        out_shape=(
            jax.ShapeDtypeStruct((layers, 3 * count, width // layers), bf16),
            jax.ShapeDtypeStruct((count, width), bf16),
            *(jax.ShapeDtypeStruct(x.shape, x.dtype) for x in small),
        ),
        scratch_shapes=[
            pltpu.VMEM((count, width), bf16),
            pltpu.VMEM((1, width), jnp.float32),
            pltpu.SemaphoreType.DMA((len(inputs),)),
        ],
        compiler_params=pltpu.CompilerParams(vmem_limit_bytes=20 << 20),
        name="norm",
    )(*(pltpu.with_memory_space_constraint(x, pltpu.HBM) for x in inputs))


def project_kernel(rows, weights, result):
    layers, count, cols = result.shape
    product = jnp.dot(
        rows[:, :count, :].reshape(layers * count, rows.shape[2]),
        weights[:, :cols],
        preferred_element_type=jnp.float32,
    )
    result[...] = product.astype(jnp.bfloat16).reshape(result.shape)


def project(rows, weights, count, cols):
    return pl.pallas_call(
        project_kernel,
        out_shape=jax.ShapeDtypeStruct((rows.shape[0], count, cols), jnp.bfloat16),
        compiler_params=pltpu.CompilerParams(vmem_limit_bytes=20 << 20),
        name="project",
    )(rows, weights)


def low_rank_kernel(
    lane, normed, down, up, base, rate_down, rate_up, gain, ids, route, result, shares
):
    f32, bf16 = jnp.float32, jnp.bfloat16
    _, count, cols = result.shape
    own = pl.ds(pl.multiple_of(lane[0] * cols, cols), cols)
    rows = normed[...]
    across = lambda w: lax.dot_general(
        rows, w[...], (((1,), (1,)), ((), ())), preferred_element_type=f32
    )
    decay_low = jnp.tanh(across(down)).astype(bf16)
    decay_pre = base[...] + jnp.dot(decay_low, up[:, own], preferred_element_type=f32)
    softplus = jnp.maximum(-decay_pre, 0.0) + jnp.log1p(jnp.exp(-jnp.abs(decay_pre)))
    result[0] = jnp.exp(-jnp.exp(-softplus - 0.5))
    rate_low = across(rate_down).astype(bf16)
    rate_pre = jnp.dot(rate_low, rate_up[:, own], preferred_element_type=f32)
    result[1] = 1.0 / (1.0 + jnp.exp(-rate_pre))
    result[2] = jnp.broadcast_to(gain[...], (count, cols))
    route_sum = jnp.sum(route[...], axis=0, keepdims=True)
    row = lax.broadcasted_iota(jnp.int32, shares.shape, 0)
    weights = jnp.zeros(shares.shape, f32)
    for k in range(ids.shape[0]):
        share = route[k : k + 1, :] / route_sum
        weights = weights + jnp.where(row == ids[k : k + 1, :], share, 0.0)
    shares[...] = weights


def low_rank(normed, decay_down, decay_up, rate_down, rate_up, small, experts, lane):
    ids, base, head_gain, route = small
    count, cols = normed.shape[0], base.shape[1]
    vmem = pl.BlockSpec(memory_space=pltpu.VMEM)
    return pl.pallas_call(
        low_rank_kernel,
        in_specs=[pl.BlockSpec(memory_space=pltpu.SMEM)] + [vmem] * 9,
        out_specs=(vmem, vmem),
        out_shape=(
            jax.ShapeDtypeStruct((3, count, cols), jnp.float32),
            jax.ShapeDtypeStruct((experts, count), jnp.float32),
        ),
        compiler_params=pltpu.CompilerParams(vmem_limit_bytes=20 << 20),
        name="low_rank",
    )(
        lane.reshape(1),
        normed,
        decay_down.T,
        decay_up,
        base,
        rate_down.T,
        rate_up,
        head_gain,
        ids,
        route,
    )


def split_terms(value):
    high = value.astype(jnp.bfloat16)
    return high, (value - high.astype(jnp.float32)).astype(jnp.bfloat16)


def exact_dot(value, chooser):
    high, low = split_terms(value)
    return jnp.dot(high, chooser, preferred_element_type=jnp.float32) + jnp.dot(
        low, chooser, preferred_element_type=jnp.float32
    )


def recurrence_kernel(size, parts, factors, state, new_state, spread_out, fresh, done):
    decays, rates, gain = factors[0], factors[1], factors[2]
    count, cols = decays.shape
    heads = cols // size
    lines = state.shape[1]
    wide = state.shape[2]
    f32, bf16 = jnp.float32, jnp.bfloat16
    iota = lambda shape, dim: lax.broadcasted_iota(jnp.int32, shape, dim)
    projected = jnp.sum(parts[...].astype(f32), axis=0).astype(bf16).astype(f32)
    queries = projected[:, :cols]
    keys = projected[:, cols : 2 * cols]
    values = projected[:, 2 * cols :]
    square = (cols, cols)
    same_head = iota(square, 0) // size == iota(square, 1) // size
    head_sum = jnp.where(same_head, 1.0, 0.0).astype(bf16)
    head_mean = jnp.where(same_head, 1.0 / size, 0.0).astype(bf16)
    units = keys * lax.rsqrt(exact_dot(keys * keys, head_sum) + 1.0)
    removal = units * rates

    def by_line(x):
        copies = jnp.broadcast_to(x[:, None, :], (count, 2 * heads, cols))
        chosen = iota(copies.shape, 2) // size == iota(copies.shape, 1) % heads
        kept = jnp.where(chosen, copies, 0.0)
        folded = kept[:, :, :wide]
        for start in range(wide, cols, wide):
            folded = folded + kept[:, :, start : start + wide]
        folded = folded.reshape(count * 2 * heads, wide)
        both = folded + pltpu.roll(folded, size, 1)
        return both.reshape(count, 1, 2 * heads, wide)

    grid_shape = (count, lines // (2 * heads), 2 * heads, wide)
    flat = (count * lines, wide)
    old = state[...].reshape(grid_shape)
    halves = (wide, wide)
    half_sum = jnp.where(iota(halves, 0) // size == iota(halves, 1) // size, 1.0, 0.0).astype(bf16)
    removed = exact_dot((old * by_line(units)).reshape(flat), half_sum).reshape(grid_shape)
    pick = (lines, cols)
    line, col = iota(pick, 0), iota(pick, 1)
    owner = (col // size == line % heads) & ((col % size) // 2 == line // heads)
    value_rows = jnp.where(owner[None], jnp.broadcast_to(values[:, None, :], (count, *pick)), 0.0)
    tall = (cols, wide)
    to_half = jnp.where(iota(tall, 0) % 2 == iota(tall, 1) // size, 1.0, 0.0).astype(bf16)
    value_grid = jnp.dot(
        value_rows.reshape(count * lines, cols).astype(bf16), to_half, preferred_element_type=f32
    ).reshape(grid_shape)
    updated = old * by_line(decays) - removed * by_line(removal) + value_grid * by_line(keys)
    fresh[...] = updated.reshape(fresh.shape)
    store = pltpu.make_async_copy(fresh, new_state, done)
    store.start()
    broad = (wide, cols)
    from_half = jnp.where(iota(broad, 0) // size == iota(broad, 1) % 2, 1.0, 0.0).astype(bf16)
    reads = exact_dot((updated * by_line(queries)).reshape(flat), from_half)
    readout = jnp.sum(jnp.where(owner[None], reads.reshape(count, *pick), 0.0), axis=1)
    centred = readout - exact_dot(readout, head_mean)
    spread = exact_dot(centred * centred, head_mean)
    scaled = (centred * lax.rsqrt(spread + group_eps) * gain).astype(bf16)
    spread_out[...] = jnp.broadcast_to(scaled[None], spread_out.shape)
    store.wait()


def recurrence(parts, factors, old_state):
    layers = parts.shape[0]
    _, count, cols = factors.shape
    heads, area = old_state.shape[1:]
    size = math.isqrt(area)
    wide = 2 * size
    lines = area // wide
    state = old_state.reshape(count, heads, lines, wide).transpose(0, 2, 1, 3)
    state = state.reshape(count, lines * heads, wide)
    new_state, spread_out = pl.pallas_call(
        functools.partial(recurrence_kernel, size),
        out_shape=(
            jax.ShapeDtypeStruct(state.shape, jnp.float32),
            jax.ShapeDtypeStruct((layers, count, cols), jnp.bfloat16),
        ),
        out_specs=(
            pl.BlockSpec(memory_space=pltpu.HBM),
            pl.BlockSpec(memory_space=pltpu.VMEM),
        ),
        scratch_shapes=[pltpu.VMEM(state.shape, jnp.float32), pltpu.SemaphoreType.DMA],
        compiler_params=pltpu.CompilerParams(vmem_limit_bytes=40 << 20),
        name="recurrence",
    )(parts, factors, state)
    new_state = new_state.reshape(count, lines, heads, wide).transpose(0, 2, 1, 3)
    return new_state.reshape(old_state.shape), spread_out


def output_kernel(heads, weights, result):
    layers, count, cols = heads.shape
    product = lax.dot_general(
        heads[...].reshape(layers * count, cols),
        weights[:, weights.shape[1] - cols :],
        (((1,), (1,)), ((), ())),
        preferred_element_type=jnp.float32,
    )
    result[...] = jnp.broadcast_to(product.astype(jnp.bfloat16)[None], result.shape)


def output(heads, weights, lanes):
    layers, count, _ = heads.shape
    shape = (lanes, layers * count, weights.shape[0])
    return pl.pallas_call(
        output_kernel,
        out_shape=jax.ShapeDtypeStruct(shape, jnp.bfloat16),
        compiler_params=pltpu.CompilerParams(vmem_limit_bytes=20 << 20),
        name="output",
    )(heads, weights)


def dispatch_kernel(parts, rows, outbound, lines):
    lanes, some, block = parts.shape
    layers = rows.shape[0]
    count = some // layers
    experts, _, wide = lines.shape
    pieces = block // wide
    f32, bf16 = jnp.float32, jnp.bfloat16
    mixed = parts[0].astype(f32)
    for part in range(1, lanes):
        mixed = mixed + parts[part].astype(f32)
    order = lax.broadcasted_iota(jnp.int32, (count, experts), 0).astype(f32)
    for k in range(layers):
        here = rows[k, count : 2 * count, :].astype(f32)
        residual = (here + mixed[k * count : (k + 1) * count]).astype(bf16)
        table = rows[k, 2 * count :, :experts].astype(f32)
        chosen = jnp.where(table == order, 1.0, 0.0).astype(bf16)
        packed = lax.dot_general(
            chosen, residual, (((0,), (0,)), ((), ())), preferred_element_type=f32
        )
        for piece in range(pieces):
            lines[:, k * pieces + piece, :] = packed[:, piece * wide : (piece + 1) * wide]
    outbound[...] = lines[...].astype(bf16)


def dispatch(parts, rows, experts):
    _, _, block = parts.shape
    wide = 128
    shape = (experts, rows.shape[0] * (block // wide), wide)
    return pl.pallas_call(
        dispatch_kernel,
        out_shape=jax.ShapeDtypeStruct(shape, jnp.bfloat16),
        scratch_shapes=[pltpu.VMEM(shape, jnp.float32)],
        compiler_params=pltpu.CompilerParams(vmem_limit_bytes=20 << 20),
        name="dispatch",
    )(parts, rows)


def expert_kernel(layers, arrived, gain, gate, up, down, result, rows, lines):
    lanes, count, quarter = result.shape
    peers = count // layers
    wide = arrived.shape[2]
    pieces = arrived.shape[1] // layers
    f32 = jnp.float32
    lines[...] = arrived[...].astype(f32)
    for k in range(layers):
        for z in range(layers):
            for piece in range(pieces):
                start = (z * pieces + piece) * wide
                block = lines[z * peers : (z + 1) * peers, k * pieces + piece, :]
                rows[k * peers : (k + 1) * peers, start : start + wide] = block.astype(
                    jnp.bfloat16
                )
    widened = rows[...].astype(f32)
    scale = lax.rsqrt(jnp.mean(widened * widened, axis=1, keepdims=True) + norm_eps)
    normed = (widened * scale * gain[...]).astype(jnp.bfloat16)
    gate_act = jnp.dot(normed, gate[...], preferred_element_type=f32)
    up_act = jnp.dot(normed, up[...], preferred_element_type=f32)
    hidden = (gate_act / (1.0 + jnp.exp(-gate_act)) * up_act).astype(jnp.bfloat16)
    for part in range(lanes):
        here = slice(part * quarter, (part + 1) * quarter)
        product = jnp.dot(hidden, down[:, here], preferred_element_type=f32)
        result[part] = product.astype(jnp.bfloat16)


def expert_rows(arrived, gain, gate, up, down, layers, lanes):
    count = arrived.shape[0]
    width = gate.shape[0]
    return pl.pallas_call(
        functools.partial(expert_kernel, layers),
        out_shape=(
            jax.ShapeDtypeStruct((lanes, count, width // lanes), jnp.bfloat16),
            jax.ShapeDtypeStruct((count, width), jnp.bfloat16),
        ),
        scratch_shapes=[pltpu.VMEM(arrived.shape, jnp.float32)],
        compiler_params=pltpu.CompilerParams(vmem_limit_bytes=20 << 20),
        name="expert",
    )(arrived, gain.reshape(1, width), gate, up, down)


def settle_kernel(lane, parts, rows, result, lines):
    lanes, count, quarter = parts.shape
    pieces, wide = lines.shape[1:]
    own = pl.ds(pl.multiple_of(lane[0] * quarter, quarter), quarter)
    total = rows[:, own].astype(jnp.float32)
    for part in range(lanes):
        total = total + parts[part].astype(jnp.float32)
    for piece in range(pieces):
        lines[:, piece, :] = total[:, piece * wide : (piece + 1) * wide]
    result[...] = lines[...].astype(jnp.bfloat16)


def settle(parts, rows, lane):
    _, count, quarter = parts.shape
    shape = (count, quarter // 128, 128)
    vmem = pl.BlockSpec(memory_space=pltpu.VMEM)
    return pl.pallas_call(
        settle_kernel,
        in_specs=[pl.BlockSpec(memory_space=pltpu.SMEM), vmem, vmem],
        out_specs=vmem,
        out_shape=jax.ShapeDtypeStruct(shape, jnp.bfloat16),
        scratch_shapes=[pltpu.VMEM(shape, jnp.float32)],
        compiler_params=pltpu.CompilerParams(vmem_limit_bytes=20 << 20),
        name="settle",
    )(lane.reshape(1), parts, rows)


def combine_kernel(shares, returned, result, lines):
    _, pieces, wide = returned.shape
    f32 = jnp.float32
    lines[...] = returned[...].astype(f32)
    terms = split_terms(shares[...])
    for piece in range(pieces):
        here = lines[:, piece, :].astype(jnp.bfloat16)
        total = 0.0
        for term in terms:
            total = total + lax.dot_general(
                term, here, (((0,), (0,)), ((), ())), preferred_element_type=f32
            )
        result[:, piece * wide : (piece + 1) * wide] = total.astype(jnp.bfloat16)


def combine(shares, returned):
    _, pieces, wide = returned.shape
    return pl.pallas_call(
        combine_kernel,
        out_shape=jax.ShapeDtypeStruct((shares.shape[1], pieces * wide), jnp.bfloat16),
        scratch_shapes=[pltpu.VMEM(returned.shape, jnp.float32)],
        compiler_params=pltpu.CompilerParams(vmem_limit_bytes=20 << 20),
        name="combine",
    )(shares, returned)


def body(
    tokens,
    head_state,
    mixer_gain,
    w_query,
    w_key,
    w_value,
    decay_down,
    decay_up,
    decay_base,
    rate_down,
    rate_up,
    head_gain,
    w_out,
    expert_gain,
    expert_ids,
    route_weight,
    w_gate,
    w_up,
    w_down,
):
    rows, width = tokens.shape
    cols = w_query.shape[1]
    layers = lax.axis_size("z")
    lanes = lax.axis_size("tp")
    experts = lax.axis_size(EP)
    lane = lax.axis_index("tp")

    spread_rows, normed, *small = norm(
        tokens, mixer_gain, expert_ids, decay_base, head_gain, route_weight, layers, experts
    )
    spread_rows = swap(spread_rows, "z")
    weights = lax.all_gather(
        jnp.concatenate([w_query, w_key, w_value, w_out.T], axis=1), PLANE, axis=0
    )
    weights = weights.reshape(-1, weights.shape[2])
    weights, normed = lax.optimization_barrier((weights, normed))
    factors, shares = low_rank(
        normed, decay_down, decay_up, rate_down, rate_up, small, experts, lane
    )
    spread_rows, factors, shares = lax.optimization_barrier((spread_rows, factors, shares))
    summed = swap(project(spread_rows, weights, rows, 3 * cols), "z")
    next_state, spread_out = recurrence(summed, factors, head_state)
    mixed_parts = swap(output(swap(spread_out, "z"), weights, lanes), "tp")
    arrived = swap(dispatch(mixed_parts, spread_rows, experts), EP)
    expert_parts, whole = expert_rows(
        arrived, expert_gain, w_gate[0], w_up[0], w_down[0], layers, lanes
    )
    returned = swap(settle(swap(expert_parts, "tp"), whole, lane), EP)
    layer_out = combine(shares, returned)
    return (layer_out, next_state)


def solution(mesh):
    side = math.isqrt(mesh.shape["ep"] // 2)
    grid = Mesh(
        mesh.devices.reshape(side, side, 2, mesh.shape["tp"]), ("z", "y", "c", "tp")
    )
    return jax.shard_map(
        body,
        mesh=grid,
        in_specs=(
            P(EP, None),
            P(EP, "tp", None),
            P(),
            P(EP, "tp"),
            P(EP, "tp"),
            P(EP, "tp"),
            P(),
            P(),
            P("tp"),
            P(),
            P(),
            P("tp"),
            P("tp", EP),
            P(),
            P(EP, None),
            P(EP, None),
            P(EP, None, "tp"),
            P(EP, None, "tp"),
            P(EP, "tp", None),
        ),
        out_specs=(P(EP, "tp"), P(EP, "tp", None)),
        check_vma=False,
    )
```

```python
import functools
import math

import jax
import jax.numpy as jnp
from jax import lax
from jax.experimental import pallas as pl
from jax.experimental.pallas import tpu as pltpu
from jax.sharding import Mesh, PartitionSpec as P

norm_eps = 1e-06
group_eps = 0.00064
EP = ("z", "y", "c")
BY_PLANE = ("y", "c", "z")
PLANE = ("y", "c")


def swap(array, axis):
    return lax.all_to_all(array, axis, split_axis=0, concat_axis=0, tiled=True)


def norm_kernel(experts, *refs):
    sources, refs = refs[:6], refs[6:]
    rows, normed, ids, base, head_gain, route, tokens, gain, done = refs
    layers, depth, block = rows.shape
    count = tokens.shape[0]
    f32, bf16 = jnp.float32, jnp.bfloat16
    targets = (tokens, gain, ids, base, head_gain, route)
    copies = [
        pltpu.make_async_copy(source, target, done.at[k])
        for k, (source, target) in enumerate(zip(sources, targets))
    ]
    for copy in copies:
        copy.start()
    for copy in copies:
        copy.wait()
    widened = tokens[...].astype(f32)
    scale = lax.rsqrt(jnp.mean(widened * widened, axis=1, keepdims=True) + norm_eps)
    scaled = (widened * scale * gain[...]).astype(bf16)
    normed[...] = scaled
    table_shape = (experts, count)
    row = lax.broadcasted_iota(jnp.int32, table_shape, 0)
    named = row == ids[0:1, :]
    for k in range(1, ids.shape[0]):
        named = named | (row == ids[k : k + 1, :])
    offsets = lax.broadcasted_iota(jnp.int32, (8, count), 1) - count
    table = count + lax.dot_general(
        offsets.astype(f32).astype(bf16),
        jnp.where(named, 1.0, 0.0).astype(bf16),
        (((1,), (1,)), ((), ())),
        preferred_element_type=f32,
    )
    table = jnp.concatenate([table, table], axis=0).astype(bf16)
    for z in range(layers):
        here = slice(z * block, (z + 1) * block)
        rows[z, :count] = scaled[:, here]
        rows[z, count : 2 * count] = tokens[:, here]
        rows[z, 2 * count :, :experts] = table


def norm(tokens, gain, expert_ids, decay_base, head_gain, route_weight, layers, experts):
    count, width = tokens.shape
    bf16 = jnp.bfloat16
    line = lambda x: x.reshape(1, -1)
    small = (expert_ids.T, line(decay_base), line(head_gain), route_weight.T)
    inputs = (tokens, line(gain), *small)
    return pl.pallas_call(
        functools.partial(norm_kernel, experts),
        in_specs=[pl.BlockSpec(memory_space=pltpu.HBM)] * len(inputs),
        out_shape=(
            jax.ShapeDtypeStruct((layers, 3 * count, width // layers), bf16),
            jax.ShapeDtypeStruct((count, width), bf16),
            *(jax.ShapeDtypeStruct(x.shape, x.dtype) for x in small),
        ),
        scratch_shapes=[
            pltpu.VMEM((count, width), bf16),
            pltpu.VMEM((1, width), jnp.float32),
            pltpu.SemaphoreType.DMA((len(inputs),)),
        ],
        compiler_params=pltpu.CompilerParams(vmem_limit_bytes=20 << 20),
        name="norm",
    )(*(pltpu.with_memory_space_constraint(x, pltpu.HBM) for x in inputs))


def project_kernel(rows, weights, result):
    layers, count, cols = result.shape
    product = jnp.dot(
        rows[:, :count, :].reshape(layers * count, rows.shape[2]),
        weights[:, :cols],
        preferred_element_type=jnp.float32,
    )
    result[...] = product.astype(jnp.bfloat16).reshape(result.shape)


def project(rows, weights, count, cols):
    return pl.pallas_call(
        project_kernel,
        out_shape=jax.ShapeDtypeStruct((rows.shape[0], count, cols), jnp.bfloat16),
        compiler_params=pltpu.CompilerParams(vmem_limit_bytes=20 << 20),
        name="project",
    )(rows, weights)


def low_rank_kernel(
    layers, lane, normed, down, up, base, rate_down, rate_up, gain, ids, route, result, shares
):
    f32, bf16 = jnp.float32, jnp.bfloat16
    _, count, cols = result.shape
    own = pl.ds(pl.multiple_of(lane[0] * cols, cols), cols)
    rows = normed[...]
    across = lambda w: lax.dot_general(
        rows, w[...], (((1,), (1,)), ((), ())), preferred_element_type=f32
    )
    decay_low = jnp.tanh(across(down)).astype(bf16)
    decay_pre = base[...] + jnp.dot(decay_low, up[:, own], preferred_element_type=f32)
    softplus = jnp.maximum(-decay_pre, 0.0) + jnp.log1p(jnp.exp(-jnp.abs(decay_pre)))
    result[0] = jnp.exp(-jnp.exp(-softplus - 0.5))
    rate_low = across(rate_down).astype(bf16)
    rate_pre = jnp.dot(rate_low, rate_up[:, own], preferred_element_type=f32)
    result[1] = 1.0 / (1.0 + jnp.exp(-rate_pre))
    result[2] = jnp.broadcast_to(gain[...], (count, cols))
    route_sum = jnp.sum(route[...], axis=0, keepdims=True)
    row = lax.broadcasted_iota(jnp.int32, shares.shape, 0)
    row = lax.rem(row, layers) * (shares.shape[0] // layers) + lax.div(row, layers)
    weights = jnp.zeros(shares.shape, f32)
    for k in range(ids.shape[0]):
        share = route[k : k + 1, :] / route_sum
        weights = weights + jnp.where(row == ids[k : k + 1, :], share, 0.0)
    shares[...] = weights


def low_rank(normed, decay_down, decay_up, rate_down, rate_up, small, layers, experts, lane):
    ids, base, head_gain, route = small
    count, cols = normed.shape[0], base.shape[1]
    vmem = pl.BlockSpec(memory_space=pltpu.VMEM)
    return pl.pallas_call(
        functools.partial(low_rank_kernel, layers),
        in_specs=[pl.BlockSpec(memory_space=pltpu.SMEM)] + [vmem] * 9,
        out_specs=(vmem, vmem),
        out_shape=(
            jax.ShapeDtypeStruct((3, count, cols), jnp.float32),
            jax.ShapeDtypeStruct((experts, count), jnp.float32),
        ),
        compiler_params=pltpu.CompilerParams(vmem_limit_bytes=20 << 20),
        name="low_rank",
    )(
        lane.reshape(1),
        normed,
        decay_down.T,
        decay_up,
        base,
        rate_down.T,
        rate_up,
        head_gain,
        ids,
        route,
    )


def split_terms(value):
    high = value.astype(jnp.bfloat16)
    return high, (value - high.astype(jnp.float32)).astype(jnp.bfloat16)


def exact_dot(value, chooser):
    high, low = split_terms(value)
    return jnp.dot(high, chooser, preferred_element_type=jnp.float32) + jnp.dot(
        low, chooser, preferred_element_type=jnp.float32
    )


def recurrence_kernel(size, parts, factors, state, new_state, spread_out, fresh, done):
    decays, rates, gain = factors[0], factors[1], factors[2]
    count, cols = decays.shape
    heads = cols // size
    lines = state.shape[1]
    wide = state.shape[2]
    f32, bf16 = jnp.float32, jnp.bfloat16
    iota = lambda shape, dim: lax.broadcasted_iota(jnp.int32, shape, dim)
    projected = jnp.sum(parts[...].astype(f32), axis=0).astype(bf16).astype(f32)
    queries = projected[:, :cols]
    keys = projected[:, cols : 2 * cols]
    values = projected[:, 2 * cols :]
    square = (cols, cols)
    same_head = iota(square, 0) // size == iota(square, 1) // size
    head_sum = jnp.where(same_head, 1.0, 0.0).astype(bf16)
    head_mean = jnp.where(same_head, 1.0 / size, 0.0).astype(bf16)
    units = keys * lax.rsqrt(exact_dot(keys * keys, head_sum) + 1.0)
    removal = units * rates

    def by_line(x):
        copies = jnp.broadcast_to(x[:, None, :], (count, 2 * heads, cols))
        chosen = iota(copies.shape, 2) // size == iota(copies.shape, 1) % heads
        kept = jnp.where(chosen, copies, 0.0)
        folded = kept[:, :, :wide]
        for start in range(wide, cols, wide):
            folded = folded + kept[:, :, start : start + wide]
        folded = folded.reshape(count * 2 * heads, wide)
        both = folded + pltpu.roll(folded, size, 1)
        return both.reshape(count, 1, 2 * heads, wide)

    grid_shape = (count, lines // (2 * heads), 2 * heads, wide)
    flat = (count * lines, wide)
    old = state[...].reshape(grid_shape)
    halves = (wide, wide)
    half_sum = jnp.where(iota(halves, 0) // size == iota(halves, 1) // size, 1.0, 0.0).astype(bf16)
    removed = exact_dot((old * by_line(units)).reshape(flat), half_sum).reshape(grid_shape)
    pick = (lines, cols)
    line, col = iota(pick, 0), iota(pick, 1)
    owner = (col // size == line % heads) & ((col % size) // 2 == line // heads)
    value_rows = jnp.where(owner[None], jnp.broadcast_to(values[:, None, :], (count, *pick)), 0.0)
    tall = (cols, wide)
    to_half = jnp.where(iota(tall, 0) % 2 == iota(tall, 1) // size, 1.0, 0.0).astype(bf16)
    value_grid = jnp.dot(
        value_rows.reshape(count * lines, cols).astype(bf16), to_half, preferred_element_type=f32
    ).reshape(grid_shape)
    updated = old * by_line(decays) - removed * by_line(removal) + value_grid * by_line(keys)
    fresh[...] = updated.reshape(fresh.shape)
    store = pltpu.make_async_copy(fresh, new_state, done)
    store.start()
    broad = (wide, cols)
    from_half = jnp.where(iota(broad, 0) // size == iota(broad, 1) % 2, 1.0, 0.0).astype(bf16)
    reads = exact_dot((updated * by_line(queries)).reshape(flat), from_half)
    readout = jnp.sum(jnp.where(owner[None], reads.reshape(count, *pick), 0.0), axis=1)
    centred = readout - exact_dot(readout, head_mean)
    spread = exact_dot(centred * centred, head_mean)
    scaled = (centred * lax.rsqrt(spread + group_eps) * gain).astype(bf16)
    spread_out[...] = jnp.broadcast_to(scaled[None], spread_out.shape)
    store.wait()


def recurrence(parts, factors, old_state):
    layers = parts.shape[0]
    _, count, cols = factors.shape
    heads, area = old_state.shape[1:]
    size = math.isqrt(area)
    wide = 2 * size
    lines = area // wide
    state = old_state.reshape(count, heads, lines, wide).transpose(0, 2, 1, 3)
    state = state.reshape(count, lines * heads, wide)
    new_state, spread_out = pl.pallas_call(
        functools.partial(recurrence_kernel, size),
        out_shape=(
            jax.ShapeDtypeStruct(state.shape, jnp.float32),
            jax.ShapeDtypeStruct((layers, count, cols), jnp.bfloat16),
        ),
        out_specs=(
            pl.BlockSpec(memory_space=pltpu.HBM),
            pl.BlockSpec(memory_space=pltpu.VMEM),
        ),
        scratch_shapes=[pltpu.VMEM(state.shape, jnp.float32), pltpu.SemaphoreType.DMA],
        compiler_params=pltpu.CompilerParams(vmem_limit_bytes=40 << 20),
        name="recurrence",
    )(parts, factors, state)
    new_state = new_state.reshape(count, lines, heads, wide).transpose(0, 2, 1, 3)
    return new_state.reshape(old_state.shape), spread_out


def output_kernel(heads, weights, result):
    layers, count, cols = heads.shape
    product = lax.dot_general(
        heads[...].reshape(layers * count, cols),
        weights[:, weights.shape[1] - cols :],
        (((1,), (1,)), ((), ())),
        preferred_element_type=jnp.float32,
    )
    result[...] = jnp.broadcast_to(product.astype(jnp.bfloat16)[None], result.shape)


def output(heads, weights, lanes):
    layers, count, _ = heads.shape
    shape = (lanes, layers * count, weights.shape[0])
    return pl.pallas_call(
        output_kernel,
        out_shape=jax.ShapeDtypeStruct(shape, jnp.bfloat16),
        compiler_params=pltpu.CompilerParams(vmem_limit_bytes=20 << 20),
        name="output",
    )(heads, weights)


def dispatch_kernel(parts, rows, outbound, lines):
    lanes, some, block = parts.shape
    layers = rows.shape[0]
    count = some // layers
    experts, _, wide = lines.shape
    pieces = block // wide
    f32, bf16 = jnp.float32, jnp.bfloat16
    mixed = parts[0].astype(f32)
    for part in range(1, lanes):
        mixed = mixed + parts[part].astype(f32)
    order = lax.broadcasted_iota(jnp.int32, (count, experts), 0).astype(f32)
    for k in range(layers):
        here = rows[k, count : 2 * count, :].astype(f32)
        residual = (here + mixed[k * count : (k + 1) * count]).astype(bf16)
        table = rows[k, 2 * count :, :experts].astype(f32)
        chosen = jnp.where(table == order, 1.0, 0.0).astype(bf16)
        packed = lax.dot_general(
            chosen, residual, (((0,), (0,)), ((), ())), preferred_element_type=f32
        )
        for piece in range(pieces):
            lines[:, piece * layers + k, :] = packed[:, piece * wide : (piece + 1) * wide]
    outbound[...] = lines[:, : pieces * layers, :].astype(bf16)


def dispatch(parts, rows, experts):
    _, _, block = parts.shape
    wide = 128
    shape = (experts, rows.shape[0] * (block // wide), wide)
    return pl.pallas_call(
        dispatch_kernel,
        out_shape=jax.ShapeDtypeStruct(shape, jnp.bfloat16),
        scratch_shapes=[pltpu.VMEM((experts, shape[1] + 8, wide), jnp.float32)],
        compiler_params=pltpu.CompilerParams(vmem_limit_bytes=20 << 20),
        name="dispatch",
    )(parts, rows)


def expert_kernel(layers, arrived, gain, gate, up, down, result, rows):
    lanes, count, quarter = result.shape
    peers = count // layers
    wide = arrived.shape[2]
    pieces = arrived.shape[1] // layers
    f32 = jnp.float32
    for z in range(layers):
        blocks = arrived[z * peers : (z + 1) * peers].astype(f32)
        for piece in range(pieces):
            start = (z * pieces + piece) * wide
            block = blocks[:, piece * layers : (piece + 1) * layers, :].reshape(count, wide)
            rows[:, start : start + wide] = block.astype(jnp.bfloat16)
    widened = rows[...].astype(f32)
    scale = lax.rsqrt(jnp.mean(widened * widened, axis=1, keepdims=True) + norm_eps)
    normed = (widened * scale * gain[...]).astype(jnp.bfloat16)
    gate_act = jnp.dot(normed, gate[...], preferred_element_type=f32)
    up_act = jnp.dot(normed, up[...], preferred_element_type=f32)
    hidden = (gate_act / (1.0 + jnp.exp(-gate_act)) * up_act).astype(jnp.bfloat16)
    for part in range(lanes):
        here = slice(part * quarter, (part + 1) * quarter)
        product = jnp.dot(hidden, down[:, here], preferred_element_type=f32)
        result[part] = product.astype(jnp.bfloat16)


def expert_rows(arrived, gain, gate, up, down, layers, lanes):
    count = arrived.shape[0]
    width = gate.shape[0]
    return pl.pallas_call(
        functools.partial(expert_kernel, layers),
        out_shape=(
            jax.ShapeDtypeStruct((lanes, count, width // lanes), jnp.bfloat16),
            jax.ShapeDtypeStruct((count, width), jnp.bfloat16),
        ),
        compiler_params=pltpu.CompilerParams(vmem_limit_bytes=20 << 20),
        name="expert",
    )(arrived, gain.reshape(1, width), gate, up, down)


def settle_kernel(lane, parts, rows, result, lines):
    lanes, count, quarter = parts.shape
    pieces, wide = lines.shape[1:]
    own = pl.ds(pl.multiple_of(lane[0] * quarter, quarter), quarter)
    total = rows[:, own].astype(jnp.float32)
    for part in range(lanes):
        total = total + parts[part].astype(jnp.float32)
    for piece in range(pieces):
        lines[:, piece, :] = total[:, piece * wide : (piece + 1) * wide]
    result[...] = lines[...].astype(jnp.bfloat16)


def settle(parts, rows, lane):
    _, count, quarter = parts.shape
    shape = (count, quarter // 128, 128)
    vmem = pl.BlockSpec(memory_space=pltpu.VMEM)
    return pl.pallas_call(
        settle_kernel,
        in_specs=[pl.BlockSpec(memory_space=pltpu.SMEM), vmem, vmem],
        out_specs=vmem,
        out_shape=jax.ShapeDtypeStruct(shape, jnp.bfloat16),
        scratch_shapes=[pltpu.VMEM(shape, jnp.float32)],
        compiler_params=pltpu.CompilerParams(vmem_limit_bytes=20 << 20),
        name="settle",
    )(lane.reshape(1), parts, rows)


def combine_kernel(shares, returned, result, lines):
    _, pieces, wide = returned.shape
    f32 = jnp.float32
    lines[...] = returned[...].astype(f32)
    terms = split_terms(shares[...])
    for piece in range(pieces):
        here = lines[:, piece, :].astype(jnp.bfloat16)
        total = 0.0
        for term in terms:
            total = total + lax.dot_general(
                term, here, (((0,), (0,)), ((), ())), preferred_element_type=f32
            )
        result[:, piece * wide : (piece + 1) * wide] = total.astype(jnp.bfloat16)


def combine(shares, returned):
    _, pieces, wide = returned.shape
    return pl.pallas_call(
        combine_kernel,
        out_shape=jax.ShapeDtypeStruct((shares.shape[1], pieces * wide), jnp.bfloat16),
        scratch_shapes=[pltpu.VMEM(returned.shape, jnp.float32)],
        compiler_params=pltpu.CompilerParams(vmem_limit_bytes=20 << 20),
        name="combine",
    )(shares, returned)


def body(
    tokens,
    head_state,
    mixer_gain,
    w_query,
    w_key,
    w_value,
    decay_down,
    decay_up,
    decay_base,
    rate_down,
    rate_up,
    head_gain,
    w_out,
    expert_gain,
    expert_ids,
    route_weight,
    w_gate,
    w_up,
    w_down,
):
    rows, width = tokens.shape
    cols = w_query.shape[1]
    layers = lax.axis_size("z")
    lanes = lax.axis_size("tp")
    experts = lax.axis_size(EP)
    lane = lax.axis_index("tp")

    spread_rows, normed, *small = norm(
        tokens, mixer_gain, expert_ids, decay_base, head_gain, route_weight, layers, experts
    )
    spread_rows = swap(spread_rows, "z")
    weights = lax.all_gather(
        jnp.concatenate([w_query, w_key, w_value, w_out.T], axis=1), PLANE, axis=0
    )
    weights = weights.reshape(-1, weights.shape[2])
    weights, normed = lax.optimization_barrier((weights, normed))
    factors, shares = low_rank(
        normed, decay_down, decay_up, rate_down, rate_up, small, layers, experts, lane
    )
    spread_rows, factors, shares = lax.optimization_barrier((spread_rows, factors, shares))
    summed = swap(project(spread_rows, weights, rows, 3 * cols), "z")
    next_state, spread_out = recurrence(summed, factors, head_state)
    mixed_parts = swap(output(swap(spread_out, "z"), weights, lanes), "tp")
    arrived = swap(dispatch(mixed_parts, spread_rows, experts), EP)
    expert_parts, whole = expert_rows(
        arrived, expert_gain, w_gate[0], w_up[0], w_down[0], layers, lanes
    )
    returned = swap(settle(swap(expert_parts, "tp"), whole, lane), BY_PLANE)
    layer_out = combine(shares, returned)
    return (layer_out, next_state)


def solution(mesh):
    side = math.isqrt(mesh.shape["ep"] // 2)
    grid = Mesh(
        mesh.devices.reshape(side, side, 2, mesh.shape["tp"]), ("z", "y", "c", "tp")
    )
    return jax.shard_map(
        body,
        mesh=grid,
        in_specs=(
            P(EP, None),
            P(EP, "tp", None),
            P(),
            P(EP, "tp"),
            P(EP, "tp"),
            P(EP, "tp"),
            P(),
            P(),
            P("tp"),
            P(),
            P(),
            P("tp"),
            P("tp", EP),
            P(),
            P(EP, None),
            P(EP, None),
            P(EP, None, "tp"),
            P(EP, None, "tp"),
            P(EP, "tp", None),
        ),
        out_specs=(P(EP, "tp"), P(EP, "tp", None)),
        check_vma=False,
    )
```

```python
import functools
import math

import jax
import jax.numpy as jnp
from jax import lax
from jax.experimental import pallas as pl
from jax.experimental.pallas import tpu as pltpu
from jax.sharding import Mesh, PartitionSpec as P

norm_eps = 1e-06
group_eps = 0.00064
EP = ("z", "y", "c")
BY_PLANE = ("y", "c", "z")
PLANE = ("y", "c")


def swap(array, axis):
    return lax.all_to_all(array, axis, split_axis=0, concat_axis=0, tiled=True)


def norm_kernel(experts, *refs):
    sources, refs = refs[:6], refs[6:]
    rows, normed, ids, base, head_gain, route, tokens, gain, done = refs
    layers, depth, block = rows.shape
    count = tokens.shape[0]
    f32, bf16 = jnp.float32, jnp.bfloat16
    targets = (tokens, gain, ids, base, head_gain, route)
    copies = [
        pltpu.make_async_copy(source, target, done.at[k])
        for k, (source, target) in enumerate(zip(sources, targets))
    ]
    for copy in copies:
        copy.start()
    for copy in copies:
        copy.wait()
    widened = tokens[...].astype(f32)
    scale = lax.rsqrt(jnp.mean(widened * widened, axis=1, keepdims=True) + norm_eps)
    scaled = (widened * scale * gain[...]).astype(bf16)
    normed[...] = scaled
    table_shape = (experts, count)
    row = lax.broadcasted_iota(jnp.int32, table_shape, 0)
    row = lax.rem(row, layers) * (experts // layers) + lax.div(row, layers)
    named = row == ids[0:1, :]
    for k in range(1, ids.shape[0]):
        named = named | (row == ids[k : k + 1, :])
    offsets = lax.broadcasted_iota(jnp.int32, (8, count), 1) - count
    table = count + lax.dot_general(
        offsets.astype(f32).astype(bf16),
        jnp.where(named, 1.0, 0.0).astype(bf16),
        (((1,), (1,)), ((), ())),
        preferred_element_type=f32,
    )
    table = jnp.concatenate([table, table], axis=0).astype(bf16)
    for z in range(layers):
        here = slice(z * block, (z + 1) * block)
        rows[z, :count] = scaled[:, here]
        rows[z, count : 2 * count] = tokens[:, here]
        rows[z, 2 * count :, :experts] = table


def norm(tokens, gain, expert_ids, decay_base, head_gain, route_weight, layers, experts):
    count, width = tokens.shape
    bf16 = jnp.bfloat16
    line = lambda x: x.reshape(1, -1)
    small = (expert_ids.T, line(decay_base), line(head_gain), route_weight.T)
    inputs = (tokens, line(gain), *small)
    return pl.pallas_call(
        functools.partial(norm_kernel, experts),
        in_specs=[pl.BlockSpec(memory_space=pltpu.HBM)] * len(inputs),
        out_shape=(
            jax.ShapeDtypeStruct((layers, 3 * count, width // layers), bf16),
            jax.ShapeDtypeStruct((count, width), bf16),
            *(jax.ShapeDtypeStruct(x.shape, x.dtype) for x in small),
        ),
        scratch_shapes=[
            pltpu.VMEM((count, width), bf16),
            pltpu.VMEM((1, width), jnp.float32),
            pltpu.SemaphoreType.DMA((len(inputs),)),
        ],
        compiler_params=pltpu.CompilerParams(vmem_limit_bytes=20 << 20),
        name="norm",
    )(*(pltpu.with_memory_space_constraint(x, pltpu.HBM) for x in inputs))


def project_kernel(rows, weights, result):
    layers, count, cols = result.shape
    product = jnp.dot(
        rows[:, :count, :].reshape(layers * count, rows.shape[2]),
        weights[:, :cols],
        preferred_element_type=jnp.float32,
    )
    result[...] = product.astype(jnp.bfloat16).reshape(result.shape)


def project(rows, weights, count, cols):
    return pl.pallas_call(
        project_kernel,
        out_shape=jax.ShapeDtypeStruct((rows.shape[0], count, cols), jnp.bfloat16),
        compiler_params=pltpu.CompilerParams(vmem_limit_bytes=20 << 20),
        name="project",
    )(rows, weights)


def low_rank_kernel(
    layers, lane, normed, down, up, base, rate_down, rate_up, gain, ids, route, result, shares
):
    f32, bf16 = jnp.float32, jnp.bfloat16
    _, count, cols = result.shape
    own = pl.ds(pl.multiple_of(lane[0] * cols, cols), cols)
    rows = normed[...]
    across = lambda w: lax.dot_general(
        rows, w[...], (((1,), (1,)), ((), ())), preferred_element_type=f32
    )
    decay_low = jnp.tanh(across(down)).astype(bf16)
    decay_pre = base[...] + jnp.dot(decay_low, up[:, own], preferred_element_type=f32)
    softplus = jnp.maximum(-decay_pre, 0.0) + jnp.log1p(jnp.exp(-jnp.abs(decay_pre)))
    result[0] = jnp.exp(-jnp.exp(-softplus - 0.5))
    rate_low = across(rate_down).astype(bf16)
    rate_pre = jnp.dot(rate_low, rate_up[:, own], preferred_element_type=f32)
    result[1] = 1.0 / (1.0 + jnp.exp(-rate_pre))
    result[2] = jnp.broadcast_to(gain[...], (count, cols))
    route_sum = jnp.sum(route[...], axis=0, keepdims=True)
    row = lax.broadcasted_iota(jnp.int32, shares.shape, 0)
    row = lax.rem(row, layers) * (shares.shape[0] // layers) + lax.div(row, layers)
    weights = jnp.zeros(shares.shape, f32)
    for k in range(ids.shape[0]):
        share = route[k : k + 1, :] / route_sum
        weights = weights + jnp.where(row == ids[k : k + 1, :], share, 0.0)
    shares[...] = weights


def low_rank(normed, decay_down, decay_up, rate_down, rate_up, small, layers, experts, lane):
    ids, base, head_gain, route = small
    count, cols = normed.shape[0], base.shape[1]
    vmem = pl.BlockSpec(memory_space=pltpu.VMEM)
    return pl.pallas_call(
        functools.partial(low_rank_kernel, layers),
        in_specs=[pl.BlockSpec(memory_space=pltpu.SMEM)] + [vmem] * 9,
        out_specs=(vmem, vmem),
        out_shape=(
            jax.ShapeDtypeStruct((3, count, cols), jnp.float32),
            jax.ShapeDtypeStruct((experts, count), jnp.float32),
        ),
        compiler_params=pltpu.CompilerParams(vmem_limit_bytes=20 << 20),
        name="low_rank",
    )(
        lane.reshape(1),
        normed,
        decay_down.T,
        decay_up,
        base,
        rate_down.T,
        rate_up,
        head_gain,
        ids,
        route,
    )


def split_terms(value):
    high = value.astype(jnp.bfloat16)
    return high, (value - high.astype(jnp.float32)).astype(jnp.bfloat16)


def exact_dot(value, chooser):
    high, low = split_terms(value)
    return jnp.dot(high, chooser, preferred_element_type=jnp.float32) + jnp.dot(
        low, chooser, preferred_element_type=jnp.float32
    )


def recurrence_kernel(size, parts, factors, state, new_state, spread_out, fresh, done):
    decays, rates, gain = factors[0], factors[1], factors[2]
    count, cols = decays.shape
    heads = cols // size
    lines = state.shape[1]
    wide = state.shape[2]
    f32, bf16 = jnp.float32, jnp.bfloat16
    iota = lambda shape, dim: lax.broadcasted_iota(jnp.int32, shape, dim)
    projected = jnp.sum(parts[...].astype(f32), axis=0).astype(bf16).astype(f32)
    queries = projected[:, :cols]
    keys = projected[:, cols : 2 * cols]
    values = projected[:, 2 * cols :]
    square = (cols, cols)
    same_head = iota(square, 0) // size == iota(square, 1) // size
    head_sum = jnp.where(same_head, 1.0, 0.0).astype(bf16)
    head_mean = jnp.where(same_head, 1.0 / size, 0.0).astype(bf16)
    units = keys * lax.rsqrt(exact_dot(keys * keys, head_sum) + 1.0)
    removal = units * rates

    def by_line(x):
        copies = jnp.broadcast_to(x[:, None, :], (count, 2 * heads, cols))
        chosen = iota(copies.shape, 2) // size == iota(copies.shape, 1) % heads
        kept = jnp.where(chosen, copies, 0.0)
        folded = kept[:, :, :wide]
        for start in range(wide, cols, wide):
            folded = folded + kept[:, :, start : start + wide]
        folded = folded.reshape(count * 2 * heads, wide)
        both = folded + pltpu.roll(folded, size, 1)
        return both.reshape(count, 1, 2 * heads, wide)

    grid_shape = (count, lines // (2 * heads), 2 * heads, wide)
    flat = (count * lines, wide)
    old = state[...].reshape(grid_shape)
    halves = (wide, wide)
    half_sum = jnp.where(iota(halves, 0) // size == iota(halves, 1) // size, 1.0, 0.0).astype(bf16)
    removed = exact_dot((old * by_line(units)).reshape(flat), half_sum).reshape(grid_shape)
    pick = (lines, cols)
    line, col = iota(pick, 0), iota(pick, 1)
    owner = (col // size == line % heads) & ((col % size) // 2 == line // heads)
    value_rows = jnp.where(owner[None], jnp.broadcast_to(values[:, None, :], (count, *pick)), 0.0)
    tall = (cols, wide)
    to_half = jnp.where(iota(tall, 0) % 2 == iota(tall, 1) // size, 1.0, 0.0).astype(bf16)
    value_grid = jnp.dot(
        value_rows.reshape(count * lines, cols).astype(bf16), to_half, preferred_element_type=f32
    ).reshape(grid_shape)
    updated = old * by_line(decays) - removed * by_line(removal) + value_grid * by_line(keys)
    fresh[...] = updated.reshape(fresh.shape)
    store = pltpu.make_async_copy(fresh, new_state, done)
    store.start()
    broad = (wide, cols)
    from_half = jnp.where(iota(broad, 0) // size == iota(broad, 1) % 2, 1.0, 0.0).astype(bf16)
    reads = exact_dot((updated * by_line(queries)).reshape(flat), from_half)
    readout = jnp.sum(jnp.where(owner[None], reads.reshape(count, *pick), 0.0), axis=1)
    centred = readout - exact_dot(readout, head_mean)
    spread = exact_dot(centred * centred, head_mean)
    scaled = (centred * lax.rsqrt(spread + group_eps) * gain).astype(bf16)
    spread_out[...] = jnp.broadcast_to(scaled[None], spread_out.shape)
    store.wait()


def recurrence(parts, factors, old_state):
    layers = parts.shape[0]
    _, count, cols = factors.shape
    heads, area = old_state.shape[1:]
    size = math.isqrt(area)
    wide = 2 * size
    lines = area // wide
    state = old_state.reshape(count, heads, lines, wide).transpose(0, 2, 1, 3)
    state = state.reshape(count, lines * heads, wide)
    new_state, spread_out = pl.pallas_call(
        functools.partial(recurrence_kernel, size),
        out_shape=(
            jax.ShapeDtypeStruct(state.shape, jnp.float32),
            jax.ShapeDtypeStruct((layers, count, cols), jnp.bfloat16),
        ),
        out_specs=(
            pl.BlockSpec(memory_space=pltpu.HBM),
            pl.BlockSpec(memory_space=pltpu.VMEM),
        ),
        scratch_shapes=[pltpu.VMEM(state.shape, jnp.float32), pltpu.SemaphoreType.DMA],
        compiler_params=pltpu.CompilerParams(vmem_limit_bytes=40 << 20),
        name="recurrence",
    )(parts, factors, state)
    new_state = new_state.reshape(count, lines, heads, wide).transpose(0, 2, 1, 3)
    return new_state.reshape(old_state.shape), spread_out


def output_kernel(heads, weights, result):
    layers, count, cols = heads.shape
    product = lax.dot_general(
        heads[...].reshape(layers * count, cols),
        weights[:, weights.shape[1] - cols :],
        (((1,), (1,)), ((), ())),
        preferred_element_type=jnp.float32,
    )
    result[...] = jnp.broadcast_to(product.astype(jnp.bfloat16)[None], result.shape)


def output(heads, weights, lanes):
    layers, count, _ = heads.shape
    shape = (lanes, layers * count, weights.shape[0])
    return pl.pallas_call(
        output_kernel,
        out_shape=jax.ShapeDtypeStruct(shape, jnp.bfloat16),
        compiler_params=pltpu.CompilerParams(vmem_limit_bytes=20 << 20),
        name="output",
    )(heads, weights)


def dispatch_kernel(parts, rows, outbound, lines):
    lanes, some, block = parts.shape
    layers = rows.shape[0]
    count = some // layers
    experts, _, wide = lines.shape
    pieces = block // wide
    f32, bf16 = jnp.float32, jnp.bfloat16
    mixed = parts[0].astype(f32)
    for part in range(1, lanes):
        mixed = mixed + parts[part].astype(f32)
    order = lax.broadcasted_iota(jnp.int32, (count, experts), 0).astype(f32)
    for k in range(layers):
        here = rows[k, count : 2 * count, :].astype(f32)
        residual = (here + mixed[k * count : (k + 1) * count]).astype(bf16)
        table = rows[k, 2 * count :, :experts].astype(f32)
        chosen = jnp.where(table == order, 1.0, 0.0).astype(bf16)
        packed = lax.dot_general(
            chosen, residual, (((0,), (0,)), ((), ())), preferred_element_type=f32
        )
        for piece in range(pieces):
            lines[:, piece * layers + k, :] = packed[:, piece * wide : (piece + 1) * wide]
    outbound[...] = lines[:, : pieces * layers, :].astype(bf16)


def dispatch(parts, rows, experts):
    _, _, block = parts.shape
    wide = 128
    shape = (experts, rows.shape[0] * (block // wide), wide)
    return pl.pallas_call(
        dispatch_kernel,
        out_shape=jax.ShapeDtypeStruct(shape, jnp.bfloat16),
        scratch_shapes=[pltpu.VMEM((experts, shape[1] + 8, wide), jnp.float32)],
        compiler_params=pltpu.CompilerParams(vmem_limit_bytes=20 << 20),
        name="dispatch",
    )(parts, rows)


def expert_kernel(layers, arrived, gain, gate, up, down, result, rows):
    lanes, count, quarter = result.shape
    peers = count // layers
    wide = arrived.shape[2]
    pieces = arrived.shape[1] // layers
    f32 = jnp.float32
    planes = arrived[...].reshape(peers, layers, *arrived.shape[1:])
    for z in range(layers):
        blocks = planes[:, z].astype(f32)
        for piece in range(pieces):
            start = (z * pieces + piece) * wide
            block = blocks[:, piece * layers : (piece + 1) * layers, :].reshape(count, wide)
            rows[:, start : start + wide] = block.astype(jnp.bfloat16)
    widened = rows[...].astype(f32)
    scale = lax.rsqrt(jnp.mean(widened * widened, axis=1, keepdims=True) + norm_eps)
    normed = (widened * scale * gain[...]).astype(jnp.bfloat16)
    gate_act = jnp.dot(normed, gate[...], preferred_element_type=f32)
    up_act = jnp.dot(normed, up[...], preferred_element_type=f32)
    hidden = (gate_act / (1.0 + jnp.exp(-gate_act)) * up_act).astype(jnp.bfloat16)
    for part in range(lanes):
        here = slice(part * quarter, (part + 1) * quarter)
        product = jnp.dot(hidden, down[:, here], preferred_element_type=f32)
        result[part] = product.astype(jnp.bfloat16)


def expert_rows(arrived, gain, gate, up, down, layers, lanes):
    count = arrived.shape[0]
    width = gate.shape[0]
    return pl.pallas_call(
        functools.partial(expert_kernel, layers),
        out_shape=(
            jax.ShapeDtypeStruct((lanes, count, width // lanes), jnp.bfloat16),
            jax.ShapeDtypeStruct((count, width), jnp.bfloat16),
        ),
        compiler_params=pltpu.CompilerParams(vmem_limit_bytes=20 << 20),
        name="expert",
    )(arrived, gain.reshape(1, width), gate, up, down)


def settle_kernel(lane, parts, rows, result, lines):
    lanes, count, quarter = parts.shape
    pieces, wide = lines.shape[1:]
    own = pl.ds(pl.multiple_of(lane[0] * quarter, quarter), quarter)
    total = rows[:, own].astype(jnp.float32)
    for part in range(lanes):
        total = total + parts[part].astype(jnp.float32)
    for piece in range(pieces):
        lines[:, piece, :] = total[:, piece * wide : (piece + 1) * wide]
    result[...] = lines[...].astype(jnp.bfloat16)


def settle(parts, rows, lane):
    _, count, quarter = parts.shape
    shape = (count, quarter // 128, 128)
    vmem = pl.BlockSpec(memory_space=pltpu.VMEM)
    return pl.pallas_call(
        settle_kernel,
        in_specs=[pl.BlockSpec(memory_space=pltpu.SMEM), vmem, vmem],
        out_specs=vmem,
        out_shape=jax.ShapeDtypeStruct(shape, jnp.bfloat16),
        scratch_shapes=[pltpu.VMEM(shape, jnp.float32)],
        compiler_params=pltpu.CompilerParams(vmem_limit_bytes=20 << 20),
        name="settle",
    )(lane.reshape(1), parts, rows)


def combine_kernel(shares, returned, result, lines):
    _, pieces, wide = returned.shape
    f32 = jnp.float32
    lines[...] = returned[...].astype(f32)
    terms = split_terms(shares[...])
    for piece in range(pieces):
        here = lines[:, piece, :].astype(jnp.bfloat16)
        total = 0.0
        for term in terms:
            total = total + lax.dot_general(
                term, here, (((0,), (0,)), ((), ())), preferred_element_type=f32
            )
        result[:, piece * wide : (piece + 1) * wide] = total.astype(jnp.bfloat16)


def combine(shares, returned):
    _, pieces, wide = returned.shape
    return pl.pallas_call(
        combine_kernel,
        out_shape=jax.ShapeDtypeStruct((shares.shape[1], pieces * wide), jnp.bfloat16),
        scratch_shapes=[pltpu.VMEM(returned.shape, jnp.float32)],
        compiler_params=pltpu.CompilerParams(vmem_limit_bytes=20 << 20),
        name="combine",
    )(shares, returned)


def body(
    tokens,
    head_state,
    mixer_gain,
    w_query,
    w_key,
    w_value,
    decay_down,
    decay_up,
    decay_base,
    rate_down,
    rate_up,
    head_gain,
    w_out,
    expert_gain,
    expert_ids,
    route_weight,
    w_gate,
    w_up,
    w_down,
):
    rows, width = tokens.shape
    cols = w_query.shape[1]
    layers = lax.axis_size("z")
    lanes = lax.axis_size("tp")
    experts = lax.axis_size(EP)
    lane = lax.axis_index("tp")

    spread_rows, normed, *small = norm(
        tokens, mixer_gain, expert_ids, decay_base, head_gain, route_weight, layers, experts
    )
    spread_rows = swap(spread_rows, "z")
    weights = lax.all_gather(
        jnp.concatenate([w_query, w_key, w_value, w_out.T], axis=1), PLANE, axis=0
    )
    weights = weights.reshape(-1, weights.shape[2])
    weights, normed = lax.optimization_barrier((weights, normed))
    factors, shares = low_rank(
        normed, decay_down, decay_up, rate_down, rate_up, small, layers, experts, lane
    )
    spread_rows, factors, shares = lax.optimization_barrier((spread_rows, factors, shares))
    summed = swap(project(spread_rows, weights, rows, 3 * cols), "z")
    next_state, spread_out = recurrence(summed, factors, head_state)
    mixed_parts = swap(output(swap(spread_out, "z"), weights, lanes), "tp")
    arrived = swap(dispatch(mixed_parts, spread_rows, experts), BY_PLANE)
    expert_parts, whole = expert_rows(
        arrived, expert_gain, w_gate[0], w_up[0], w_down[0], layers, lanes
    )
    returned = swap(settle(swap(expert_parts, "tp"), whole, lane), BY_PLANE)
    layer_out = combine(shares, returned)
    return (layer_out, next_state)


def solution(mesh):
    side = math.isqrt(mesh.shape["ep"] // 2)
    grid = Mesh(
        mesh.devices.reshape(side, side, 2, mesh.shape["tp"]), ("z", "y", "c", "tp")
    )
    return jax.shard_map(
        body,
        mesh=grid,
        in_specs=(
            P(EP, None),
            P(EP, "tp", None),
            P(),
            P(EP, "tp"),
            P(EP, "tp"),
            P(EP, "tp"),
            P(),
            P(),
            P("tp"),
            P(),
            P(),
            P("tp"),
            P("tp", EP),
            P(),
            P(EP, None),
            P(EP, None),
            P(EP, None, "tp"),
            P(EP, None, "tp"),
            P(EP, "tp", None),
        ),
        out_specs=(P(EP, "tp"), P(EP, "tp", None)),
        check_vma=False,
    )
```
